32 devices in a mesh: ep: 8 (over z, x), tp: 4 (over y, core).
Axes of the slice: x: 2, y: 2, z: 4, core: 2. Of those that a mesh axis runs over, the one named last changes fastest.
Arguments:
- mix_in: bfloat16 [1024, 2048], P('ep'), may hold values from -6 to 6
- mix_gain: float32 [2048], replicated, may hold values from 0.1 to 1.9
- query_weight: bfloat16 [2048, 3072], P(None, 'tp'), may hold values from -0.125 to 0.125
- latent_weight: bfloat16 [2048, 512], replicated, may hold values from -0.125 to 0.125
- rotary_weight: bfloat16 [2048, 64], replicated, may hold values from -0.125 to 0.125
- latent_gain: float32 [512], replicated, may hold values from 0.1 to 1.9
- key_weight: bfloat16 [512, 2048], P(None, 'tp'), may hold values from -0.25 to 0.25
- value_weight: bfloat16 [512, 2048], P(None, 'tp'), may hold values from -0.25 to 0.25
- output_weight: bfloat16 [2048, 2048], P('tp'), may hold values from -0.125 to 0.125
- out_gain: float32 [2048], replicated, may hold values from 0.1 to 1.9
- ffn_in: bfloat16 [1024, 2048], P('ep'), may hold values from -6 to 6
- ffn_gain: float32 [2048], replicated, may hold values from 0.1 to 1.9
- gate_weight: bfloat16 [8, 2048, 1024], P('ep', None, 'tp'), may hold values from -0.375 to 0.375
- up_weight: bfloat16 [8, 2048, 1024], P('ep', None, 'tp'), may hold values from -0.375 to 0.375
- down_weight: bfloat16 [8, 1024, 2048], P('ep', 'tp'), may hold values from -0.046875 to 0.046875
- routes: int32 [1024, 4], P('ep'), may hold values from 0 to 7, all different within a row; in each aligned block of 32 rows (0 to 31, 32 to 63, ...) at most 32 rows name the same one
- route_scores: float32 [1024, 4], P('ep'), may hold values from -6 to 6
Outputs:
- mixed: bfloat16 [1024, 2048], P(('ep', 'tp'))
- moe_out: bfloat16 [1024, 2048], P(('ep', 'tp'))
The draws below stay inside these ranges and needn't reach their ends.
Inputs may be any that keep to these rules, and one draw needn't show every extreme that they name: `routes`: each row names 4 different experts; in each aligned block of 32 rows no expert is named by more than 32 rows, a bound that some blocks reach.
All inputs are finite; a program needn't handle non-finite values.
Results may differ from the reference program's by a relative error of at most 0.014.
Values may be sent and summed in bfloat16 or wider, within the bound.
A program may use at most 192 MiB of HBM per device.

```python
import math
import jax
import jax.numpy as jnp
import numpy as np
from jax import lax

D = 2048
HEADS = 16
NOPE = 128
ROPE = 64
VD = 128
KVR = 512
FF = 1024
TOP = 4
EXPERTS = 8
TOKENS_A = 1024
TOKENS_B = 1024
QB = 32
MOST = 32
N_TP = 4


def steps_of(own_key, shape, pieces, least, high):
    factor_of = 1.0
    for position, blocks in pieces:
        heights = jax.random.uniform(jax.random.fold_in(jax.random.fold_in(own_key, 6), position), (blocks,), jnp.float32, least / len(pieces), high / len(pieces))
        factor_of = factor_of * jnp.repeat(jnp.exp(heights), shape[position] // blocks).reshape((-1,) + (1,) * (len(shape) - 1 - position))
    return factor_of


def assign_block(key, own, number, rows, count, top, bound, slope):
    ranking = jax.random.permutation(key, count)
    crowded, usual = portions_of(count, rows * top, bound, slope, True), portions_of(count, rows * top, bound, slope, False)
    places = jnp.arange(count)

    def named(lengths, turn):
        used = int((lengths > 0).sum())
        fixed = max(1, used // 4)
        moved = fixed + (places - fixed + turn * (used - fixed)) % max(1, count - fixed)
        return jnp.zeros((count,), jnp.int32).at[ranking[jnp.where(places < fixed, places, moved)]].set(jnp.asarray(lengths, jnp.int32))

    lengths = jnp.where(number % 4 == 0, named(crowded, number // 4), named(usual, number - number // 4 - 1))
    mixed = jax.random.permutation(jax.random.fold_in(own, 3), count)
    source_of, taker = mixed[0:count // 2 * 2:2], mixed[1:count // 2 * 2:2]
    room = jnp.minimum(lengths[source_of] - 1, bound - lengths[taker]) // 2
    room = jnp.where((source_of == ranking[0]) | (taker == ranking[0]) | (lengths[taker] == 0), 0, jnp.maximum(room, 0))
    moved = jax.random.randint(jax.random.fold_in(own, 4), (count // 2,), 0, 1 << 20) % (room + 1)
    lengths = lengths.at[source_of].add(-moved).at[taker].add(moved)
    items = jnp.searchsorted(jnp.cumsum(lengths), jnp.arange(rows * top), side="right").astype(jnp.int32)
    table = items.reshape(top, rows).T
    table = table[jax.random.permutation(jax.random.fold_in(own, 1), rows)]
    turn = jax.random.randint(jax.random.fold_in(own, 2), (rows, 1), 0, top)
    return jnp.take_along_axis(table, (jnp.arange(top)[None, :] + turn) % top, axis=1)


def portions_of(count, total, most, lean, full):
    portions = [(1 << 20) // math.isqrt(grade ** lean) + 1 for grade in range(1, count + 1)]
    largest = most if full else min(most, max(-(-total // count), total * portions[0] // sum(portions)))
    least = 1 if total - largest >= count - 1 else 0
    holding, rest = [largest] + [least] * (count - 1), total - largest - least * (count - 1)
    while rest > 0:
        movable = [i for i in range(1, count) if holding[i] < largest] or [i for i in range(1, count) if holding[i] < most]
        mass, budget = sum([portions[i] for i in movable]), rest
        for i in movable:
            more = min(most - holding[i], max(1, budget * portions[i] // mass), rest)
            holding[i] = holding[i] + more
            rest = rest - more
    return np.array(holding)


def noise(own_key, dims, deviation, limit, split=(), kind=jnp.bfloat16):
    gain = steps_of(own_key, dims, split, -0.22, 0.18) if split else 1.0
    drawn = jax.random.normal(own_key, dims, jnp.float32) * deviation * gain
    return jnp.minimum(jnp.maximum(drawn, -limit), limit).astype(kind)


def setup_inputs(seed: int = 0) -> dict:
    key_list = jax.random.split(jax.random.key(seed), 18)
    mix_in = noise(key_list[0], (TOKENS_A, D), 1.0, 6.0, ((0, 8),))
    mix_gain = jnp.clip(1.0 + 0.18 * jax.random.normal(key_list[1], (D,), jnp.float32), 0.1, 1.9)
    query_weight = noise(key_list[2], (D, HEADS * (NOPE + ROPE)), D ** -0.5, 0.125, ((1, 4),))
    latent_weight = noise(key_list[3], (D, KVR), D ** -0.5, 0.125)
    rotary_weight = noise(key_list[4], (D, ROPE), D ** -0.5, 0.125)
    latent_gain = jnp.clip(1.0 + 0.18 * jax.random.normal(key_list[5], (KVR,), jnp.float32), 0.1, 1.9)
    key_weight = noise(key_list[6], (KVR, HEADS * NOPE), KVR ** -0.5, 0.25, ((1, 4),))
    value_weight = noise(key_list[7], (KVR, HEADS * VD), KVR ** -0.5, 0.25, ((1, 4),))
    output_weight = noise(key_list[8], (HEADS * VD, D), (HEADS * VD) ** -0.5, 0.125, ((0, 4),))
    out_gain = jnp.clip(1.0 + 0.18 * jax.random.normal(key_list[9], (D,), jnp.float32), 0.1, 1.9)
    ffn_in = noise(key_list[10], (TOKENS_B, D), 1.0, 6.0, ((0, 8),))
    ffn_gain = jnp.clip(1.0 + 0.18 * jax.random.normal(key_list[11], (D,), jnp.float32), 0.1, 1.9)
    gate_weight = noise(key_list[12], (EXPERTS, D, FF), (D // 8) ** -0.5, 0.375, ((0, 8), (2, 4)))
    up_weight = noise(key_list[13], (EXPERTS, D, FF), (D // 8) ** -0.5, 0.375, ((0, 8), (2, 4)))
    down_weight = noise(key_list[14], (EXPERTS, FF, D), (FF * 16) ** -0.5, 0.046875, ((0, 8), (1, 4)))
    routes_keys = jax.random.split(jax.random.fold_in(key_list[15], 1), TOKENS_B // QB)
    routes_turns = jax.random.permutation(jax.random.fold_in(key_list[15], 3), TOKENS_B // QB)
    routes = jax.vmap(lambda own, number: assign_block(jax.random.fold_in(key_list[15], 2), own, number, QB, EXPERTS, TOP, MOST, 2))(routes_keys, routes_turns).reshape((TOKENS_B, TOP))
    route_scores = noise(key_list[16], (TOKENS_B, TOP), 1.0, 6.0, ((0, 8),), jnp.float32)
    return dict(mix_in=mix_in, mix_gain=mix_gain, query_weight=query_weight, latent_weight=latent_weight, rotary_weight=rotary_weight, latent_gain=latent_gain, key_weight=key_weight, value_weight=value_weight, output_weight=output_weight, out_gain=out_gain, ffn_in=ffn_in, ffn_gain=ffn_gain, gate_weight=gate_weight, up_weight=up_weight, down_weight=down_weight, routes=routes, route_scores=route_scores)


norm_eps = 1e-06
clamp_limit = 7.0
gate_slope = 1.702
rope_base = 10000.0

def rms_rows(rows_in, scales):
    mean_square = lax.optimization_barrier(jnp.mean(rows_in * rows_in, axis=-1, keepdims=True))
    return rows_in * lax.rsqrt(mean_square + norm_eps) * scales.astype(jnp.float32)

def angle_tables(positions):
    inverse = rope_base ** (-jnp.arange(0, ROPE, 2).astype(jnp.float32) / ROPE)
    angle_rows = positions.astype(jnp.float32)[:, None] * inverse[None, :]
    return (jnp.cos(angle_rows), jnp.sin(angle_rows))

def rotate_last(vectors, cosine, sine_rows):
    half_rope = vectors.shape[-1] // 2
    upper_half = vectors[..., :half_rope]
    lower_half = vectors[..., half_rope:]
    return jnp.concatenate([upper_half * cosine - lower_half * sine_rows, lower_half * cosine + upper_half * sine_rows], axis=-1)

def clamped_unit(gate_part, linear):
    gate_part = jnp.minimum(gate_part, clamp_limit)
    linear = jnp.clip(linear, -clamp_limit, clamp_limit)
    return gate_part * jax.nn.sigmoid(gate_slope * gate_part) * (linear + 1.0)

def rounded(vectors):
    return lax.optimization_barrier(vectors.astype(jnp.bfloat16)).astype(jnp.float32)

def mixer_half(mix_in, mix_gain, query_weight, latent_weight, rotary_weight, latent_gain, key_weight, value_weight, output_weight, out_gain):
    length = mix_in.shape[0]
    normed = rms_rows(mix_in.astype(jnp.float32), mix_gain).astype(jnp.bfloat16)
    positions = jnp.arange(length, dtype=jnp.int32)
    cosine, sine_rows = angle_tables(positions)
    queries = jnp.dot(normed, query_weight, preferred_element_type=jnp.float32).reshape(length, HEADS, NOPE + ROPE)
    query_plain = queries[..., :NOPE].astype(jnp.bfloat16)
    query_turn = rotate_last(queries[..., NOPE:], cosine[:, None, :], sine_rows[:, None, :]).astype(jnp.bfloat16)
    latent = rms_rows(jnp.dot(normed, latent_weight, preferred_element_type=jnp.float32), latent_gain).astype(jnp.bfloat16)
    rotary_key = rotate_last(jnp.dot(normed, rotary_weight, preferred_element_type=jnp.float32), cosine, sine_rows).astype(jnp.bfloat16)
    key_rows = jnp.dot(latent, key_weight, preferred_element_type=jnp.float32).astype(jnp.bfloat16)
    key_rows = key_rows.reshape(length, HEADS, NOPE).astype(jnp.float32)
    value_rows = jnp.dot(latent, value_weight, preferred_element_type=jnp.float32).astype(jnp.bfloat16)
    value_rows = value_rows.reshape(length, HEADS, VD).astype(jnp.float32)
    rotary_wide = rotary_key.astype(jnp.float32)
    score_scale = (NOPE + ROPE) ** (-0.5)
    block_rows = math.gcd(length, 256)
    block_count = length // block_rows

    def attend(block_index):
        start_row = block_index * block_rows
        plain_block = lax.dynamic_slice_in_dim(query_plain, start_row, block_rows, 0).astype(jnp.float32)
        turn_block = lax.dynamic_slice_in_dim(query_turn, start_row, block_rows, 0).astype(jnp.float32)
        scores = jnp.einsum('ihd,jhd->hij', plain_block, key_rows)
        scores = scores + jnp.einsum('ihd,jd->hij', turn_block, rotary_wide)
        query_places = start_row + jnp.arange(block_rows, dtype=jnp.int32)
        allowed = positions[None, :] <= query_places[:, None]
        weights = jnp.where(allowed[None], jnp.exp(scores * score_scale), 0.0)
        totals = lax.optimization_barrier(jnp.sum(weights, axis=-1))
        weighted = jnp.einsum('hij,jhd->hid', rounded(weights), value_rows)
        return (weighted / totals[..., None]).astype(jnp.bfloat16)
    attended = lax.map(attend, jnp.arange(block_count))
    attended = attended.transpose(0, 2, 1, 3).reshape(length, HEADS, VD)
    group_heads = HEADS // N_TP
    projected = jnp.zeros((length, D), jnp.float32)
    for group in range(N_TP):
        head_block = attended[:, group * group_heads:(group + 1) * group_heads, :].reshape(length, group_heads * VD)
        weight_rows = output_weight[group * group_heads * VD:(group + 1) * group_heads * VD]
        projected = projected + rounded(jnp.dot(head_block, weight_rows, preferred_element_type=jnp.float32))
    return rms_rows(projected, out_gain).astype(jnp.bfloat16)

def expert_half(ffn_in, ffn_gain, gate_weight, up_weight, down_weight, routes, route_scores):
    row_count = ffn_in.shape[0]
    normed = rms_rows(ffn_in.astype(jnp.float32), ffn_gain).astype(jnp.bfloat16)
    padded = jnp.concatenate([normed, jnp.zeros((1, D), jnp.bfloat16)], axis=0)
    gate_share = jax.nn.softmax(route_scores.astype(jnp.float32), axis=-1).reshape(-1)
    gate_share = jnp.concatenate([gate_share, jnp.zeros((1,), jnp.float32)], axis=0)
    flat_routes = routes.reshape(-1)
    assignment_count = flat_routes.shape[0]
    capacity_all = MOST * (row_count // QB)
    unit_group = FF // N_TP

    def one_expert(totals, expert):
        matches = flat_routes == expert
        slot_rank = jnp.cumsum(matches.astype(jnp.int32)) - 1
        destination = jnp.where(matches, slot_rank, capacity_all).astype(jnp.int32)
        slot_of = jnp.full((capacity_all + 1,), assignment_count, jnp.int32)
        slot_of = slot_of.at[destination].set(jnp.arange(assignment_count, dtype=jnp.int32))[:capacity_all]
        token_of = slot_of // TOP
        gathered = padded[token_of]
        gate_part = jnp.dot(gathered, gate_weight[expert], preferred_element_type=jnp.float32)
        up_part = jnp.dot(gathered, up_weight[expert], preferred_element_type=jnp.float32)
        hidden = clamped_unit(gate_part, up_part).astype(jnp.bfloat16)
        expert_sum = jnp.zeros((capacity_all, D), jnp.float32)
        for group in range(N_TP):
            expert_sum = expert_sum + rounded(jnp.dot(hidden[:, group * unit_group:(group + 1) * unit_group], down_weight[expert][group * unit_group:(group + 1) * unit_group], preferred_element_type=jnp.float32))
        weighted = rounded(expert_sum) * gate_share[slot_of][:, None]
        totals = totals.at[token_of].add(weighted, mode='drop')
        return (totals, None)
    totals, _ = lax.scan(one_expert, jnp.zeros((row_count, D), jnp.float32), jnp.arange(EXPERTS, dtype=jnp.int32))
    return totals.astype(jnp.bfloat16)

def reference(mix_in, mix_gain, query_weight, latent_weight, rotary_weight, latent_gain, key_weight, value_weight, output_weight, out_gain, ffn_in, ffn_gain, gate_weight, up_weight, down_weight, routes, route_scores):
    mixed = mixer_half(mix_in, mix_gain, query_weight, latent_weight, rotary_weight, latent_gain, key_weight, value_weight, output_weight, out_gain)
    moe_out = expert_half(ffn_in, ffn_gain, gate_weight, up_weight, down_weight, routes, route_scores)
    return (mixed, moe_out)
```

```python
import jax
import jax.numpy as jnp
import functools
import numpy as np
from jax import lax
from jax.experimental import pallas as pl
from jax.experimental.pallas import tpu as pltpu
from jax.sharding import PartitionSpec as P

NOPE = 128
ROPE = 64
VD = 128


norm_eps = 1e-06
clamp_limit = 7.0
gate_slope = 1.702
rope_base = 10000.0


def rms_rows(rows_in, scales):
    mean_square = jnp.mean(rows_in * rows_in, axis=-1, keepdims=True)
    return rows_in * lax.rsqrt(mean_square + norm_eps) * scales


def rms_columns(columns, scales):
    mean_square = jnp.mean(columns * columns, axis=0, keepdims=True)
    return columns * lax.rsqrt(mean_square + norm_eps) * scales[:, None]


def turn_table(positions):
    inverse = rope_base ** (-jnp.arange(0, ROPE, 2).astype(jnp.float32) / ROPE)
    angle_rows = inverse[:, None] * positions.astype(jnp.float32)[None, :]
    return (jnp.cos(angle_rows), jnp.sin(angle_rows))


def clamped_unit(gate_part, linear):
    gate_part = jnp.minimum(gate_part, clamp_limit)
    linear = jnp.clip(linear, -clamp_limit, clamp_limit)
    return gate_part * jax.nn.sigmoid(gate_slope * gate_part) * (linear + 1.0)


def keep_state(running):
    return running


def local(
    mix_in,
    mix_gain,
    query_weight,
    latent_weight,
    rotary_weight,
    latent_gain,
    key_weight,
    value_weight,
    output_weight,
    out_gain,
    ffn_in,
    ffn_gain,
    gate_weight,
    up_weight,
    down_weight,
    routes,
    route_scores,
):
    row_count = mix_in.shape[0]
    first_row = lax.axis_index("ep") * row_count
    last_row = first_row + row_count - 1
    positions = first_row + jnp.arange(row_count, dtype=jnp.int32)
    normed = rms_rows(mix_in.astype(jnp.float32), mix_gain).astype(jnp.bfloat16)
    head_count = query_weight.shape[1] // (NOPE + ROPE)
    half_rope = ROPE // 2
    cosine, sine_rows = turn_table(positions)
    queries = jnp.dot(normed, query_weight, preferred_element_type=jnp.float32).reshape(
        row_count, head_count, NOPE + ROPE
    )
    query_plain = queries[..., :NOPE].astype(jnp.bfloat16)
    query_cos = cosine.T[:, None, :]
    query_sin = sine_rows.T[:, None, :]
    query_upper = queries[..., NOPE : NOPE + half_rope]
    query_lower = queries[..., NOPE + half_rope :]
    query_turn = jnp.concatenate(
        [
            query_upper * query_cos - query_lower * query_sin,
            query_lower * query_cos + query_upper * query_sin,
        ],
        axis=-1,
    ).astype(jnp.bfloat16)
    across = (((0,), (1,)), ((), ()))
    latent = rms_columns(
        lax.dot_general(latent_weight, normed, across, preferred_element_type=jnp.float32),
        latent_gain,
    ).astype(jnp.bfloat16)
    rot_raw = lax.dot_general(rotary_weight, normed, across, preferred_element_type=jnp.float32)
    rotary_key = jnp.concatenate(
        [
            rot_raw[:half_rope] * cosine - rot_raw[half_rope:] * sine_rows,
            rot_raw[half_rope:] * cosine + rot_raw[:half_rope] * sine_rows,
        ],
        axis=0,
    ).astype(jnp.bfloat16)
    score_scale = (NOPE + ROPE) ** (-0.5)
    contract_first = (((0,), (0,)), ((), ()))

    def expand(latent_block):
        key_block = lax.dot_general(
            key_weight, latent_block, contract_first, preferred_element_type=jnp.float32
        ).astype(jnp.bfloat16)
        value_block = lax.dot_general(
            value_weight, latent_block, contract_first, preferred_element_type=jnp.float32
        ).astype(jnp.bfloat16)
        return (key_block, value_block)

    def attend(key_block, value_block, turn_block):
        key_count = key_block.shape[1]
        key_block = key_block.reshape(head_count, NOPE, key_count)
        value_block = value_block.reshape(head_count, VD, key_count)
        scores = jnp.einsum(
            "ihd,hdj->hij", query_plain, key_block, preferred_element_type=jnp.float32
        )
        scores = scores + jnp.einsum(
            "ihd,dj->hij", query_turn, turn_block, preferred_element_type=jnp.float32
        )
        key_places = jnp.arange(key_count, dtype=jnp.int32)
        allowed = key_places[None, :] <= positions[:, None]
        weights = jnp.where(allowed[None], jnp.exp(scores * score_scale), 0.0)
        weighted = jnp.einsum(
            "hij,hdj->hid",
            weights.astype(jnp.bfloat16),
            value_block,
            preferred_element_type=jnp.float32,
        )
        return (jnp.sum(weights, axis=-1), weighted)

    initial = (
        jnp.zeros((head_count, row_count), jnp.float32),
        jnp.zeros((head_count, row_count, VD), jnp.float32),
    )
    shard_piece = (
        lax.all_gather(latent, "ep", axis=1, tiled=True),
        lax.all_gather(rotary_key, "ep", axis=1, tiled=True),
    )

    def compute_piece(running):
        key_block, value_block = expand(shard_piece[0])
        return attend(key_block, value_block, shard_piece[1])

    totals, weighted = lax.cond(jnp.int32(0) > last_row, keep_state, compute_piece, initial)
    attended = (weighted / totals[..., None]).astype(jnp.bfloat16)
    mixing = output_weight.reshape(head_count, VD, output_weight.shape[1])
    partial_value = jnp.einsum("hid,hde->ie", attended, mixing, preferred_element_type=jnp.float32)
    projected = lax.psum_scatter(
        lax.optimization_barrier(partial_value.astype(jnp.bfloat16))
        .astype(jnp.float32)
        .astype(jnp.bfloat16),
        "tp",
        scatter_dimension=0,
        tiled=True,
    ).astype(jnp.float32)
    mixed = rms_rows(projected, out_gain).astype(jnp.bfloat16)
    tokens = ffn_in.shape[0]
    part_count = lax.axis_size("tp")
    quarter_rows = tokens // part_count
    experts = lax.axis_size("ep")
    choose = routes.shape[1]
    capacity = max(2, 2 * quarter_rows * choose // experts)
    slot_count = capacity * part_count
    tp_index = lax.axis_index("tp")
    normed_b = rms_rows(ffn_in.astype(jnp.float32), ffn_gain).astype(jnp.bfloat16)
    padded = jnp.concatenate([normed_b, jnp.zeros((1, normed_b.shape[1]), jnp.bfloat16)], axis=0)
    gate_share = jax.nn.softmax(route_scores, axis=-1)
    grouped = routes.reshape(part_count, quarter_rows * choose)
    onehot = (grouped[:, :, None] == jnp.arange(experts, dtype=jnp.int32)[None, None, :]).astype(
        jnp.int32
    )
    slot_rank = jnp.sum((jnp.cumsum(onehot, axis=1) - 1) * onehot, axis=2)
    slot_index = jnp.arange(part_count, dtype=jnp.int32)[:, None] * capacity + slot_rank
    place_index = (slot_index * experts + grouped).reshape(-1)
    owners = jnp.arange(tokens * choose, dtype=jnp.int32) // choose
    slot_token = jnp.full((slot_count * experts,), tokens, jnp.int32).at[place_index].set(owners)
    unit_count = gate_weight.shape[2]
    chosen = lax.dynamic_slice_in_dim(
        slot_token, tp_index * capacity * experts, capacity * experts, 0
    )
    outgoing = padded[chosen].reshape(capacity, experts, -1)
    arrived = lax.all_to_all(outgoing, "ep", split_axis=1, concat_axis=1, tiled=True)
    row_block = lax.all_gather(arrived, "tp", axis=0, tiled=True)
    block_slots = row_block.shape[0]
    flat_rows = row_block.reshape(-1, row_block.shape[2])
    gate_part = jnp.dot(flat_rows, gate_weight[0], preferred_element_type=jnp.float32)
    up_part = jnp.dot(flat_rows, up_weight[0], preferred_element_type=jnp.float32)
    hidden = (
        clamped_unit(gate_part, up_part).astype(jnp.bfloat16).reshape(block_slots, -1, unit_count)
    )
    sources = hidden.shape[1]
    hidden_flat = hidden.reshape(slot_count * sources, unit_count)
    partial_value = jnp.dot(hidden_flat, down_weight[0], preferred_element_type=jnp.float32)
    result = lax.psum_scatter(
        lax.optimization_barrier(partial_value.astype(jnp.bfloat16))
        .astype(jnp.float32)
        .astype(jnp.bfloat16),
        "tp",
        scatter_dimension=0,
        tiled=True,
    )
    result = result.reshape(capacity, sources, -1)
    returned = lax.all_to_all(result, "ep", split_axis=1, concat_axis=1, tiled=True)
    back_rows = returned.reshape(capacity * experts, -1)
    own_rank = lax.dynamic_index_in_dim(slot_rank, tp_index, 0, keepdims=False)
    own_expert = lax.dynamic_index_in_dim(grouped, tp_index, 0, keepdims=False)
    picked = (
        back_rows[own_rank * experts + own_expert]
        .astype(jnp.float32)
        .reshape(quarter_rows, choose, -1)
    )
    own_gates = lax.dynamic_slice_in_dim(gate_share, tp_index * quarter_rows, quarter_rows, 0)
    moe_out = jnp.sum(picked * own_gates[:, :, None], axis=1).astype(jnp.bfloat16)
    return (mixed, moe_out)


MESH = pl.DeviceIdType.MESH


def flip(value, bits):
    bit = 1
    while bit <= bits:
        if bits & bit:
            value = value + bit - 2 * bit * ((value // bit) % 2)
        bit *= 2
    return value


def here():
    ep, tp = lax.axis_index("ep"), lax.axis_index("tp")
    return ep // 2, ep % 2, tp // 2, tp % 2


def place(z, x, y, core):
    return {"ep": z * 2 + x, "tp": y * 2 + core}


def greet(partners):
    barrier = pltpu.get_barrier_semaphore()
    for partner in partners:
        pl.semaphore_signal(barrier, inc=1, device_id=partner, device_id_type=MESH)
    pl.semaphore_wait(barrier, len(partners))


def layer_kernel(
    depth, heads, side_width,
    ffn_hbm, mix_hbm, ffn_gain_hbm, mix_gain_hbm, latent_gain_hbm, out_gain_hbm, routes_hbm, scores_hbm,
    base_hbm, step_hbm, latent_hbm, rotary_hbm, query_hbm, gate_hbm, up_hbm, down_hbm, key_hbm,
    value_hbm, output_hbm, mixed_ref, moe_ref,
    row_ref, side_ref, query_ref,
    rows_all, side_all, part_ref, work, twin_in, hop_in, direct_in, relay_in, column_in,
    heads_ref, heads_work, heads_twin, heads_in, keys, values, attended, own_total, table_ref, turn_ref,
    ffn_ref, mix_ref, ffn_gain, mix_gain, latent_gain, gain_ref, routes_ref, scores_ref,
    base_ref, step_ref, latent_ref, rotary_ref, query_w, gate_ref, up_ref, down_ref, key_ref, value_ref, output_ref,
    spread_sem, recv_sem, send_sem, twin_sem, square_sem, column_sem, heads_sem, load_sem,
):
    f32, bf16 = jnp.float32, jnp.bfloat16
    ep, tp = lax.axis_index("ep"), lax.axis_index("tp")
    z, x, y, core = here()
    x_next, y_next, twin = place(z, 1 - x, y, core), place(z, x, 1 - y, core), place(z, x, y, 1 - core)
    columns = [place(flip(z, d), x, y, core) for d in range(1, depth)]
    parts, quarter, width = part_ref.shape[1:]
    row_count = parts * quarter
    latent_width = key_ref.shape[0]
    experts = 2 * depth
    half = ROPE // 2
    first_own = pl.multiple_of(tp * quarter, quarter)
    pairs = (
        (ffn_hbm.at[pl.ds(first_own, quarter)], ffn_ref), (ffn_gain_hbm, ffn_gain),
        (mix_hbm, mix_ref), (mix_gain_hbm, mix_gain), (latent_hbm, latent_ref), (rotary_hbm, rotary_ref),
        (latent_gain_hbm, latent_gain), (base_hbm, base_ref), (step_hbm, step_ref),
        (routes_hbm, routes_ref), (scores_hbm, scores_ref), (query_hbm, query_w),
        (gate_hbm, gate_ref), (up_hbm, up_ref), (down_hbm, down_ref),
        (key_hbm, key_ref), (value_hbm, value_ref), (output_hbm, output_ref), (out_gain_hbm, gain_ref),
    )
    loads = [pltpu.make_async_copy(src, dst, load_sem.at[n]) for n, (src, dst) in enumerate(pairs)]
    for load in loads:
        load.start()
    waited = [0]

    def loaded(count):
        while waited[0] < count:
            loads[waited[0]].wait()
            waited[0] += 1

    greet(columns + [x_next, y_next, twin])
    spread, started = [], []

    def copies(origin, target, own):
        e, t = origin["ep"], origin["tp"]
        number = len(spread)
        return [
            pltpu.make_async_remote_copy(
                src_ref=held if own else out.at[e, t],
                dst_ref=out.at[e, t],
                send_sem=spread_sem.at[a, number],
                recv_sem=recv_sem.at[a, e, t],
                device_id=target,
                device_id_type=MESH,
            )
            for a, (held, out) in enumerate(((row_ref, rows_all), (side_ref, side_all)))
        ]

    def give(origin, target):
        pair = copies(origin, target, False)
        for copy in pair:
            copy.start()
        spread.append(pair)

    def take(origin):
        for copy in copies(origin, twin, False):
            copy.wait_recv()

    def make(src, dst, sem, target):
        return pltpu.make_async_remote_copy(
            src_ref=src, dst_ref=dst, send_sem=send_sem.at[len(started)], recv_sem=sem,
            device_id=target, device_id_type=MESH,
        )

    def send(src, dst, sem, target):
        copy = make(src, dst, sem, target)
        copy.start()
        started.append(copy)

    def arrive(dst, sem):
        make(dst, dst, sem, twin).wait_recv()

    def forward_column(d):
        origin = place(flip(z, d), x, y, core)
        take(origin)
        for target in (x_next, y_next, twin):
            give(origin, target)

    def forward_square(d):
        at = flip(z, d)
        from_x, from_y = place(at, 1 - x, y, core), place(at, x, 1 - y, core)
        take(from_x)
        if d % 2 == 0:
            give(from_x, y_next)
        give(from_x, twin)
        take(from_y)
        if d % 2 == 1:
            give(from_y, x_next)
        give(from_y, twin)

    def forward_corner(d):
        origin = place(flip(z, d), 1 - x, 1 - y, core)
        take(origin)
        give(origin, twin)

    def side_block(e):
        return side_all[e].reshape(row_count, side_width)

    def expert_plane(d):
        for a in (0, 1):
            for b in (0, 1):
                take(place(flip(z, d), flip(x, a), flip(y, b), 1 - core))
        first = flip(z, d) * 2
        pair = pl.ds(first, 2)
        block = rows_all[pair].reshape(2 * row_count, width)
        gate_part = jnp.dot(block, gate_ref[...], preferred_element_type=f32)
        up_part = jnp.dot(block, up_ref[...], preferred_element_type=f32)
        hidden = clamped_unit(gate_part, up_part).astype(bf16)
        table = side_all[pair, :, :, latent_width:].reshape(2 * row_count, side_width - latent_width)
        lane = lax.broadcasted_iota(jnp.int32, table.shape, 1)
        is_mine = (lane == ROPE + ep) | (lane == ROPE + experts + ep)
        share = jnp.sum(jnp.where(is_mine, table.astype(f32), 0.0), axis=1, keepdims=True)
        chunk = 512
        for n in range(0, width, chunk):
            piece = jnp.dot(hidden, down_ref[:, n : n + chunk], preferred_element_type=f32) * share
            part_ref[pair, :, :, n : n + chunk] = piece.astype(bf16).reshape(2, parts, quarter, chunk)
        for a, b in ((1, 1), (1, 0), (0, 1), (0, 0)):
            e, t = flip(z, d) * 2 + flip(x, a), flip(y, b) * 2 + 1 - core
            send(part_ref.at[e, t], twin_in.at[d, a, b], twin_sem.at[d, a, b], twin)

    def paired(d, a, b):
        arrive(twin_in.at[d, a, b], twin_sem.at[d, a, b])
        own = part_ref[flip(z, d) * 2 + flip(x, a), flip(y, b) * 2 + core]
        return own.astype(f32) + twin_in[d, a, b].astype(f32)

    def sum_pairs(d):
        work[d, 1, 1] = paired(d, 1, 1).astype(bf16)
        send(work.at[d, 1, 1], hop_in.at[d], square_sem.at[0, d], y_next if d % 2 else x_next)
        a, b = (0, 1) if d % 2 else (1, 0)
        work[d, a, b] = paired(d, a, b).astype(bf16)
        send(work.at[d, a, b], direct_in.at[d], square_sem.at[1, d], y_next if d % 2 else x_next)

    def sum_relay(d):
        a, b = (1, 0) if d % 2 else (0, 1)
        value = paired(d, a, b)
        arrive(hop_in.at[d], square_sem.at[0, d])
        work[d, a, b] = (value + hop_in[d].astype(f32)).astype(bf16)
        send(work.at[d, a, b], relay_in.at[d], square_sem.at[2, d], x_next if d % 2 else y_next)

    def sum_square(d):
        value = paired(d, 0, 0)
        arrive(direct_in.at[d], square_sem.at[1, d])
        value = value + direct_in[d].astype(f32)
        arrive(relay_in.at[d], square_sem.at[2, d])
        value = value + relay_in[d].astype(f32)
        if d:
            work[d, 0, 0] = value.astype(bf16)
            send(work.at[d, 0, 0], column_in.at[d], column_sem.at[d], columns[d - 1])
        else:
            own_total[...] = value

    across = (((1,), (1,)), ((), ()))
    score_scale = (NOPE + ROPE) ** (-0.5)

    def angles():
        near, far = base_ref[...], step_ref[pl.ds(ep, 1), :]
        swapped = pltpu.roll(near, ROPE, 1)
        lane = lax.broadcasted_iota(jnp.int32, near.shape, 1)
        cosine, sine = jnp.where(lane < ROPE, near, swapped), jnp.where(lane < ROPE, swapped, near)
        far_swapped = pltpu.roll(jnp.broadcast_to(far, near.shape), ROPE, 1)
        far = jnp.broadcast_to(far, near.shape)
        far_cos, far_sin = jnp.where(lane < ROPE, far, far_swapped), jnp.where(lane < ROPE, far_swapped, far)
        turn_ref[...] = jnp.where(
            lane < ROPE, cosine * far_cos - sine * far_sin, sine * far_cos + cosine * far_sin
        )

    def rotate(vectors, table):
        lane = lax.broadcasted_iota(jnp.int32, vectors.shape, 1)
        size = vectors.shape[1]
        turned = jnp.where(
            lane < half, -pltpu.roll(vectors, size - half, 1), pltpu.roll(vectors, half, 1)
        )
        sine = pltpu.roll(table, size - ROPE, 1)
        return jnp.where(lane < ROPE, vectors * table + turned * sine, 0.0)

    def prepare_rows():
        loaded(2)
        row_ref[...] = rms_rows(ffn_ref[...].astype(f32), ffn_gain[...]).astype(bf16)

    def prepare_side():
        loaded(11)
        own = pl.ds(first_own, quarter)
        normed = rms_rows(mix_ref[own, :].astype(f32), mix_gain[...]).astype(bf16)
        latent = jnp.dot(normed, latent_ref[...], preferred_element_type=f32)
        side_ref[:, :latent_width] = rms_rows(latent, latent_gain[...]).astype(bf16)
        angles()
        turned = lax.dot_general(normed, rotary_ref[...], across, preferred_element_type=f32)
        spare = side_width - latent_width - ROPE
        turned = jnp.concatenate([turned, jnp.zeros((quarter, spare), f32)], axis=1)
        rotary_key = rotate(turned, turn_ref[own, :])
        scores = scores_ref[...]
        shares = jnp.exp(scores - jnp.max(scores, axis=0, keepdims=True))
        shares = shares / jnp.sum(shares, axis=0, keepdims=True)
        routes = routes_ref[...]
        lane = lax.broadcasted_iota(jnp.int32, (side_width - latent_width, row_count), 0)
        named = jnp.zeros((side_width - latent_width, row_count), f32)
        for k in range(routes.shape[0]):
            hit = (lane == routes[k : k + 1] + ROPE) | (lane == routes[k : k + 1] + ROPE + experts)
            named = named + jnp.where(hit, shares[k : k + 1], 0.0)
        coarse = named.astype(bf16).astype(f32)
        table_ref[...] = jnp.where(lane < ROPE + experts, coarse, named - coarse).T
        side_ref[:, latent_width:] = (rotary_key + table_ref[own, :]).astype(bf16)

    def prepare_queries():
        loaded(12)
        normed = rms_rows(mix_ref[...].astype(f32), mix_gain[...]).astype(bf16)
        plain_and_turn = NOPE + ROPE
        for h in range(0, heads, 2):
            columns_of = slice(h * plain_and_turn, (h + 2) * plain_and_turn)
            two = jnp.dot(normed, query_w[:, columns_of], preferred_element_type=f32)
            table = turn_ref[...]
            middle = two[:, NOPE : 2 * NOPE]
            query_ref[h, :, :NOPE] = two[:, :NOPE].astype(bf16)
            query_ref[h, :, NOPE:] = rotate(middle, table).astype(bf16)
            last = two[:, 2 * NOPE :]
            lane = lax.broadcasted_iota(jnp.int32, last.shape, 1)
            low, high = pltpu.roll(middle, ROPE, 1), pltpu.roll(last, ROPE, 1)
            query_ref[h + 1, :, :NOPE] = jnp.where(lane < ROPE, low, high).astype(bf16)
            query_ref[h + 1, :, NOPE:] = rotate(high, table).astype(bf16)

    def expand():
        @pl.loop(0, depth)
        def _(d):
            block = side_all[pl.ds(2 * d, 2)].reshape(2 * row_count, side_width)
            latent, rest = block[:, :latent_width], block[:, latent_width:]
            at = pl.ds(pl.multiple_of(2 * d * row_count, 2 * row_count), 2 * row_count)
            key_block = jnp.dot(latent, key_ref[...], preferred_element_type=f32).astype(bf16)
            value_block = jnp.dot(latent, value_ref[...], preferred_element_type=f32).astype(bf16)
            for h in range(heads):
                keys[h, at, :NOPE] = key_block[:, h * NOPE : (h + 1) * NOPE]
                keys[h, at, NOPE:] = rest
                values[h, at, :] = value_block[:, h * VD : (h + 1) * VD]

    def attend(h):
        tokens = experts * row_count
        chunk = 256
        totals = jnp.zeros((row_count, 1), f32)
        weighted = jnp.zeros((row_count, VD), f32)
        places = lax.broadcasted_iota(jnp.int32, (row_count, chunk), 0) + ep * row_count
        for n in range(0, tokens, chunk):
            scores = lax.dot_general(
                query_ref[h], keys[h, n : n + chunk, :], across, preferred_element_type=f32
            )
            allowed = lax.broadcasted_iota(jnp.int32, (row_count, chunk), 1) + n <= places
            weights = jnp.where(allowed, jnp.exp(scores * score_scale), 0.0)
            totals = totals + jnp.sum(weights, axis=1, keepdims=True)
            weighted = weighted + jnp.dot(
                weights.astype(bf16), values[h, n : n + chunk, :], preferred_element_type=f32
            )
        attended[:, h * VD : (h + 1) * VD] = (weighted / totals).astype(bf16)

    def project():
        chunk = 512
        for n in range(0, width, chunk):
            piece = jnp.dot(attended[...], output_ref[:, n : n + chunk], preferred_element_type=f32)
            heads_ref[:, :, n : n + chunk] = piece.astype(bf16).reshape(parts, quarter, chunk)
        for b in (1, 0):
            send(heads_ref.at[flip(y, b) * 2 + 1 - core], heads_twin.at[b], heads_sem.at[b], twin)

    me = place(z, x, y, core)
    targets = columns + [x_next, y_next, twin]
    prepare_rows()
    for target in targets:
        pair = copies(me, target, True)
        pair[0].start()
        spread.append(pair)
    rows_all[me["ep"], me["tp"]] = row_ref[...]
    prepare_side()
    for pair in spread:
        pair[1].start()
    side_all[me["ep"], me["tp"]] = side_ref[...]
    prepare_queries()

    def reduce_after(last):
        for step, back in ((sum_pairs, 0), (sum_relay, 1), (sum_square, 2)):
            if 0 <= last - back < depth:
                step(last - back)

    for d in range(1, depth + 3):
        if d < depth:
            forward_column(d)
        if d - 1 < depth:
            forward_square(d - 1)
        if 0 <= d - 2 < depth:
            forward_corner(d - 2)
        if 0 <= d - 3 < depth:
            loaded(15)
            expert_plane(d - 3)
        if 0 <= d - 4:
            reduce_after(d - 4)
    loaded(len(loads))
    expand()
    reduce_after(depth - 1)
    for h in range(heads):
        attend(h)
        if h % 2 == 0 and h < 4:
            reduce_after(depth + h // 2)
    for h in range((heads + 1) // 2, 2):
        reduce_after(depth + h)
    project()
    arrive(heads_twin.at[1], heads_sem.at[1])
    heads_work[...] = (
        heads_ref[(1 - y) * 2 + core].astype(f32) + heads_twin[1].astype(f32)
    ).astype(bf16)
    send(heads_work, heads_in, heads_sem.at[2], y_next)
    total = own_total[...]
    for d in range(1, depth):
        arrive(column_in.at[d], column_sem.at[d])
        total = total + column_in[d].astype(f32)
    moe_ref[...] = total.astype(bf16)
    arrive(heads_twin.at[0], heads_sem.at[0])
    arrive(heads_in, heads_sem.at[2])
    projected = (
        heads_ref[y * 2 + core].astype(f32) + heads_twin[0].astype(f32) + heads_in[...].astype(f32)
    )
    mixed_ref[...] = rms_rows(projected, gain_ref[...]).astype(bf16)
    for copy in started:
        copy.wait_send()
    for pair in spread:
        for copy in pair:
            copy.wait_send()


def turn_tables(row_count, experts):
    inverse = rope_base ** (-np.arange(0, ROPE, 2) / ROPE)
    near, far = np.arange(row_count)[:, None] * inverse, row_count * np.arange(experts)[:, None] * inverse

    def lanes(angle):
        return np.concatenate([np.cos(angle)] * 2 + [np.sin(angle)] * 2, axis=1).astype(np.float32)

    return lanes(near), lanes(far)


def dense_local(
    mix_in, mix_gain, query_weight, latent_weight, rotary_weight, latent_gain, key_weight,
    value_weight, output_weight, out_gain, ffn_in, ffn_gain, gate_weight, up_weight, down_weight,
    routes, route_scores,
):
    experts, parts = lax.axis_size("ep"), lax.axis_size("tp")
    row_count, width = mix_in.shape
    quarter, depth = row_count // parts, experts // 2
    tokens = experts * row_count
    latent_width = latent_weight.shape[1]
    heads = query_weight.shape[1] // (NOPE + ROPE)
    side_width = latent_width + 2 * ROPE
    base, step = turn_tables(row_count, experts)
    row = lambda gain: gain.reshape(1, -1)
    operands = (
        ffn_in, mix_in, row(ffn_gain), row(mix_gain), row(latent_gain), row(out_gain), routes.T,
        route_scores.T, jnp.asarray(base), jnp.asarray(step), latent_weight, rotary_weight.T, query_weight,
        gate_weight[0], up_weight[0], down_weight[0], key_weight, value_weight, output_weight,
    )
    held = lambda *lead: pltpu.VMEM(lead + (quarter, width), jnp.bfloat16)
    scratch = lambda *shape: pltpu.VMEM(shape, jnp.bfloat16)
    sems = lambda *shape: pltpu.SemaphoreType.DMA(shape)
    gives = depth + 2 + 3 * (depth - 1) + 3 * depth + depth
    return pl.pallas_call(
        functools.partial(layer_kernel, depth, heads, side_width),
        out_shape=[jax.ShapeDtypeStruct((quarter, width), jnp.bfloat16)] * 2,
        in_specs=[pl.BlockSpec(memory_space=pl.ANY)] * len(operands),
        out_specs=[pl.BlockSpec(memory_space=pltpu.VMEM)] * 2,
        scratch_shapes=[
            held(), scratch(quarter, side_width), scratch(heads, row_count, NOPE + 2 * ROPE),
            held(experts, parts), scratch(experts, parts, quarter, side_width),
            held(experts, parts), held(depth, 2, 2), held(depth, 2, 2),
            held(depth), held(depth), held(depth), held(depth),
            held(parts), held(), held(2), held(),
            scratch(heads, tokens, NOPE + 2 * ROPE), scratch(heads, tokens, VD),
            scratch(row_count, heads * VD), pltpu.VMEM((quarter, width), jnp.float32),
            pltpu.VMEM((row_count, 2 * ROPE), jnp.float32), pltpu.VMEM((row_count, 2 * ROPE), jnp.float32),
            pltpu.VMEM((quarter, width), ffn_in.dtype), pltpu.VMEM(mix_in.shape, mix_in.dtype),
        ]
        + [pltpu.VMEM(a.shape, a.dtype) for a in operands[2:]]
        + [
            sems(2, gives + 1), sems(2, experts, parts), sems(3 + 8 * depth), sems(depth, 2, 2),
            sems(3, depth), sems(depth), sems(3), sems(len(operands)),
        ],
        compiler_params=pltpu.CompilerParams(
            collective_id=0, has_side_effects=True, vmem_limit_bytes=60 * 1024 * 1024
        ),
        name="layer",
    )(*operands)


def solution(mesh):
    experts, parts = mesh.shape["ep"], mesh.shape["tp"]

    def body(*args):
        quarter, choose = args[10].shape[0] // parts, args[15].shape[1]
        every_row = 2 * quarter * choose >= quarter * experts
        paired = parts == 4 and experts % 2 == 0 and (experts // 2) & (experts // 2 - 1) == 0
        return (dense_local if every_row and paired else local)(*args)
    placed = (
        P("ep", None),
        P(),
        P(None, "tp"),
        P(),
        P(),
        P(),
        P(None, "tp"),
        P(None, "tp"),
        P("tp", None),
        P(),
        P("ep", None),
        P(),
        P("ep", None, "tp"),
        P("ep", None, "tp"),
        P("ep", "tp", None),
        P("ep", None),
        P("ep", None),
    )
    return jax.shard_map(
        body,
        mesh=mesh,
        in_specs=placed,
        out_specs=(P(("ep", "tp"), None), P(("ep", "tp"), None)),
        check_vma=False,
    )
```

```python
import jax
import jax.numpy as jnp
import functools
import numpy as np
from jax import lax
from jax.experimental import pallas as pl
from jax.experimental.pallas import tpu as pltpu
from jax.sharding import PartitionSpec as P

NOPE = 128
ROPE = 64
VD = 128


norm_eps = 1e-06
clamp_limit = 7.0
gate_slope = 1.702
rope_base = 10000.0


def rms_rows(rows_in, scales):
    mean_square = jnp.mean(rows_in * rows_in, axis=-1, keepdims=True)
    return rows_in * lax.rsqrt(mean_square + norm_eps) * scales


def rms_columns(columns, scales):
    mean_square = jnp.mean(columns * columns, axis=0, keepdims=True)
    return columns * lax.rsqrt(mean_square + norm_eps) * scales[:, None]


def turn_table(positions):
    inverse = rope_base ** (-jnp.arange(0, ROPE, 2).astype(jnp.float32) / ROPE)
    angle_rows = inverse[:, None] * positions.astype(jnp.float32)[None, :]
    return (jnp.cos(angle_rows), jnp.sin(angle_rows))


def clamped_unit(gate_part, linear):
    gate_part = jnp.minimum(gate_part, clamp_limit)
    linear = jnp.clip(linear, -clamp_limit, clamp_limit)
    return gate_part * jax.nn.sigmoid(gate_slope * gate_part) * (linear + 1.0)


def keep_state(running):
    return running


def local(
    mix_in,
    mix_gain,
    query_weight,
    latent_weight,
    rotary_weight,
    latent_gain,
    key_weight,
    value_weight,
    output_weight,
    out_gain,
    ffn_in,
    ffn_gain,
    gate_weight,
    up_weight,
    down_weight,
    routes,
    route_scores,
):
    row_count = mix_in.shape[0]
    first_row = lax.axis_index("ep") * row_count
    last_row = first_row + row_count - 1
    positions = first_row + jnp.arange(row_count, dtype=jnp.int32)
    normed = rms_rows(mix_in.astype(jnp.float32), mix_gain).astype(jnp.bfloat16)
    head_count = query_weight.shape[1] // (NOPE + ROPE)
    half_rope = ROPE // 2
    cosine, sine_rows = turn_table(positions)
    queries = jnp.dot(normed, query_weight, preferred_element_type=jnp.float32).reshape(
        row_count, head_count, NOPE + ROPE
    )
    query_plain = queries[..., :NOPE].astype(jnp.bfloat16)
    query_cos = cosine.T[:, None, :]
    query_sin = sine_rows.T[:, None, :]
    query_upper = queries[..., NOPE : NOPE + half_rope]
    query_lower = queries[..., NOPE + half_rope :]
    query_turn = jnp.concatenate(
        [
            query_upper * query_cos - query_lower * query_sin,
            query_lower * query_cos + query_upper * query_sin,
        ],
        axis=-1,
    ).astype(jnp.bfloat16)
    across = (((0,), (1,)), ((), ()))
    latent = rms_columns(
        lax.dot_general(latent_weight, normed, across, preferred_element_type=jnp.float32),
        latent_gain,
    ).astype(jnp.bfloat16)
    rot_raw = lax.dot_general(rotary_weight, normed, across, preferred_element_type=jnp.float32)
    rotary_key = jnp.concatenate(
        [
            rot_raw[:half_rope] * cosine - rot_raw[half_rope:] * sine_rows,
            rot_raw[half_rope:] * cosine + rot_raw[:half_rope] * sine_rows,
        ],
        axis=0,
    ).astype(jnp.bfloat16)
    score_scale = (NOPE + ROPE) ** (-0.5)
    contract_first = (((0,), (0,)), ((), ()))

    def expand(latent_block):
        key_block = lax.dot_general(
            key_weight, latent_block, contract_first, preferred_element_type=jnp.float32
        ).astype(jnp.bfloat16)
        value_block = lax.dot_general(
            value_weight, latent_block, contract_first, preferred_element_type=jnp.float32
        ).astype(jnp.bfloat16)
        return (key_block, value_block)

    def attend(key_block, value_block, turn_block):
        key_count = key_block.shape[1]
        key_block = key_block.reshape(head_count, NOPE, key_count)
        value_block = value_block.reshape(head_count, VD, key_count)
        scores = jnp.einsum(
            "ihd,hdj->hij", query_plain, key_block, preferred_element_type=jnp.float32
        )
        scores = scores + jnp.einsum(
            "ihd,dj->hij", query_turn, turn_block, preferred_element_type=jnp.float32
        )
        key_places = jnp.arange(key_count, dtype=jnp.int32)
        allowed = key_places[None, :] <= positions[:, None]
        weights = jnp.where(allowed[None], jnp.exp(scores * score_scale), 0.0)
        weighted = jnp.einsum(
            "hij,hdj->hid",
            weights.astype(jnp.bfloat16),
            value_block,
            preferred_element_type=jnp.float32,
        )
        return (jnp.sum(weights, axis=-1), weighted)

    initial = (
        jnp.zeros((head_count, row_count), jnp.float32),
        jnp.zeros((head_count, row_count, VD), jnp.float32),
    )
    shard_piece = (
        lax.all_gather(latent, "ep", axis=1, tiled=True),
        lax.all_gather(rotary_key, "ep", axis=1, tiled=True),
    )

    def compute_piece(running):
        key_block, value_block = expand(shard_piece[0])
        return attend(key_block, value_block, shard_piece[1])

    totals, weighted = lax.cond(jnp.int32(0) > last_row, keep_state, compute_piece, initial)
    attended = (weighted / totals[..., None]).astype(jnp.bfloat16)
    mixing = output_weight.reshape(head_count, VD, output_weight.shape[1])
    partial_value = jnp.einsum("hid,hde->ie", attended, mixing, preferred_element_type=jnp.float32)
    projected = lax.psum_scatter(
        lax.optimization_barrier(partial_value.astype(jnp.bfloat16))
        .astype(jnp.float32)
        .astype(jnp.bfloat16),
        "tp",
        scatter_dimension=0,
        tiled=True,
    ).astype(jnp.float32)
    mixed = rms_rows(projected, out_gain).astype(jnp.bfloat16)
    tokens = ffn_in.shape[0]
    part_count = lax.axis_size("tp")
    quarter_rows = tokens // part_count
    experts = lax.axis_size("ep")
    choose = routes.shape[1]
    capacity = max(2, 2 * quarter_rows * choose // experts)
    slot_count = capacity * part_count
    tp_index = lax.axis_index("tp")
    normed_b = rms_rows(ffn_in.astype(jnp.float32), ffn_gain).astype(jnp.bfloat16)
    padded = jnp.concatenate([normed_b, jnp.zeros((1, normed_b.shape[1]), jnp.bfloat16)], axis=0)
    gate_share = jax.nn.softmax(route_scores, axis=-1)
    grouped = routes.reshape(part_count, quarter_rows * choose)
    onehot = (grouped[:, :, None] == jnp.arange(experts, dtype=jnp.int32)[None, None, :]).astype(
        jnp.int32
    )
    slot_rank = jnp.sum((jnp.cumsum(onehot, axis=1) - 1) * onehot, axis=2)
    slot_index = jnp.arange(part_count, dtype=jnp.int32)[:, None] * capacity + slot_rank
    place_index = (slot_index * experts + grouped).reshape(-1)
    owners = jnp.arange(tokens * choose, dtype=jnp.int32) // choose
    slot_token = jnp.full((slot_count * experts,), tokens, jnp.int32).at[place_index].set(owners)
    unit_count = gate_weight.shape[2]
    chosen = lax.dynamic_slice_in_dim(
        slot_token, tp_index * capacity * experts, capacity * experts, 0
    )
    outgoing = padded[chosen].reshape(capacity, experts, -1)
    arrived = lax.all_to_all(outgoing, "ep", split_axis=1, concat_axis=1, tiled=True)
    row_block = lax.all_gather(arrived, "tp", axis=0, tiled=True)
    block_slots = row_block.shape[0]
    flat_rows = row_block.reshape(-1, row_block.shape[2])
    gate_part = jnp.dot(flat_rows, gate_weight[0], preferred_element_type=jnp.float32)
    up_part = jnp.dot(flat_rows, up_weight[0], preferred_element_type=jnp.float32)
    hidden = (
        clamped_unit(gate_part, up_part).astype(jnp.bfloat16).reshape(block_slots, -1, unit_count)
    )
    sources = hidden.shape[1]
    hidden_flat = hidden.reshape(slot_count * sources, unit_count)
    partial_value = jnp.dot(hidden_flat, down_weight[0], preferred_element_type=jnp.float32)
    result = lax.psum_scatter(
        lax.optimization_barrier(partial_value.astype(jnp.bfloat16))
        .astype(jnp.float32)
        .astype(jnp.bfloat16),
        "tp",
        scatter_dimension=0,
        tiled=True,
    )
    result = result.reshape(capacity, sources, -1)
    returned = lax.all_to_all(result, "ep", split_axis=1, concat_axis=1, tiled=True)
    back_rows = returned.reshape(capacity * experts, -1)
    own_rank = lax.dynamic_index_in_dim(slot_rank, tp_index, 0, keepdims=False)
    own_expert = lax.dynamic_index_in_dim(grouped, tp_index, 0, keepdims=False)
    picked = (
        back_rows[own_rank * experts + own_expert]
        .astype(jnp.float32)
        .reshape(quarter_rows, choose, -1)
    )
    own_gates = lax.dynamic_slice_in_dim(gate_share, tp_index * quarter_rows, quarter_rows, 0)
    moe_out = jnp.sum(picked * own_gates[:, :, None], axis=1).astype(jnp.bfloat16)
    return (mixed, moe_out)


MESH = pl.DeviceIdType.MESH
PIECES = 2
OUTER = (
    ["prep", "lats", "Lown", "Y0b"],
    ["X0a", "XY0", "Z10", "Z11"],
    ["C00", "qry", "Z20", "LZ1"],
    ["C01", "LX0", "E0", "Z21"],
    ["P0a", "Y1", "LY0", "D10"],
    ["Z30", "LZ2", "X1", "D11"],
    ["LC0", "E1", "Z31", "LY1"],
    ["P1a", "D20", "X2", "Y2"],
    ["P0b", "D21", "R00", "E2"],
    ["LX2", "P1b", "P2a", "D30"],
    ["LZ3", "Y3", "LY2", "X3"],
    ["P2b", "LD1", "D31", "A0"],
    ["LD2", "LX1", "R20", "E3"],
    ["R10", "LD3", "R21", "LY3"],
    ["P3a", "R11", "Q20", "A2"],
    ["Q21", "LX3", "A1", "Q10"],
    ["P3b", "R30", "R01", "A3"],
    ["R31", "PR", "Q00", "Q11"],
    ["Q30", "CH", "Q31", "Q01"],
    ["FH", "FM"],
)
INNER = (
    ["prep", "lats", "Lown", "Y0b"],
    ["X0a", "Z10", "Z20", "Z11"],
    ["XY0", "Z21", "LZ2", "C00"],
    ["LZ1", "LX0", "Z30", "C01"],
    ["LY0", "E0", "D10", "Z31"],
    ["Y1", "D20", "D11", "X1"],
    ["LY2", "LX2", "Y2", "X2"],
    ["P0a", "D21", "LZ3", "LC0"],
    ["D30", "E1", "LY1", "E2"],
    ["P1a", "P2a", "P2b", "LY3"],
    ["LD1", "P1b", "D31", "X3"],
    ["qry", "R10", "Y3", "A0"],
    ["LD2", "R20", "E3", "LD3"],
    ["LX3", "R21", "R11", "P0b"],
    ["A2", "P3a", "LX1", "Q20"],
    ["Q21", "P3b", "A3", "A1"],
    ["R30", "Q10", "R31", "PR"],
    ["R00", "R01", "Q11", "Q30"],
    ["CH", "Q31", "Q00", "Q01"],
    ["FM", "FH"],
)


def flip(value, bits):
    bit = 1
    while bit <= bits:
        if bits & bit:
            value = value + bit - 2 * bit * ((value // bit) % 2)
        bit *= 2
    return value


def here():
    ep, tp = lax.axis_index("ep"), lax.axis_index("tp")
    return ep // 2, ep % 2, tp // 2, tp % 2


def place(z, x, y, core):
    return {"ep": z * 2 + x, "tp": y * 2 + core}


def greet(partners):
    barrier = pltpu.get_barrier_semaphore()
    for partner in partners:
        pl.semaphore_signal(barrier, inc=1, device_id=partner, device_id_type=MESH)
    pl.semaphore_wait(barrier, len(partners))


def layer_kernel(
    width, heads,
    ffn_hbm, mix_hbm, ffn_gain_hbm, mix_gain_hbm, latent_gain_hbm, out_gain_hbm, routes_hbm, scores_hbm,
    base_hbm, step_hbm, latent_hbm, rotary_hbm, query_hbm, gate_hbm, up_hbm, down_hbm, key_hbm,
    value_hbm, output_hbm, mixed_ref, moe_ref,
    rows_all, lat_all, part_ref, work, twin_in, hop_in, direct_in, relay_in, column_in,
    heads_ref, heads_work, heads_twin, heads_in, query_ref, keys, values, weighted, totals, attended, own_total,
    table_ref, turn_ref, ffn_ref, mix_ref,
    ffn_gain, mix_gain, latent_gain, gain_ref, routes_ref, scores_ref, base_ref, step_ref, latent_ref,
    rotary_ref, query_w, gate_ref, up_ref, down_ref, key_ref, value_ref, output_ref,
    row_send, row_recv, lat_send, lat_recv, send_sem, twin_sem, square_sem, column_sem, heads_sem, load_sem,
):
    f32, bf16 = jnp.float32, jnp.bfloat16
    ep, tp = lax.axis_index("ep"), lax.axis_index("tp")
    z, x, y, core = here()
    inner = ((z + 1) // 2) % 2
    planes = [z, flip(z, 1)]
    far = flip(z, 2)
    planes.append(far + inner * (1 - 2 * (far % 2)))
    planes.append(flip(planes[2], 1))
    depth = len(planes)
    x_next, y_next, twin = place(z, 1 - x, y, core), place(z, x, 1 - y, core), place(z, x, y, 1 - core)
    z_out, z_in = place(planes[1], x, y, core), place(flip(z, 3), x, y, core)
    parts, quarter = part_ref.shape[2:4]
    row_count = parts * quarter
    block_rows = 2 * row_count
    experts = 2 * depth
    half = ROPE // 2
    piece = quarter // PIECES
    first_own = pl.multiple_of(tp * quarter, quarter)
    copied = (
        (ffn_hbm.at[pl.ds(first_own, quarter)], ffn_ref), (ffn_gain_hbm, ffn_gain),
        (mix_hbm, mix_ref), (mix_gain_hbm, mix_gain), (rotary_hbm, rotary_ref),
        (base_hbm, base_ref), (step_hbm, step_ref), (routes_hbm, routes_ref), (scores_hbm, scores_ref),
        (latent_hbm, latent_ref), (latent_gain_hbm, latent_gain), (query_hbm, query_w),
        (gate_hbm, gate_ref), (up_hbm, up_ref), (down_hbm, down_ref),
        (key_hbm, key_ref), (value_hbm, value_ref), (output_hbm, output_ref), (out_gain_hbm, gain_ref),
    )
    loads = [pltpu.make_async_copy(src, dst, load_sem.at[n]) for n, (src, dst) in enumerate(copied)]
    for load in loads:
        load.start()
    waited = [0]

    def loaded(count):
        while waited[0] < count:
            loads[waited[0]].wait()
            waited[0] += 1

    greet([place(p, x, y, core) for p in planes[1:]] + [x_next, y_next, twin])
    always = None
    issued = {}

    def guarded(condition, action):
        if condition is None:
            action()
        else:
            pl.when(condition)(action)

    role = ["both"]

    def post(key, build, condition=always):
        if condition == "inner":
            if role[0] == "outer":
                return
            condition = always if role[0] == "inner" else is_inner
        issued.setdefault(key, (build, condition))
        guarded(condition, lambda: build().start())

    numbers = {}

    def number(kind, key):
        taken = numbers.setdefault(kind, {})
        return taken.setdefault(key, len(taken))

    def at_piece(ref, g):
        return ref if g is None else ref.at[pl.ds(g * piece, piece)]

    def row_copy(origin, g, target, key):
        e, t = origin["ep"], origin["tp"]
        ref = at_piece(rows_all.at[e, t], g)
        return pltpu.make_async_remote_copy(
            src_ref=ref, dst_ref=ref, send_sem=row_send.at[number("row", key)],
            recv_sem=row_recv.at[e, t, g or 0], device_id=target, device_id_type=MESH,
        )

    def give_row(name, origin, g, target, towards, condition=always):
        key = (name, g, towards)
        post(("row",) + key, lambda: row_copy(origin, g, target, key), condition)

    def take_row(origin, g):
        row_copy(origin, g, twin, ("any",)).wait_recv()

    def lat_copy(origin, target, key):
        e, t = origin["ep"], origin["tp"]
        ref = lat_all.at[e, t]
        return pltpu.make_async_remote_copy(
            src_ref=ref, dst_ref=ref, send_sem=lat_send.at[number("lat", key)],
            recv_sem=lat_recv.at[e, t], device_id=target, device_id_type=MESH,
        )

    def give_lat(name, origin, target, towards, condition=always):
        key = (name, towards)
        post(("lat",) + key, lambda: lat_copy(origin, target, key), condition)

    def take_lat(origin):
        lat_copy(origin, twin, ("any",)).wait_recv()

    def make(src, dst, sem, target, key):
        return pltpu.make_async_remote_copy(
            src_ref=src, dst_ref=dst, send_sem=send_sem.at[number("sum", key)], recv_sem=sem,
            device_id=target, device_id_type=MESH,
        )

    def send(src, dst, sem, target, *key):
        post(("sum",) + key, lambda: make(src, dst, sem, target, key))

    def arrive(dst, sem):
        make(dst, dst, sem, twin, ("any",)).wait_recv()

    is_inner, is_outer = inner == 1, inner == 0
    up_out, up_in = z % 2 == 0, z == 1
    me = place(z, x, y, core)

    origins = {
        (s, dx, dy): place(planes[s], flip(x, dx), flip(y, dy), core)
        for s in range(depth) for dx in (0, 1) for dy in (0, 1)
    }

    def origin_of(s, dx, dy):
        return origins[s, dx, dy]

    def own_rows():
        for g in range(PIECES):
            give_row("own", me, g, z_out, "out")
            give_row("own", me, g, z_in, "in", "inner")
            give_row("own", me, g, x_next, "x")
            give_row("own", me, PIECES - 1 - g, y_next, "y")
        give_row("own", me, None, twin, "twin")

    def side_rows(first):
        by_x, by_y = origin_of(0, 1, 0), origin_of(0, 0, 1)
        for g in range(PIECES // 2):
            if first == "x":
                take_row(by_x, g)
                give_row("x0", by_x, g, y_next, "y")
            else:
                take_row(by_y, PIECES - 1 - g)
                give_row("y0", by_y, PIECES - 1 - g, x_next, "x")

    def side_rows_rest():
        by_x, by_y = origin_of(0, 1, 0), origin_of(0, 0, 1)
        for g in range(PIECES // 2):
            take_row(by_x, PIECES - 1 - g)
            take_row(by_y, g)
        give_row("x0", by_x, None, twin, "twin")
        give_row("y0", by_y, None, twin, "twin")

    def last(g):
        return g == PIECES - 1

    def corner_rows(g):
        corner = origin_of(0, 1, 1)
        take_row(corner, g)
        give_row("c0", corner, g, z_out, "out")
        give_row("c0", corner, g, z_in, "in", "inner")
        if last(g):
            give_row("c0", corner, None, twin, "twin")

    def column_rows(s, g, dx):
        origin = origin_of(s, dx, dx)
        name = f"{'zd'[dx]}{s}"
        take_row(origin, g)
        if s == 1:
            give_row(name, origin, g, z_in, "in", "inner")
        else:
            give_row(name, origin, g, z_out, "out", "inner")
        if not dx:
            give_row(name, origin, g, x_next, "x")
            give_row(name, origin, g, y_next, "y")
        if last(g):
            give_row(name, origin, None, twin, "twin")

    def square_rows(s, dx):
        origin = origin_of(s, dx, 1 - dx)
        for g in range(PIECES):
            take_row(origin, g)
        give_row(f"{'yx'[dx]}{s}", origin, None, twin, "twin")

    def own_lats():
        give_lat("own", me, z_out, "out", up_out)
        give_lat("own", me, z_in, "in", up_in)
        give_lat("own", me, x_next, "x")
        give_lat("own", me, y_next, "y")
        give_lat("own", me, twin, "twin")

    def side_lats(dx):
        origin = origin_of(0, dx, 1 - dx)
        name = f"{'yx'[dx]}0"
        take_lat(origin)
        if dx:
            give_lat(name, origin, y_next, "y")
        give_lat(name, origin, twin, "twin")

    def corner_lats():
        corner = origin_of(0, 1, 1)
        take_lat(corner)
        give_lat("c0", corner, z_out, "out", up_out)
        give_lat("c0", corner, z_in, "in", up_in)
        give_lat("c0", corner, twin, "twin")

    lower = [plane < z for plane in planes]
    up_two = z == 2

    def below(s):
        return lower[s]

    def column_lats(s, dx):
        origin = origin_of(s, dx, dx)
        name = f"{'zd'[dx]}{s}"

        @pl.when(below(s))
        def _():
            take_lat(origin)

        if s == 1:
            give_lat(name, origin, z_in, "in", up_in)
        else:
            give_lat(name, origin, z_out, "out", up_two)
        if not dx:
            give_lat(name, origin, x_next, "x", below(s))
            give_lat(name, origin, y_next, "y", below(s))
        give_lat(name, origin, twin, "twin", below(s))

    def square_lats(s, dx):
        origin = origin_of(s, dx, 1 - dx)

        @pl.when(below(s))
        def _():
            take_lat(origin)

        give_lat(f"{'yx'[dx]}{s}", origin, twin, "twin", below(s))

    def expert_plane(s):
        loaded(15)
        for a in (0, 1):
            for b in (0, 1):
                take_row(place(planes[s], flip(x, a), flip(y, b), 1 - core), None)
        pair = pl.ds(planes[s] * 2, 2)
        block = rows_all[pair, :, :, :width].reshape(block_rows, width)
        gate_part = jnp.dot(block, gate_ref[...], preferred_element_type=f32)
        up_part = jnp.dot(block, up_ref[...], preferred_element_type=f32)
        hidden = clamped_unit(gate_part, up_part).astype(bf16)
        table = rows_all[pair, :, :, width:].reshape(block_rows, 2 * ROPE)
        lane = lax.broadcasted_iota(jnp.int32, table.shape, 1)
        is_mine = (lane == ROPE + ep) | (lane == ROPE + experts + ep)
        share = jnp.sum(jnp.where(is_mine, table.astype(f32), 0.0), axis=1, keepdims=True)
        chunk = 512
        for n in range(0, width, chunk):
            out = jnp.dot(hidden, down_ref[:, n : n + chunk], preferred_element_type=f32) * share
            part_ref[s, :, :, :, n : n + chunk] = out.astype(bf16).reshape(2, parts, quarter, chunk)
        for a, b in ((1, 1), (0, 1), (1, 0), (0, 0)) if s % 2 else ((1, 1), (1, 0), (0, 1), (0, 0)):
            mine = part_ref.at[s, flip(x, a), flip(y, b) * 2 + 1 - core]
            send(mine, twin_in.at[s, a, b], twin_sem.at[s, a, b], twin, "twin", s, a, b)

    def paired(s, a, b, g=None):
        if not g:
            arrive(twin_in.at[s, a, b], twin_sem.at[s, a, b])
        rows = slice(None) if g is None else rows_of(g)
        own = part_ref[s, flip(x, a), flip(y, b) * 2 + core, rows]
        return own.astype(f32) + twin_in[s, a, b, rows].astype(f32)

    def rows_of(g):
        return pl.ds(g * piece, piece)

    def sum_pairs(s, corner):
        a, b = (1, 1) if corner else (0, 1) if s % 2 else (1, 0)
        landing, which = (hop_in, 0) if corner else (direct_in, 1)
        work[s, a, b] = paired(s, a, b).astype(bf16)
        for g in range(PIECES):
            send(
                work.at[s, a, b, rows_of(g)], landing.at[s, rows_of(g)], square_sem.at[which, s, g],
                y_next if s % 2 else x_next, which, s, g,
            )

    def sum_relay(s, g):
        a, b = (1, 0) if s % 2 else (0, 1)
        rows = rows_of(g)
        value = paired(s, a, b, g)
        arrive(hop_in.at[s, rows], square_sem.at[0, s, g])
        work[s, a, b, rows] = (value + hop_in[s, rows].astype(f32)).astype(bf16)
        send(
            work.at[s, a, b, rows], relay_in.at[s, rows], square_sem.at[2, s, g],
            x_next if s % 2 else y_next, 2, s, g,
        )

    def sum_square(s, g):
        rows = rows_of(g)
        value = paired(s, 0, 0, g)
        arrive(direct_in.at[s, rows], square_sem.at[1, s, g])
        value = value + direct_in[s, rows].astype(f32)
        arrive(relay_in.at[s, rows], square_sem.at[2, s, g])
        value = value + relay_in[s, rows].astype(f32)
        if s:
            work[s, 0, 0, rows] = value.astype(bf16)
            send(
                work.at[s, 0, 0, rows], column_in.at[z, rows], column_sem.at[z, g],
                place(planes[s], x, y, core), "column", s, g,
            )
        else:
            own_total[rows, :] = value

    across = (((1,), (1,)), ((), ()))
    score_scale = (NOPE + ROPE) ** (-0.5)

    def angles():
        near = base_ref[...]
        swapped = pltpu.roll(near, ROPE, 1)
        lane = lax.broadcasted_iota(jnp.int32, near.shape, 1)
        cosine, sine = jnp.where(lane < ROPE, near, swapped), jnp.where(lane < ROPE, swapped, near)
        step = jnp.broadcast_to(step_ref[pl.ds(ep, 1), :], near.shape)
        step_swapped = pltpu.roll(step, ROPE, 1)
        step_cos, step_sin = jnp.where(lane < ROPE, step, step_swapped), jnp.where(lane < ROPE, step_swapped, step)
        turn_ref[...] = jnp.where(
            lane < ROPE, cosine * step_cos - sine * step_sin, sine * step_cos + cosine * step_sin
        )

    def rotate(vectors, table):
        lane = lax.broadcasted_iota(jnp.int32, vectors.shape, 1)
        size = vectors.shape[1]
        turned = jnp.where(
            lane < half, -pltpu.roll(vectors, size - half, 1), pltpu.roll(vectors, half, 1)
        )
        sine = pltpu.roll(table, size - ROPE, 1)
        return jnp.where(lane < ROPE, vectors * table + turned * sine, 0.0)

    own = pl.ds(first_own, quarter)

    def own_normed():
        return rms_rows(mix_ref[own, :].astype(f32), mix_gain[...]).astype(bf16)

    def prepare_rows():
        loaded(9)
        rows_all[ep, tp, :, :width] = rms_rows(ffn_ref[...].astype(f32), ffn_gain[...]).astype(bf16)
        angles()
        turned = lax.dot_general(own_normed(), rotary_ref[...], across, preferred_element_type=f32)
        turned = jnp.concatenate([turned, jnp.zeros((quarter, ROPE), f32)], axis=1)
        rotary_key = rotate(turned, turn_ref[own, :])
        scores = scores_ref[...]
        shares = jnp.exp(scores - jnp.max(scores, axis=0, keepdims=True))
        shares = shares / jnp.sum(shares, axis=0, keepdims=True)
        routes = routes_ref[...]
        lane = lax.broadcasted_iota(jnp.int32, (2 * ROPE, row_count), 0)
        named = jnp.zeros((2 * ROPE, row_count), f32)
        for k in range(routes.shape[0]):
            hit = (lane == routes[k : k + 1] + ROPE) | (lane == routes[k : k + 1] + ROPE + experts)
            named = named + jnp.where(hit, shares[k : k + 1], 0.0)
        coarse = named.astype(bf16).astype(f32)
        table_ref[...] = jnp.where(lane < ROPE + experts, coarse, named - coarse).T
        rows_all[ep, tp, :, width:] = (rotary_key + table_ref[own, :]).astype(bf16)

    def prepare_lats():
        loaded(11)
        latent = jnp.dot(own_normed(), latent_ref[...], preferred_element_type=f32)
        lat_all[ep, tp] = rms_rows(latent, latent_gain[...]).astype(bf16)

    def prepare_queries():
        loaded(12)
        normed = rms_rows(mix_ref[...].astype(f32), mix_gain[...]).astype(bf16)
        for h in range(0, heads, 2):
            columns_of = slice(h * (NOPE + ROPE), (h + 2) * (NOPE + ROPE))
            two = jnp.dot(normed, query_w[:, columns_of], preferred_element_type=f32)
            table = turn_ref[...]
            middle, last = two[:, NOPE : 2 * NOPE], two[:, 2 * NOPE :]
            lane = lax.broadcasted_iota(jnp.int32, last.shape, 1)
            low, high = pltpu.roll(middle, ROPE, 1), pltpu.roll(last, ROPE, 1)
            query_ref[h, :, :NOPE] = two[:, :NOPE].astype(bf16)
            query_ref[h, :, NOPE:] = rotate(middle, table).astype(bf16)
            query_ref[h + 1, :, :NOPE] = jnp.where(lane < ROPE, low, high).astype(bf16)
            query_ref[h + 1, :, NOPE:] = rotate(high, table).astype(bf16)

    def attend_block(s):
        for a in (0, 1):
            for b in (0, 1):
                take_lat(place(planes[s], flip(x, a), flip(y, b), 1 - core))
        pair = pl.ds(planes[s] * 2, 2)
        latent = lat_all[pair].reshape(block_rows, lat_all.shape[3])
        rest = rows_all[pair, :, :, width:].reshape(block_rows, 2 * ROPE)
        key_block = jnp.dot(latent, key_ref[...], preferred_element_type=f32).astype(bf16)
        value_block = jnp.dot(latent, value_ref[...], preferred_element_type=f32).astype(bf16)
        for h in range(heads):
            keys[h, :, :NOPE] = key_block[:, h * NOPE : (h + 1) * NOPE]
            keys[h, :, NOPE:] = rest
            values[h] = value_block[:, h * VD : (h + 1) * VD]
        shape = (row_count, block_rows)
        places = lax.broadcasted_iota(jnp.int32, shape, 0) + ep * row_count
        allowed = lax.broadcasted_iota(jnp.int32, shape, 1) + planes[s] * block_rows <= places
        for h in range(heads):
            scores = lax.dot_general(query_ref[h], keys[h], across, preferred_element_type=f32)
            weights = jnp.where(allowed, jnp.exp(scores * score_scale), 0.0)
            total = jnp.broadcast_to(jnp.sum(weights, axis=1, keepdims=True), (row_count, VD))
            update = jnp.dot(weights.astype(bf16), values[h], preferred_element_type=f32)
            totals[h] = total if s == 0 else totals[h] + total
            weighted[h] = update if s == 0 else weighted[h] + update

    def attend_plane(s):
        loaded(17)
        if s == 0:
            attend_block(s)
        else:
            pl.when(below(s))(lambda: attend_block(s))

    def project():
        loaded(18)
        for h in range(heads):
            attended[:, h * VD : (h + 1) * VD] = (weighted[h] / totals[h]).astype(bf16)
        chunk = 512
        for n in range(0, width, chunk):
            out = jnp.dot(attended[...], output_ref[:, n : n + chunk], preferred_element_type=f32)
            heads_ref[:, :, n : n + chunk] = out.astype(bf16).reshape(parts, quarter, chunk)
        for b in (1, 0):
            send(
                heads_ref.at[flip(y, b) * 2 + 1 - core], heads_twin.at[b], heads_sem.at[b], twin,
                "heads", b,
            )

    def cross_heads():
        arrive(heads_twin.at[1], heads_sem.at[1])
        heads_work[...] = (
            heads_ref[(1 - y) * 2 + core].astype(f32) + heads_twin[1].astype(f32)
        ).astype(bf16)
        send(heads_work, heads_in, heads_sem.at[2], y_next, "heads", 2)

    def finish_heads():
        loaded(len(loads))
        arrive(heads_twin.at[0], heads_sem.at[0])
        arrive(heads_in, heads_sem.at[2])
        projected = (
            heads_ref[y * 2 + core].astype(f32) + heads_twin[0].astype(f32) + heads_in[...].astype(f32)
        )
        mixed_ref[...] = rms_rows(projected, gain_ref[...]).astype(bf16)

    def finish_moe():
        for g in range(PIECES):
            rows = rows_of(g)
            total = own_total[rows, :]
            for s in range(1, depth):
                arrive(column_in.at[planes[s], rows], column_sem.at[planes[s], g])
                total = total + column_in[planes[s], rows].astype(f32)
            moe_ref[rows, :] = total.astype(bf16)

    def start_rows():
        prepare_rows()
        own_rows()

    steps = {
        "prep": start_rows, "lats": prepare_lats, "qry": prepare_queries, "Lown": own_lats,
        "X0a": lambda: side_rows("x"), "Y0b": lambda: side_rows("y"), "XY0": side_rows_rest,
        "C00": lambda: corner_rows(0), "C01": lambda: corner_rows(1),
        "LX0": lambda: side_lats(1), "LY0": lambda: side_lats(0), "LC0": corner_lats,
        "PR": project, "CH": cross_heads, "FH": finish_heads, "FM": finish_moe,
    }
    kinds = {
        "Z": lambda s, g: column_rows(s, g, 0), "D": lambda s, g: column_rows(s, g, 1),
        "X": lambda s: square_rows(s, 1), "Y": lambda s: square_rows(s, 0),
        "LZ": lambda s: column_lats(s, 0), "LD": lambda s: column_lats(s, 1),
        "LX": lambda s: square_lats(s, 1), "LY": lambda s: square_lats(s, 0),
        "E": expert_plane, "A": attend_plane, "R": sum_relay, "Q": sum_square,
    }

    def run(step):
        if step in steps:
            steps[step]()
        elif step[0] == "P":
            sum_pairs(int(step[1]), step[2] == "a")
        else:
            kind = step.rstrip("0123456789")
            kinds[kind](*(int(digit) for digit in step[len(kind) :]))

    orders = [sum(order, []) for order in (OUTER, INNER)]
    shared = 0
    while orders[0][shared] == orders[1][shared]:
        run(orders[0][shared])
        shared += 1
    ready, sent = waited[0], dict(issued)
    for name, chosen, order in (("outer", is_outer, orders[0]), ("inner", is_inner, orders[1])):
        role[0], waited[0] = name, ready
        issued.clear()
        issued.update(sent)

        @pl.when(chosen)
        def _():
            for step in order[shared:]:
                run(step)
            for build, condition in issued.values():
                guarded(condition, lambda: build().wait_send())


def turn_tables(row_count, experts):
    inverse = rope_base ** (-np.arange(0, ROPE, 2) / ROPE)
    near, far = np.arange(row_count)[:, None] * inverse, row_count * np.arange(experts)[:, None] * inverse

    def lanes(angle):
        return np.concatenate([np.cos(angle)] * 2 + [np.sin(angle)] * 2, axis=1).astype(np.float32)

    return lanes(near), lanes(far)


def dense_local(
    mix_in, mix_gain, query_weight, latent_weight, rotary_weight, latent_gain, key_weight,
    value_weight, output_weight, out_gain, ffn_in, ffn_gain, gate_weight, up_weight, down_weight,
    routes, route_scores,
):
    experts, parts = lax.axis_size("ep"), lax.axis_size("tp")
    row_count, width = mix_in.shape
    quarter, depth = row_count // parts, experts // 2
    block_rows = 2 * row_count
    heads = query_weight.shape[1] // (NOPE + ROPE)
    base, step = turn_tables(row_count, experts)
    row = lambda gain: gain.reshape(1, -1)
    operands = (
        ffn_in, mix_in, row(ffn_gain), row(mix_gain), row(latent_gain), row(out_gain), routes.T,
        route_scores.T, jnp.asarray(base), jnp.asarray(step), latent_weight, rotary_weight.T, query_weight,
        gate_weight[0], up_weight[0], down_weight[0], key_weight, value_weight, output_weight,
    )
    held = lambda *lead: pltpu.VMEM(lead + (quarter, width), jnp.bfloat16)
    scratch = lambda *shape: pltpu.VMEM(shape, jnp.bfloat16)
    wide = lambda *shape: pltpu.VMEM(shape, jnp.float32)
    sems = lambda *shape: pltpu.SemaphoreType.DMA(shape)
    return pl.pallas_call(
        functools.partial(layer_kernel, width, heads),
        out_shape=[pltpu.VMEM((quarter, width), jnp.bfloat16)] * 2,
        in_specs=[pl.BlockSpec(memory_space=pl.ANY)] * len(operands),
        out_specs=[pl.BlockSpec(memory_space=pltpu.VMEM)] * 2,
        scratch_shapes=[
            scratch(experts, parts, quarter, width + 2 * ROPE),
            scratch(experts, parts, quarter, latent_weight.shape[1]),
            held(depth, 2, parts), held(depth, 2, 2), held(depth, 2, 2),
            held(depth), held(depth), held(depth), held(depth),
            held(parts), held(), held(2), held(),
            scratch(heads, row_count, NOPE + 2 * ROPE), scratch(heads, block_rows, NOPE + 2 * ROPE),
            scratch(heads, block_rows, VD), wide(heads, row_count, VD), wide(heads, row_count, VD),
            scratch(row_count, heads * VD), wide(quarter, width),
            wide(row_count, 2 * ROPE), wide(row_count, 2 * ROPE),
            pltpu.VMEM((quarter, width), ffn_in.dtype), pltpu.VMEM(mix_in.shape, mix_in.dtype),
        ]
        + [pltpu.VMEM(a.shape, a.dtype) for a in operands[2:]]
        + [
            sems(96), sems(experts, parts, PIECES), sems(48), sems(experts, parts), sems(64),
            sems(depth, 2, 2), sems(3, depth, PIECES), sems(depth, PIECES), sems(3), sems(len(operands)),
        ],
        compiler_params=pltpu.CompilerParams(
            collective_id=0, has_side_effects=True, vmem_limit_bytes=60 * 1024 * 1024
        ),
        name="layer",
    )(*operands)


def solution(mesh):
    experts, parts = mesh.shape["ep"], mesh.shape["tp"]

    def body(*args):
        quarter, choose = args[10].shape[0] // parts, args[15].shape[1]
        every_row = 2 * quarter * choose >= quarter * experts
        paired = parts == 4 and experts == 8 and quarter % (16 * PIECES) == 0
        return (dense_local if every_row and paired else local)(*args)
    placed = (
        P("ep", None),
        P(),
        P(None, "tp"),
        P(),
        P(),
        P(),
        P(None, "tp"),
        P(None, "tp"),
        P("tp", None),
        P(),
        P("ep", None),
        P(),
        P("ep", None, "tp"),
        P("ep", None, "tp"),
        P("ep", "tp", None),
        P("ep", None),
        P("ep", None),
    )
    return jax.shard_map(
        body,
        mesh=mesh,
        in_specs=placed,
        out_specs=(P(("ep", "tp"), None), P(("ep", "tp"), None)),
        check_vma=False,
    )
```

```python
import jax
import jax.numpy as jnp
import functools
import numpy as np
from jax import lax
from jax.experimental import pallas as pl
from jax.experimental.pallas import tpu as pltpu
from jax.sharding import PartitionSpec as P

NOPE = 128
ROPE = 64
VD = 128


norm_eps = 1e-06
clamp_limit = 7.0
gate_slope = 1.702
rope_base = 10000.0


def rms_rows(rows_in, scales):
    mean_square = jnp.mean(rows_in * rows_in, axis=-1, keepdims=True)
    return rows_in * lax.rsqrt(mean_square + norm_eps) * scales


def rms_columns(columns, scales):
    mean_square = jnp.mean(columns * columns, axis=0, keepdims=True)
    return columns * lax.rsqrt(mean_square + norm_eps) * scales[:, None]


def turn_table(positions):
    inverse = rope_base ** (-jnp.arange(0, ROPE, 2).astype(jnp.float32) / ROPE)
    angle_rows = inverse[:, None] * positions.astype(jnp.float32)[None, :]
    return (jnp.cos(angle_rows), jnp.sin(angle_rows))


def clamped_unit(gate_part, linear):
    gate_part = jnp.minimum(gate_part, clamp_limit)
    linear = jnp.clip(linear, -clamp_limit, clamp_limit)
    return gate_part * jax.nn.sigmoid(gate_slope * gate_part) * (linear + 1.0)


def keep_state(running):
    return running


def local(
    mix_in,
    mix_gain,
    query_weight,
    latent_weight,
    rotary_weight,
    latent_gain,
    key_weight,
    value_weight,
    output_weight,
    out_gain,
    ffn_in,
    ffn_gain,
    gate_weight,
    up_weight,
    down_weight,
    routes,
    route_scores,
):
    row_count = mix_in.shape[0]
    first_row = lax.axis_index("ep") * row_count
    last_row = first_row + row_count - 1
    positions = first_row + jnp.arange(row_count, dtype=jnp.int32)
    normed = rms_rows(mix_in.astype(jnp.float32), mix_gain).astype(jnp.bfloat16)
    head_count = query_weight.shape[1] // (NOPE + ROPE)
    half_rope = ROPE // 2
    cosine, sine_rows = turn_table(positions)
    queries = jnp.dot(normed, query_weight, preferred_element_type=jnp.float32).reshape(
        row_count, head_count, NOPE + ROPE
    )
    query_plain = queries[..., :NOPE].astype(jnp.bfloat16)
    query_cos = cosine.T[:, None, :]
    query_sin = sine_rows.T[:, None, :]
    query_upper = queries[..., NOPE : NOPE + half_rope]
    query_lower = queries[..., NOPE + half_rope :]
    query_turn = jnp.concatenate(
        [
            query_upper * query_cos - query_lower * query_sin,
            query_lower * query_cos + query_upper * query_sin,
        ],
        axis=-1,
    ).astype(jnp.bfloat16)
    across = (((0,), (1,)), ((), ()))
    latent = rms_columns(
        lax.dot_general(latent_weight, normed, across, preferred_element_type=jnp.float32),
        latent_gain,
    ).astype(jnp.bfloat16)
    rot_raw = lax.dot_general(rotary_weight, normed, across, preferred_element_type=jnp.float32)
    rotary_key = jnp.concatenate(
        [
            rot_raw[:half_rope] * cosine - rot_raw[half_rope:] * sine_rows,
            rot_raw[half_rope:] * cosine + rot_raw[:half_rope] * sine_rows,
        ],
        axis=0,
    ).astype(jnp.bfloat16)
    score_scale = (NOPE + ROPE) ** (-0.5)
    contract_first = (((0,), (0,)), ((), ()))

    def expand(latent_block):
        key_block = lax.dot_general(
            key_weight, latent_block, contract_first, preferred_element_type=jnp.float32
        ).astype(jnp.bfloat16)
        value_block = lax.dot_general(
            value_weight, latent_block, contract_first, preferred_element_type=jnp.float32
        ).astype(jnp.bfloat16)
        return (key_block, value_block)

    def attend(key_block, value_block, turn_block):
        key_count = key_block.shape[1]
        key_block = key_block.reshape(head_count, NOPE, key_count)
        value_block = value_block.reshape(head_count, VD, key_count)
        scores = jnp.einsum(
            "ihd,hdj->hij", query_plain, key_block, preferred_element_type=jnp.float32
        )
        scores = scores + jnp.einsum(
            "ihd,dj->hij", query_turn, turn_block, preferred_element_type=jnp.float32
        )
        key_places = jnp.arange(key_count, dtype=jnp.int32)
        allowed = key_places[None, :] <= positions[:, None]
        weights = jnp.where(allowed[None], jnp.exp(scores * score_scale), 0.0)
        weighted = jnp.einsum(
            "hij,hdj->hid",
            weights.astype(jnp.bfloat16),
            value_block,
            preferred_element_type=jnp.float32,
        )
        return (jnp.sum(weights, axis=-1), weighted)

    initial = (
        jnp.zeros((head_count, row_count), jnp.float32),
        jnp.zeros((head_count, row_count, VD), jnp.float32),
    )
    shard_piece = (
        lax.all_gather(latent, "ep", axis=1, tiled=True),
        lax.all_gather(rotary_key, "ep", axis=1, tiled=True),
    )

    def compute_piece(running):
        key_block, value_block = expand(shard_piece[0])
        return attend(key_block, value_block, shard_piece[1])

    totals, weighted = lax.cond(jnp.int32(0) > last_row, keep_state, compute_piece, initial)
    attended = (weighted / totals[..., None]).astype(jnp.bfloat16)
    mixing = output_weight.reshape(head_count, VD, output_weight.shape[1])
    partial_value = jnp.einsum("hid,hde->ie", attended, mixing, preferred_element_type=jnp.float32)
    projected = lax.psum_scatter(
        lax.optimization_barrier(partial_value.astype(jnp.bfloat16))
        .astype(jnp.float32)
        .astype(jnp.bfloat16),
        "tp",
        scatter_dimension=0,
        tiled=True,
    ).astype(jnp.float32)
    mixed = rms_rows(projected, out_gain).astype(jnp.bfloat16)
    tokens = ffn_in.shape[0]
    part_count = lax.axis_size("tp")
    quarter_rows = tokens // part_count
    experts = lax.axis_size("ep")
    choose = routes.shape[1]
    capacity = max(2, 2 * quarter_rows * choose // experts)
    slot_count = capacity * part_count
    tp_index = lax.axis_index("tp")
    normed_b = rms_rows(ffn_in.astype(jnp.float32), ffn_gain).astype(jnp.bfloat16)
    padded = jnp.concatenate([normed_b, jnp.zeros((1, normed_b.shape[1]), jnp.bfloat16)], axis=0)
    gate_share = jax.nn.softmax(route_scores, axis=-1)
    grouped = routes.reshape(part_count, quarter_rows * choose)
    onehot = (grouped[:, :, None] == jnp.arange(experts, dtype=jnp.int32)[None, None, :]).astype(
        jnp.int32
    )
    slot_rank = jnp.sum((jnp.cumsum(onehot, axis=1) - 1) * onehot, axis=2)
    slot_index = jnp.arange(part_count, dtype=jnp.int32)[:, None] * capacity + slot_rank
    place_index = (slot_index * experts + grouped).reshape(-1)
    owners = jnp.arange(tokens * choose, dtype=jnp.int32) // choose
    slot_token = jnp.full((slot_count * experts,), tokens, jnp.int32).at[place_index].set(owners)
    unit_count = gate_weight.shape[2]
    chosen = lax.dynamic_slice_in_dim(
        slot_token, tp_index * capacity * experts, capacity * experts, 0
    )
    outgoing = padded[chosen].reshape(capacity, experts, -1)
    arrived = lax.all_to_all(outgoing, "ep", split_axis=1, concat_axis=1, tiled=True)
    row_block = lax.all_gather(arrived, "tp", axis=0, tiled=True)
    block_slots = row_block.shape[0]
    flat_rows = row_block.reshape(-1, row_block.shape[2])
    gate_part = jnp.dot(flat_rows, gate_weight[0], preferred_element_type=jnp.float32)
    up_part = jnp.dot(flat_rows, up_weight[0], preferred_element_type=jnp.float32)
    hidden = (
        clamped_unit(gate_part, up_part).astype(jnp.bfloat16).reshape(block_slots, -1, unit_count)
    )
    sources = hidden.shape[1]
    hidden_flat = hidden.reshape(slot_count * sources, unit_count)
    partial_value = jnp.dot(hidden_flat, down_weight[0], preferred_element_type=jnp.float32)
    result = lax.psum_scatter(
        lax.optimization_barrier(partial_value.astype(jnp.bfloat16))
        .astype(jnp.float32)
        .astype(jnp.bfloat16),
        "tp",
        scatter_dimension=0,
        tiled=True,
    )
    result = result.reshape(capacity, sources, -1)
    returned = lax.all_to_all(result, "ep", split_axis=1, concat_axis=1, tiled=True)
    back_rows = returned.reshape(capacity * experts, -1)
    own_rank = lax.dynamic_index_in_dim(slot_rank, tp_index, 0, keepdims=False)
    own_expert = lax.dynamic_index_in_dim(grouped, tp_index, 0, keepdims=False)
    picked = (
        back_rows[own_rank * experts + own_expert]
        .astype(jnp.float32)
        .reshape(quarter_rows, choose, -1)
    )
    own_gates = lax.dynamic_slice_in_dim(gate_share, tp_index * quarter_rows, quarter_rows, 0)
    moe_out = jnp.sum(picked * own_gates[:, :, None], axis=1).astype(jnp.bfloat16)
    return (mixed, moe_out)


MESH = pl.DeviceIdType.MESH
PIECES = 2
NAMES = (
    "A0", "A1", "A2", "A3", "C00", "C01", "CH", "D10", "D11", "D20", "D21", "D30", "D31", "E0", "E1", "E2", "E3",
    "FH", "FM", "LC0", "LD1", "LD2", "LD3", "LX0", "LX1", "LX2", "LX3", "LY0", "LY1", "LY2", "LY3", "LZ1", "LZ2",
    "LZ3", "Lown", "P0a", "P0b", "P1a", "P1b", "P2a", "P2b", "P3a", "P3b", "PR", "Q00", "Q01", "Q10", "Q11",
    "Q20", "Q21", "Q30", "Q31", "R00", "R01", "R10", "R11", "R20", "R21", "R30", "R31", "X0a", "X1", "X2", "X3",
    "XY0", "Y0b", "Y1", "Y2", "Y3", "Z10", "Z11", "Z20", "Z21", "Z30", "Z31", "lats", "prep", "qry",
)
OUTER = (
    76, 75, 60, 34, 77, 65, 69, 4, 70, (1, 35), 5, 64, 23, 71, (4, 34), 13, (6, 23), 19, 7, 27, 72, (8, 21), 73,
    61, 66, (8, 53), 8, 31, (12, 53), 74, 14, 0, 37, 38, 62, 9, 54, 67, 55, 10, (22, 24), 68, 63, (22, 15), 15,
    32, 11, (25, 18), 12, 33, 39, 40, 28, 56, 20, 57, 16, 24, (35, 46), 41, 46, 29, 35, 25, 22, 26, 30, 1, 42, 21,
    48, 3, 58, 47, 2, 59, 43, 36, 52, (48, 39), 50, 6, (57, 46), 51, 49, 53, (57, 45), 44, (66, 96), 17, (69, 40),
    45, 18,
)
INNER = (
    76, 75, 34, 60, 65, 71, 69, 70, 72, 32, 31, 77, 27, 4, 73, 23, 5, (2, 53), 74, 7, (5, 23), 61, 8, 66, 9, 10,
    62, 20, 67, 14, 15, 11, 12, 64, 33, 19, 63, 37, 25, 38, 39, 40, 68, 26, 30, 16, 56, 22, 21, 13, 54, 41, 55,
    42, 29, 57, 28, 24, 0, 3, (34, 27), 58, 48, 46, 2, 1, 47, 59, 43, 35, 50, 6, 36, (50, 29), 51, (50, 49), 52,
    (52, 71), 17, 49, 53, (67, 36), 44, (68, 74), 45, (72, 53), 18,
)
CROSS = (1, 2)


def flip(value, bits):
    bit = 1
    while bit <= bits:
        if bits & bit:
            value = value + bit - 2 * bit * ((value // bit) % 2)
        bit *= 2
    return value


def here():
    ep, tp = lax.axis_index("ep"), lax.axis_index("tp")
    return ep // 2, ep % 2, tp // 2, tp % 2


def place(z, x, y, core):
    return {"ep": z * 2 + x, "tp": y * 2 + core}


def greet(partners, extra, has_extra):
    barrier = pltpu.get_barrier_semaphore()
    for partner in partners:
        pl.semaphore_signal(barrier, inc=1, device_id=partner, device_id_type=MESH)

    @pl.when(has_extra)
    def _():
        pl.semaphore_signal(barrier, inc=1, device_id=extra, device_id_type=MESH)
        pl.semaphore_wait(barrier, len(partners) + 1)

    @pl.when(jnp.logical_not(has_extra))
    def _():
        pl.semaphore_wait(barrier, len(partners))


def layer_kernel(
    width, heads,
    ffn_hbm, mix_hbm, ffn_gain_hbm, mix_gain_hbm, latent_gain_hbm, out_gain_hbm, routes_hbm, scores_hbm,
    base_hbm, step_hbm, latent_hbm, rotary_hbm, query_hbm, gate_hbm, up_hbm, down_hbm, key_hbm,
    value_hbm, output_hbm, mixed_ref, moe_ref,
    rows_all, lat_all, part_ref, work, twin_in, hop_in, direct_in, relay_in, column_in, corner_in,
    heads_ref, heads_work, heads_twin, heads_in, query_ref, keys, values, weighted, totals, attended, own_total,
    table_ref, turn_ref, ffn_ref, mix_ref,
    ffn_gain, mix_gain, latent_gain, gain_ref, routes_ref, scores_ref, base_ref, step_ref, latent_ref,
    rotary_ref, query_w, gate_ref, up_ref, down_ref, key_ref, value_ref, output_ref,
    row_send, row_recv, lat_send, lat_recv, send_sem, twin_sem, square_sem, column_sem, corner_sem, heads_sem, load_sem,
):
    f32, bf16 = jnp.float32, jnp.bfloat16
    ep, tp = lax.axis_index("ep"), lax.axis_index("tp")
    z, x, y, core = here()
    inner = ((z + 1) // 2) % 2
    planes = [z, flip(z, 1)]
    far = flip(z, 2)
    planes.append(far + inner * (1 - 2 * (far % 2)))
    planes.append(flip(planes[2], 1))
    depth = len(planes)
    x_next, y_next, twin = place(z, 1 - x, y, core), place(z, x, 1 - y, core), place(z, x, y, 1 - core)
    z_out, z_in = place(planes[1], x, y, core), place(flip(z, 3), x, y, core)
    parts, quarter = part_ref.shape[2:4]
    row_count = parts * quarter
    block_rows = 2 * row_count
    experts = 2 * depth
    half = ROPE // 2
    piece = quarter // PIECES
    first_own = pl.multiple_of(tp * quarter, quarter)
    copied = (
        (ffn_hbm.at[pl.ds(first_own, quarter)], ffn_ref), (ffn_gain_hbm, ffn_gain),
        (mix_hbm, mix_ref), (mix_gain_hbm, mix_gain), (rotary_hbm, rotary_ref),
        (base_hbm, base_ref), (step_hbm, step_ref), (routes_hbm, routes_ref), (scores_hbm, scores_ref),
        (latent_hbm, latent_ref), (latent_gain_hbm, latent_gain), (query_hbm, query_w),
        (gate_hbm, gate_ref), (up_hbm, up_ref), (down_hbm, down_ref),
        (key_hbm, key_ref), (value_hbm, value_ref), (output_hbm, output_ref), (out_gain_hbm, gain_ref),
    )
    loads = [pltpu.make_async_copy(src, dst, load_sem.at[n]) for n, (src, dst) in enumerate(copied)]
    for load in loads:
        load.start()
    waited = [0]

    def loaded(count):
        while waited[0] < count:
            loads[waited[0]].wait()
            waited[0] += 1

    greet([z_out, x_next, y_next, twin], z_in, inner == 1)
    always = None
    issued, settled, now = {}, set(), [0]

    def guarded(condition, action):
        if condition is None:
            action()
        else:
            pl.when(condition)(action)

    role = ["both"]

    def post(key, build, condition=always):
        if condition == "inner":
            if role[0] == "outer":
                return
            condition = always if role[0] == "inner" else is_inner
        issued.setdefault(key, (build, condition, now[0]))
        guarded(condition, lambda: build().start())

    numbers = {}

    def number(kind, key):
        taken = numbers.setdefault(kind, {})
        return taken.setdefault(key, len(taken))

    def at_piece(ref, g):
        return ref if g is None else ref.at[pl.ds(g * piece, piece)]

    def row_copy(origin, g, target, key):
        e, t = origin["ep"], origin["tp"]
        ref = at_piece(rows_all.at[e, t], g)
        return pltpu.make_async_remote_copy(
            src_ref=ref, dst_ref=ref, send_sem=row_send.at[number("row", key)],
            recv_sem=row_recv.at[e, t, g or 0], device_id=target, device_id_type=MESH,
        )

    def give_row(name, origin, g, target, towards, condition=always):
        key = (name, g, towards)
        post(("row",) + key, lambda: row_copy(origin, g, target, key), condition)

    def take_row(origin, g):
        row_copy(origin, g, twin, ("any",)).wait_recv()

    def lat_copy(origin, target, key):
        e, t = origin["ep"], origin["tp"]
        ref = lat_all.at[e, t]
        return pltpu.make_async_remote_copy(
            src_ref=ref, dst_ref=ref, send_sem=lat_send.at[number("lat", key)],
            recv_sem=lat_recv.at[e, t], device_id=target, device_id_type=MESH,
        )

    def give_lat(name, origin, target, towards, condition=always):
        key = (name, towards)
        post(("lat",) + key, lambda: lat_copy(origin, target, key), condition)

    def take_lat(origin):
        lat_copy(origin, twin, ("any",)).wait_recv()

    def make(src, dst, sem, target, key):
        return pltpu.make_async_remote_copy(
            src_ref=src, dst_ref=dst, send_sem=send_sem.at[number("sum", key)], recv_sem=sem,
            device_id=target, device_id_type=MESH,
        )

    def send(src, dst, sem, target, *key):
        post(("sum",) + key, lambda: make(src, dst, sem, target, key))

    def arrive(dst, sem):
        make(dst, dst, sem, twin, ("any",)).wait_recv()

    is_inner, is_outer = inner == 1, inner == 0
    up_out, up_in = z % 2 == 0, z == 1
    me = place(z, x, y, core)

    origins = {
        (s, dx, dy): place(planes[s], flip(x, dx), flip(y, dy), core)
        for s in range(depth) for dx in (0, 1) for dy in (0, 1)
    }

    def origin_of(s, dx, dy):
        return origins[s, dx, dy]

    def own_rows():
        for g in range(PIECES):
            give_row("own", me, g, z_out, "out")
            give_row("own", me, g, z_in, "in", "inner")
            give_row("own", me, g, x_next, "x")
            give_row("own", me, PIECES - 1 - g, y_next, "y")
        give_row("own", me, None, twin, "twin")

    def side_rows(first):
        by_x, by_y = origin_of(0, 1, 0), origin_of(0, 0, 1)
        for g in range(PIECES // 2):
            if first == "x":
                take_row(by_x, g)
                give_row("x0", by_x, g, y_next, "y")
            else:
                take_row(by_y, PIECES - 1 - g)
                give_row("y0", by_y, PIECES - 1 - g, x_next, "x")

    def side_rows_rest():
        by_x, by_y = origin_of(0, 1, 0), origin_of(0, 0, 1)
        for g in range(PIECES // 2):
            take_row(by_x, PIECES - 1 - g)
            take_row(by_y, g)
        give_row("x0", by_x, None, twin, "twin")
        give_row("y0", by_y, None, twin, "twin")

    def last(g):
        return g == PIECES - 1

    def corner_rows(g):
        corner = origin_of(0, 1, 1)
        take_row(corner, g)
        give_row("c0", corner, g, z_out, "out")
        give_row("c0", corner, g, z_in, "in", "inner")
        if last(g):
            give_row("c0", corner, None, twin, "twin")

    def column_rows(s, g, dx):
        origin = origin_of(s, dx, dx)
        name = f"{'zd'[dx]}{s}"
        take_row(origin, g)
        if s == 1:
            give_row(name, origin, g, z_in, "in", "inner")
        else:
            give_row(name, origin, g, z_out, "out", "inner")
        if not dx:
            give_row(name, origin, g, x_next, "x")
            give_row(name, origin, g, y_next, "y")
        if last(g):
            give_row(name, origin, None, twin, "twin")

    def square_rows(s, dx):
        origin = origin_of(s, dx, 1 - dx)
        for g in range(PIECES):
            take_row(origin, g)
        give_row(f"{'yx'[dx]}{s}", origin, None, twin, "twin")

    def own_lats():
        give_lat("own", me, z_out, "out", up_out)
        give_lat("own", me, z_in, "in", up_in)
        give_lat("own", me, x_next, "x")
        give_lat("own", me, y_next, "y")
        give_lat("own", me, twin, "twin")

    def side_lats(dx):
        origin = origin_of(0, dx, 1 - dx)
        name = f"{'yx'[dx]}0"
        take_lat(origin)
        if dx:
            give_lat(name, origin, y_next, "y")
        give_lat(name, origin, twin, "twin")

    def corner_lats():
        corner = origin_of(0, 1, 1)
        take_lat(corner)
        give_lat("c0", corner, z_out, "out", up_out)
        give_lat("c0", corner, z_in, "in", up_in)
        give_lat("c0", corner, twin, "twin")

    lower = [plane < z for plane in planes]
    up_two = z == 2

    def below(s):
        return lower[s]

    def column_lats(s, dx):
        origin = origin_of(s, dx, dx)
        name = f"{'zd'[dx]}{s}"

        @pl.when(below(s))
        def _():
            take_lat(origin)

        if s == 1:
            give_lat(name, origin, z_in, "in", up_in)
        else:
            give_lat(name, origin, z_out, "out", up_two)
        if not dx:
            give_lat(name, origin, x_next, "x", below(s))
            give_lat(name, origin, y_next, "y", below(s))
        give_lat(name, origin, twin, "twin", below(s))

    def square_lats(s, dx):
        origin = origin_of(s, dx, 1 - dx)

        @pl.when(below(s))
        def _():
            take_lat(origin)

        give_lat(f"{'yx'[dx]}{s}", origin, twin, "twin", below(s))

    def expert_plane(s):
        loaded(15)
        for a in (0, 1):
            for b in (0, 1):
                take_row(place(planes[s], flip(x, a), flip(y, b), 1 - core), None)
        pair = pl.ds(planes[s] * 2, 2)
        block = rows_all[pair, :, :, :width].reshape(block_rows, width)
        gate_part = jnp.dot(block, gate_ref[...], preferred_element_type=f32)
        up_part = jnp.dot(block, up_ref[...], preferred_element_type=f32)
        hidden = clamped_unit(gate_part, up_part).astype(bf16)
        table = rows_all[pair, :, :, width:].reshape(block_rows, 2 * ROPE)
        lane = lax.broadcasted_iota(jnp.int32, table.shape, 1)
        is_mine = (lane == ROPE + ep) | (lane == ROPE + experts + ep)
        share = jnp.sum(jnp.where(is_mine, table.astype(f32), 0.0), axis=1, keepdims=True)
        chunk = 512
        for n in range(0, width, chunk):
            out = jnp.dot(hidden, down_ref[:, n : n + chunk], preferred_element_type=f32) * share
            part_ref[s, :, :, :, n : n + chunk] = out.astype(bf16).reshape(2, parts, quarter, chunk)
        for a, b in ((1, 1), (0, 1), (1, 0), (0, 0)) if s % 2 else ((1, 1), (1, 0), (0, 1), (0, 0)):
            mine = part_ref.at[s, flip(x, a), flip(y, b) * 2 + 1 - core]
            send(mine, twin_in.at[s, a, b], twin_sem.at[s, a, b], twin, "twin", s, a, b)

    def paired(s, a, b, g=None):
        if not g:
            arrive(twin_in.at[s, a, b], twin_sem.at[s, a, b])
        rows = slice(None) if g is None else rows_of(g)
        own = part_ref[s, flip(x, a), flip(y, b) * 2 + core, rows]
        return own.astype(f32) + twin_in[s, a, b, rows].astype(f32)

    def rows_of(g):
        return pl.ds(g * piece, piece)

    def sum_pairs(s, corner):
        a, b = (1, 1) if corner else (0, 1) if s % 2 else (1, 0)
        value = paired(s, a, b)
        if corner and s == 0 and CROSS:
            for n in (1,) if role[0] == "outer" else (1, 2, 3):
                for g in range(PIECES):
                    arrive(corner_in.at[planes[n], rows_of(g)], corner_sem.at[planes[n], g])
                value = value + corner_in[planes[n]].astype(f32)
        work[s, a, b] = value.astype(bf16)
        for g in range(PIECES):
            rows = rows_of(g)
            if corner and s in CROSS:
                send(
                    work.at[s, a, b, rows], corner_in.at[z, rows], corner_sem.at[z, g],
                    place(planes[s], x, y, core), "corner", s, g,
                )
                continue
            landing, which = (hop_in, 0) if corner else (direct_in, 1)
            send(
                work.at[s, a, b, rows], landing.at[s, rows], square_sem.at[which, s, g],
                y_next if s % 2 else x_next, which, s, g,
            )

    def sum_relay(s, g):
        a, b = (1, 0) if s % 2 else (0, 1)
        rows = rows_of(g)
        value = paired(s, a, b, g)
        if s not in CROSS:
            arrive(hop_in.at[s, rows], square_sem.at[0, s, g])
            value = value + hop_in[s, rows].astype(f32)
        work[s, a, b, rows] = value.astype(bf16)
        send(
            work.at[s, a, b, rows], relay_in.at[s, rows], square_sem.at[2, s, g],
            x_next if s % 2 else y_next, 2, s, g,
        )

    def sum_square(s, g):
        rows = rows_of(g)
        value = paired(s, 0, 0, g)
        arrive(direct_in.at[s, rows], square_sem.at[1, s, g])
        value = value + direct_in[s, rows].astype(f32)
        arrive(relay_in.at[s, rows], square_sem.at[2, s, g])
        value = value + relay_in[s, rows].astype(f32)
        if s:
            work[s, 0, 0, rows] = value.astype(bf16)
            send(
                work.at[s, 0, 0, rows], column_in.at[z, rows], column_sem.at[z, g],
                place(planes[s], x, y, core), "column", s, g,
            )
        else:
            own_total[rows, :] = value

    across = (((1,), (1,)), ((), ()))
    score_scale = (NOPE + ROPE) ** (-0.5)

    def angles():
        near = base_ref[...]
        swapped = pltpu.roll(near, ROPE, 1)
        lane = lax.broadcasted_iota(jnp.int32, near.shape, 1)
        cosine, sine = jnp.where(lane < ROPE, near, swapped), jnp.where(lane < ROPE, swapped, near)
        step = jnp.broadcast_to(step_ref[pl.ds(ep, 1), :], near.shape)
        step_swapped = pltpu.roll(step, ROPE, 1)
        step_cos, step_sin = jnp.where(lane < ROPE, step, step_swapped), jnp.where(lane < ROPE, step_swapped, step)
        turn_ref[...] = jnp.where(
            lane < ROPE, cosine * step_cos - sine * step_sin, sine * step_cos + cosine * step_sin
        )

    def rotate(vectors, table):
        lane = lax.broadcasted_iota(jnp.int32, vectors.shape, 1)
        size = vectors.shape[1]
        turned = jnp.where(
            lane < half, -pltpu.roll(vectors, size - half, 1), pltpu.roll(vectors, half, 1)
        )
        sine = pltpu.roll(table, size - ROPE, 1)
        return jnp.where(lane < ROPE, vectors * table + turned * sine, 0.0)

    own = pl.ds(first_own, quarter)

    def own_normed():
        return rms_rows(mix_ref[own, :].astype(f32), mix_gain[...]).astype(bf16)

    def prepare_rows():
        loaded(9)
        rows_all[ep, tp, :, :width] = rms_rows(ffn_ref[...].astype(f32), ffn_gain[...]).astype(bf16)
        angles()
        turned = lax.dot_general(own_normed(), rotary_ref[...], across, preferred_element_type=f32)
        turned = jnp.concatenate([turned, jnp.zeros((quarter, ROPE), f32)], axis=1)
        rotary_key = rotate(turned, turn_ref[own, :])
        scores = scores_ref[...]
        shares = jnp.exp(scores - jnp.max(scores, axis=0, keepdims=True))
        shares = shares / jnp.sum(shares, axis=0, keepdims=True)
        routes = routes_ref[...]
        lane = lax.broadcasted_iota(jnp.int32, (2 * ROPE, row_count), 0)
        named = jnp.zeros((2 * ROPE, row_count), f32)
        for k in range(routes.shape[0]):
            hit = (lane == routes[k : k + 1] + ROPE) | (lane == routes[k : k + 1] + ROPE + experts)
            named = named + jnp.where(hit, shares[k : k + 1], 0.0)
        coarse = named.astype(bf16).astype(f32)
        table_ref[...] = jnp.where(lane < ROPE + experts, coarse, named - coarse).T
        rows_all[ep, tp, :, width:] = (rotary_key + table_ref[own, :]).astype(bf16)

    def prepare_lats():
        loaded(11)
        latent = jnp.dot(own_normed(), latent_ref[...], preferred_element_type=f32)
        lat_all[ep, tp] = rms_rows(latent, latent_gain[...]).astype(bf16)

    def prepare_queries():
        loaded(12)
        normed = rms_rows(mix_ref[...].astype(f32), mix_gain[...]).astype(bf16)
        for h in range(0, heads, 2):
            columns_of = slice(h * (NOPE + ROPE), (h + 2) * (NOPE + ROPE))
            two = jnp.dot(normed, query_w[:, columns_of], preferred_element_type=f32)
            table = turn_ref[...]
            middle, last = two[:, NOPE : 2 * NOPE], two[:, 2 * NOPE :]
            lane = lax.broadcasted_iota(jnp.int32, last.shape, 1)
            low, high = pltpu.roll(middle, ROPE, 1), pltpu.roll(last, ROPE, 1)
            query_ref[h, :, :NOPE] = two[:, :NOPE].astype(bf16)
            query_ref[h, :, NOPE:] = rotate(middle, table).astype(bf16)
            query_ref[h + 1, :, :NOPE] = jnp.where(lane < ROPE, low, high).astype(bf16)
            query_ref[h + 1, :, NOPE:] = rotate(high, table).astype(bf16)

    def attend_block(s):
        for a in (0, 1):
            for b in (0, 1):
                take_lat(place(planes[s], flip(x, a), flip(y, b), 1 - core))
        pair = pl.ds(planes[s] * 2, 2)
        latent = lat_all[pair].reshape(block_rows, lat_all.shape[3])
        rest = rows_all[pair, :, :, width:].reshape(block_rows, 2 * ROPE)
        key_block = jnp.dot(latent, key_ref[...], preferred_element_type=f32).astype(bf16)
        value_block = jnp.dot(latent, value_ref[...], preferred_element_type=f32).astype(bf16)
        for h in range(heads):
            keys[h, :, :NOPE] = key_block[:, h * NOPE : (h + 1) * NOPE]
            keys[h, :, NOPE:] = rest
            values[h] = value_block[:, h * VD : (h + 1) * VD]
        shape = (row_count, block_rows)
        places = lax.broadcasted_iota(jnp.int32, shape, 0) + ep * row_count
        allowed = lax.broadcasted_iota(jnp.int32, shape, 1) + planes[s] * block_rows <= places
        for h in range(heads):
            scores = lax.dot_general(query_ref[h], keys[h], across, preferred_element_type=f32)
            weights = jnp.where(allowed, jnp.exp(scores * score_scale), 0.0)
            total = jnp.broadcast_to(jnp.sum(weights, axis=1, keepdims=True), (row_count, VD))
            update = jnp.dot(weights.astype(bf16), values[h], preferred_element_type=f32)
            totals[h] = total if s == 0 else totals[h] + total
            weighted[h] = update if s == 0 else weighted[h] + update

    def attend_plane(s):
        loaded(17)
        if s == 0:
            attend_block(s)
        else:
            pl.when(below(s))(lambda: attend_block(s))

    def project():
        loaded(18)
        for h in range(heads):
            attended[:, h * VD : (h + 1) * VD] = (weighted[h] / totals[h]).astype(bf16)
        chunk = 512
        for n in range(0, width, chunk):
            out = jnp.dot(attended[...], output_ref[:, n : n + chunk], preferred_element_type=f32)
            heads_ref[:, :, n : n + chunk] = out.astype(bf16).reshape(parts, quarter, chunk)
        for b in (1, 0):
            send(
                heads_ref.at[flip(y, b) * 2 + 1 - core], heads_twin.at[b], heads_sem.at[b], twin,
                "heads", b,
            )

    def cross_heads():
        arrive(heads_twin.at[1], heads_sem.at[1])
        heads_work[...] = (
            heads_ref[(1 - y) * 2 + core].astype(f32) + heads_twin[1].astype(f32)
        ).astype(bf16)
        send(heads_work, heads_in, heads_sem.at[2], y_next, "heads", 2)

    def finish_heads():
        loaded(len(loads))
        arrive(heads_twin.at[0], heads_sem.at[0])
        arrive(heads_in, heads_sem.at[2])
        projected = (
            heads_ref[y * 2 + core].astype(f32) + heads_twin[0].astype(f32) + heads_in[...].astype(f32)
        )
        mixed_ref[...] = rms_rows(projected, gain_ref[...]).astype(bf16)

    def finish_moe():
        for g in range(PIECES):
            rows = rows_of(g)
            total = own_total[rows, :]
            for s in range(1, depth):
                arrive(column_in.at[planes[s], rows], column_sem.at[planes[s], g])
                total = total + column_in[planes[s], rows].astype(f32)
            moe_ref[rows, :] = total.astype(bf16)

    def start_rows():
        prepare_rows()
        own_rows()

    steps = {
        "prep": start_rows, "lats": prepare_lats, "qry": prepare_queries, "Lown": own_lats,
        "X0a": lambda: side_rows("x"), "Y0b": lambda: side_rows("y"), "XY0": side_rows_rest,
        "C00": lambda: corner_rows(0), "C01": lambda: corner_rows(1),
        "LX0": lambda: side_lats(1), "LY0": lambda: side_lats(0), "LC0": corner_lats,
        "PR": project, "CH": cross_heads, "FH": finish_heads, "FM": finish_moe,
    }
    kinds = {
        "Z": lambda s, g: column_rows(s, g, 0), "D": lambda s, g: column_rows(s, g, 1),
        "X": lambda s: square_rows(s, 1), "Y": lambda s: square_rows(s, 0),
        "LZ": lambda s: column_lats(s, 0), "LD": lambda s: column_lats(s, 1),
        "LX": lambda s: square_lats(s, 1), "LY": lambda s: square_lats(s, 0),
        "E": expert_plane, "A": attend_plane, "R": sum_relay, "Q": sum_square,
    }

    def run(step):
        if step in steps:
            steps[step]()
        elif step[0] == "P":
            sum_pairs(int(step[1]), step[2] == "a")
        else:
            kind = step.rstrip("0123456789")
            kinds[kind](*(int(digit) for digit in step[len(kind) :]))

    def settle(until, most):
        ready = [k for k, (_, _, step) in issued.items() if k not in settled and step <= until]
        for key in ready[:most]:
            build, condition, _ = issued[key]
            guarded(condition, lambda: build().wait_send())
            settled.add(key)

    def walk(order):
        for step in order:
            if isinstance(step, tuple):
                settle(*step)
            else:
                run(NAMES[step])
                now[0] += 1

    orders = (OUTER, INNER)
    shared = 0
    while orders[0][shared] == orders[1][shared]:
        shared += 1
    walk(orders[0][:shared])
    ready, sent, step_now, done = waited[0], dict(issued), now[0], set(settled)
    for name, chosen, order in (("outer", is_outer, orders[0]), ("inner", is_inner, orders[1])):
        role[0], waited[0], now[0] = name, ready, step_now
        issued.clear()
        issued.update(sent)
        settled.clear()
        settled.update(done)

        @pl.when(chosen)
        def _():
            walk(order[shared:])
            settle(now[0], len(issued))


def scoped_kernel(width, heads, sems, *refs):
    pl.run_scoped(lambda *held: layer_kernel(width, heads, *refs, *held), *sems)


def turn_tables(row_count, experts):
    inverse = rope_base ** (-np.arange(0, ROPE, 2) / ROPE)
    near, far = np.arange(row_count)[:, None] * inverse, row_count * np.arange(experts)[:, None] * inverse

    def lanes(angle):
        return np.concatenate([np.cos(angle)] * 2 + [np.sin(angle)] * 2, axis=1).astype(np.float32)

    return lanes(near), lanes(far)


def dense_local(
    mix_in, mix_gain, query_weight, latent_weight, rotary_weight, latent_gain, key_weight,
    value_weight, output_weight, out_gain, ffn_in, ffn_gain, gate_weight, up_weight, down_weight,
    routes, route_scores,
):
    experts, parts = lax.axis_size("ep"), lax.axis_size("tp")
    row_count, width = mix_in.shape
    quarter, depth = row_count // parts, experts // 2
    block_rows = 2 * row_count
    heads = query_weight.shape[1] // (NOPE + ROPE)
    base, step = turn_tables(row_count, experts)
    row = lambda gain: gain.reshape(1, -1)
    operands = (
        ffn_in, mix_in, row(ffn_gain), row(mix_gain), row(latent_gain), row(out_gain), routes.T,
        route_scores.T, jnp.asarray(base), jnp.asarray(step), latent_weight, rotary_weight.T, query_weight,
        gate_weight[0], up_weight[0], down_weight[0], key_weight, value_weight, output_weight,
    )
    held = lambda *lead: pltpu.VMEM(lead + (quarter, width), jnp.bfloat16)
    scratch = lambda *shape: pltpu.VMEM(shape, jnp.bfloat16)
    wide = lambda *shape: pltpu.VMEM(shape, jnp.float32)
    sems = lambda *shape: pltpu.SemaphoreType.DMA(shape)
    semaphores = (
        sems(96), sems(experts, parts, PIECES), sems(48), sems(experts, parts), sems(64),
        sems(depth, 2, 2), sems(3, depth, PIECES), sems(depth, PIECES), sems(depth, PIECES), sems(3),
        sems(len(operands)),
        )
    return pl.pallas_call(
        functools.partial(scoped_kernel, width, heads, semaphores),
        out_shape=[pltpu.VMEM((quarter, width), jnp.bfloat16)] * 2,
        in_specs=[pl.BlockSpec(memory_space=pl.ANY)] * len(operands),
        out_specs=[pl.BlockSpec(memory_space=pltpu.VMEM)] * 2,
        scratch_shapes=[
            scratch(experts, parts, quarter, width + 2 * ROPE),
            scratch(experts, parts, quarter, latent_weight.shape[1]),
            held(depth, 2, parts), held(depth, 2, 2), held(depth, 2, 2),
            held(depth), held(depth), held(depth), held(depth), held(depth),
            held(parts), held(), held(2), held(),
            scratch(heads, row_count, NOPE + 2 * ROPE), scratch(heads, block_rows, NOPE + 2 * ROPE),
            scratch(heads, block_rows, VD), wide(heads, row_count, VD), wide(heads, row_count, VD),
            scratch(row_count, heads * VD), wide(quarter, width),
            wide(row_count, 2 * ROPE), wide(row_count, 2 * ROPE),
            pltpu.VMEM((quarter, width), ffn_in.dtype), pltpu.VMEM(mix_in.shape, mix_in.dtype),
        ]
        + [pltpu.VMEM(a.shape, a.dtype) for a in operands[2:]],
        compiler_params=pltpu.CompilerParams(
            collective_id=0, has_side_effects=True, vmem_limit_bytes=60 * 1024 * 1024
        ),
        name="layer",
    )(*operands)


def solution(mesh):
    experts, parts = mesh.shape["ep"], mesh.shape["tp"]

    def body(*args):
        quarter, choose = args[10].shape[0] // parts, args[15].shape[1]
        every_row = 2 * quarter * choose >= quarter * experts
        paired = parts == 4 and experts == 8 and quarter % (16 * PIECES) == 0
        return (dense_local if every_row and paired else local)(*args)
    placed = (
        P("ep", None),
        P(),
        P(None, "tp"),
        P(),
        P(),
        P(),
        P(None, "tp"),
        P(None, "tp"),
        P("tp", None),
        P(),
        P("ep", None),
        P(),
        P("ep", None, "tp"),
        P("ep", None, "tp"),
        P("ep", "tp", None),
        P("ep", None),
        P("ep", None),
    )
    return jax.shard_map(
        body,
        mesh=mesh,
        in_specs=placed,
        out_specs=(P(("ep", "tp"), None), P(("ep", "tp"), None)),
        check_vma=False,
    )
```

```python
import jax
import jax.numpy as jnp
import functools
import numpy as np
from jax import lax
from jax.experimental import pallas as pl
from jax.experimental.pallas import tpu as pltpu
from jax.sharding import PartitionSpec as P

NOPE = 128
ROPE = 64
VD = 128


norm_eps = 1e-06
clamp_limit = 7.0
gate_slope = 1.702
rope_base = 10000.0


def rms_rows(rows_in, scales):
    mean_square = jnp.mean(rows_in * rows_in, axis=-1, keepdims=True)
    return rows_in * lax.rsqrt(mean_square + norm_eps) * scales


def rms_columns(columns, scales):
    mean_square = jnp.mean(columns * columns, axis=0, keepdims=True)
    return columns * lax.rsqrt(mean_square + norm_eps) * scales[:, None]


def turn_table(positions):
    inverse = rope_base ** (-jnp.arange(0, ROPE, 2).astype(jnp.float32) / ROPE)
    angle_rows = inverse[:, None] * positions.astype(jnp.float32)[None, :]
    return (jnp.cos(angle_rows), jnp.sin(angle_rows))


def clamped_unit(gate_part, linear):
    gate_part = jnp.minimum(gate_part, clamp_limit)
    linear = jnp.clip(linear, -clamp_limit, clamp_limit)
    return gate_part * jax.nn.sigmoid(gate_slope * gate_part) * (linear + 1.0)


def keep_state(running):
    return running


def local(
    mix_in,
    mix_gain,
    query_weight,
    latent_weight,
    rotary_weight,
    latent_gain,
    key_weight,
    value_weight,
    output_weight,
    out_gain,
    ffn_in,
    ffn_gain,
    gate_weight,
    up_weight,
    down_weight,
    routes,
    route_scores,
):
    row_count = mix_in.shape[0]
    first_row = lax.axis_index("ep") * row_count
    last_row = first_row + row_count - 1
    positions = first_row + jnp.arange(row_count, dtype=jnp.int32)
    normed = rms_rows(mix_in.astype(jnp.float32), mix_gain).astype(jnp.bfloat16)
    head_count = query_weight.shape[1] // (NOPE + ROPE)
    half_rope = ROPE // 2
    cosine, sine_rows = turn_table(positions)
    queries = jnp.dot(normed, query_weight, preferred_element_type=jnp.float32).reshape(
        row_count, head_count, NOPE + ROPE
    )
    query_plain = queries[..., :NOPE].astype(jnp.bfloat16)
    query_cos = cosine.T[:, None, :]
    query_sin = sine_rows.T[:, None, :]
    query_upper = queries[..., NOPE : NOPE + half_rope]
    query_lower = queries[..., NOPE + half_rope :]
    query_turn = jnp.concatenate(
        [
            query_upper * query_cos - query_lower * query_sin,
            query_lower * query_cos + query_upper * query_sin,
        ],
        axis=-1,
    ).astype(jnp.bfloat16)
    across = (((0,), (1,)), ((), ()))
    latent = rms_columns(
        lax.dot_general(latent_weight, normed, across, preferred_element_type=jnp.float32),
        latent_gain,
    ).astype(jnp.bfloat16)
    rot_raw = lax.dot_general(rotary_weight, normed, across, preferred_element_type=jnp.float32)
    rotary_key = jnp.concatenate(
        [
            rot_raw[:half_rope] * cosine - rot_raw[half_rope:] * sine_rows,
            rot_raw[half_rope:] * cosine + rot_raw[:half_rope] * sine_rows,
        ],
        axis=0,
    ).astype(jnp.bfloat16)
    score_scale = (NOPE + ROPE) ** (-0.5)
    contract_first = (((0,), (0,)), ((), ()))

    def expand(latent_block):
        key_block = lax.dot_general(
            key_weight, latent_block, contract_first, preferred_element_type=jnp.float32
        ).astype(jnp.bfloat16)
        value_block = lax.dot_general(
            value_weight, latent_block, contract_first, preferred_element_type=jnp.float32
        ).astype(jnp.bfloat16)
        return (key_block, value_block)

    def attend(key_block, value_block, turn_block):
        key_count = key_block.shape[1]
        key_block = key_block.reshape(head_count, NOPE, key_count)
        value_block = value_block.reshape(head_count, VD, key_count)
        scores = jnp.einsum(
            "ihd,hdj->hij", query_plain, key_block, preferred_element_type=jnp.float32
        )
        scores = scores + jnp.einsum(
            "ihd,dj->hij", query_turn, turn_block, preferred_element_type=jnp.float32
        )
        key_places = jnp.arange(key_count, dtype=jnp.int32)
        allowed = key_places[None, :] <= positions[:, None]
        weights = jnp.where(allowed[None], jnp.exp(scores * score_scale), 0.0)
        weighted = jnp.einsum(
            "hij,hdj->hid",
            weights.astype(jnp.bfloat16),
            value_block,
            preferred_element_type=jnp.float32,
        )
        return (jnp.sum(weights, axis=-1), weighted)

    initial = (
        jnp.zeros((head_count, row_count), jnp.float32),
        jnp.zeros((head_count, row_count, VD), jnp.float32),
    )
    shard_piece = (
        lax.all_gather(latent, "ep", axis=1, tiled=True),
        lax.all_gather(rotary_key, "ep", axis=1, tiled=True),
    )

    def compute_piece(running):
        key_block, value_block = expand(shard_piece[0])
        return attend(key_block, value_block, shard_piece[1])

    totals, weighted = lax.cond(jnp.int32(0) > last_row, keep_state, compute_piece, initial)
    attended = (weighted / totals[..., None]).astype(jnp.bfloat16)
    mixing = output_weight.reshape(head_count, VD, output_weight.shape[1])
    partial_value = jnp.einsum("hid,hde->ie", attended, mixing, preferred_element_type=jnp.float32)
    projected = lax.psum_scatter(
        lax.optimization_barrier(partial_value.astype(jnp.bfloat16))
        .astype(jnp.float32)
        .astype(jnp.bfloat16),
        "tp",
        scatter_dimension=0,
        tiled=True,
    ).astype(jnp.float32)
    mixed = rms_rows(projected, out_gain).astype(jnp.bfloat16)
    tokens = ffn_in.shape[0]
    part_count = lax.axis_size("tp")
    quarter_rows = tokens // part_count
    experts = lax.axis_size("ep")
    choose = routes.shape[1]
    capacity = max(2, 2 * quarter_rows * choose // experts)
    slot_count = capacity * part_count
    tp_index = lax.axis_index("tp")
    normed_b = rms_rows(ffn_in.astype(jnp.float32), ffn_gain).astype(jnp.bfloat16)
    padded = jnp.concatenate([normed_b, jnp.zeros((1, normed_b.shape[1]), jnp.bfloat16)], axis=0)
    gate_share = jax.nn.softmax(route_scores, axis=-1)
    grouped = routes.reshape(part_count, quarter_rows * choose)
    onehot = (grouped[:, :, None] == jnp.arange(experts, dtype=jnp.int32)[None, None, :]).astype(
        jnp.int32
    )
    slot_rank = jnp.sum((jnp.cumsum(onehot, axis=1) - 1) * onehot, axis=2)
    slot_index = jnp.arange(part_count, dtype=jnp.int32)[:, None] * capacity + slot_rank
    place_index = (slot_index * experts + grouped).reshape(-1)
    owners = jnp.arange(tokens * choose, dtype=jnp.int32) // choose
    slot_token = jnp.full((slot_count * experts,), tokens, jnp.int32).at[place_index].set(owners)
    unit_count = gate_weight.shape[2]
    chosen = lax.dynamic_slice_in_dim(
        slot_token, tp_index * capacity * experts, capacity * experts, 0
    )
    outgoing = padded[chosen].reshape(capacity, experts, -1)
    arrived = lax.all_to_all(outgoing, "ep", split_axis=1, concat_axis=1, tiled=True)
    row_block = lax.all_gather(arrived, "tp", axis=0, tiled=True)
    block_slots = row_block.shape[0]
    flat_rows = row_block.reshape(-1, row_block.shape[2])
    gate_part = jnp.dot(flat_rows, gate_weight[0], preferred_element_type=jnp.float32)
    up_part = jnp.dot(flat_rows, up_weight[0], preferred_element_type=jnp.float32)
    hidden = (
        clamped_unit(gate_part, up_part).astype(jnp.bfloat16).reshape(block_slots, -1, unit_count)
    )
    sources = hidden.shape[1]
    hidden_flat = hidden.reshape(slot_count * sources, unit_count)
    partial_value = jnp.dot(hidden_flat, down_weight[0], preferred_element_type=jnp.float32)
    result = lax.psum_scatter(
        lax.optimization_barrier(partial_value.astype(jnp.bfloat16))
        .astype(jnp.float32)
        .astype(jnp.bfloat16),
        "tp",
        scatter_dimension=0,
        tiled=True,
    )
    result = result.reshape(capacity, sources, -1)
    returned = lax.all_to_all(result, "ep", split_axis=1, concat_axis=1, tiled=True)
    back_rows = returned.reshape(capacity * experts, -1)
    own_rank = lax.dynamic_index_in_dim(slot_rank, tp_index, 0, keepdims=False)
    own_expert = lax.dynamic_index_in_dim(grouped, tp_index, 0, keepdims=False)
    picked = (
        back_rows[own_rank * experts + own_expert]
        .astype(jnp.float32)
        .reshape(quarter_rows, choose, -1)
    )
    own_gates = lax.dynamic_slice_in_dim(gate_share, tp_index * quarter_rows, quarter_rows, 0)
    moe_out = jnp.sum(picked * own_gates[:, :, None], axis=1).astype(jnp.bfloat16)
    return (mixed, moe_out)


MESH = pl.DeviceIdType.MESH
PIECES = 4
NAMES = (
    "A0", "A1", "A2", "A3", "C00", "C01", "C02", "C03", "CH", "D10", "D11", "D12", "D13", "D20", "D21", "D22",
    "D23", "D30", "D31", "D32", "D33", "E0", "E1", "E2", "E3", "FH", "FM", "LC0", "LD1", "LD2", "LD3", "LX0",
    "LX1", "LX2", "LX3", "LY0", "LY1", "LY2", "LY3", "LZ1", "LZ2", "LZ3", "Lown", "P0a", "P0b", "P1a", "P1b",
    "P2a", "P2b", "P3a", "P3b", "PR", "Q00", "Q01", "Q02", "Q03", "Q10", "Q11", "Q12", "Q13", "Q20", "Q21", "Q22",
    "Q23", "Q30", "Q31", "Q32", "Q33", "R00", "R01", "R02", "R03", "R10", "R11", "R12", "R13", "R20", "R21",
    "R22", "R23", "R30", "R31", "R32", "R33", "X0a", "X1", "X2", "X3", "XY0", "Y0b", "Y1", "Y2", "Y3", "Z10",
    "Z11", "Z12", "Z13", "Z20", "Z21", "Z22", "Z23", "Z30", "Z31", "Z32", "Z33", "lats", "prep", "qry",
)
OUTER = (
    106, 105, 42, 89, 84, 93, 94, 95, 96, 4, 31, (2, 22), 5, 6, 7, 35, (2, 111), 90, 97, 98, (7, 19), 27, 9, 10,
    88, 99, 100, 40, 101, (12, 23), 102, 107, 39, 85, 11, 12, (16, 23), 103, (21, 17), 22, 104, 91, (23, 45), 45,
    13, 86, 14, 15, 37, 46, 72, 73, 74, 16, 75, 21, 87, 92, 23, 17, 18, 19, 20, 41, 47, 48, 76, 77, 33, 78, 79,
    36, 32, 24, (50, 47), 49, 43, 50, 34, 60, 28, 61, 0, 62, 63, 30, 29, 56, 57, 38, 58, 59, 1, 80, 81, 3, 82, 83,
    44, 68, 2, 69, 51, 70, 64, 65, (68, 13), 8, 66, 67, 71, (68, 182), 25, 52, 53, 54, 55, 26,
)
INNER = (
    106, 105, 42, 84, 89, 97, 93, 98, 99, 94, 100, 95, 107, 96, 40, 4, (2, 21), 5, 101, 102, 6, 31, 7, (2, 46), 9,
    (6, 23), 10, 88, 103, 104, 13, (7, 18), 11, (8, 21), 86, 14, 91, 12, 15, 16, (10, 33), 90, 39, 35, 85, 23, 17,
    18, 22, 47, 87, 19, 20, 33, 41, 45, 32, 37, 92, 48, 28, 46, 21, 36, 27, 24, 34, (40, 45), 49, 72, 73, 76, 30,
    50, 29, 74, 38, 75, 77, 0, 56, (48, 20), 57, 3, 78, 79, 1, 80, 58, 59, 81, 82, 83, 2, 51, (60, 14), 64, 8, 65,
    43, 66, 60, (65, 18), 67, 44, (70, 32), 68, (75, 21), 69, (76, 21), 70, (87, 21), 71, 61, 62, (87, 50), 52,
    (87, 20), 53, 25, 63, 54, (93, 20), 55, (96, 20), 26,
)
CROSS = (1, 2)


def flip(value, bits):
    bit = 1
    while bit <= bits:
        if bits & bit:
            value = value + bit - 2 * bit * ((value // bit) % 2)
        bit *= 2
    return value


def here():
    ep, tp = lax.axis_index("ep"), lax.axis_index("tp")
    return ep // 2, ep % 2, tp // 2, tp % 2


def place(z, x, y, core):
    return {"ep": z * 2 + x, "tp": y * 2 + core}


def greet(partners, extra, has_extra):
    barrier = pltpu.get_barrier_semaphore()
    for partner in partners:
        pl.semaphore_signal(barrier, inc=1, device_id=partner, device_id_type=MESH)

    @pl.when(has_extra)
    def _():
        pl.semaphore_signal(barrier, inc=1, device_id=extra, device_id_type=MESH)

    def wait():
        @pl.when(has_extra)
        def _():
            pl.semaphore_wait(barrier, len(partners) + 1)

        @pl.when(jnp.logical_not(has_extra))
        def _():
            pl.semaphore_wait(barrier, len(partners))

    return wait


def layer_kernel(
    width, heads,
    ffn_hbm, mix_hbm, ffn_gain_hbm, mix_gain_hbm, latent_gain_hbm, out_gain_hbm, routes_hbm, scores_hbm,
    base_hbm, step_hbm, latent_hbm, rotary_hbm, query_hbm, gate_hbm, up_hbm, down_hbm, key_hbm,
    value_hbm, output_hbm, out_ref,
    rows_all, lat_all, part_ref, work, twin_in, hop_in, direct_in, relay_in, column_in, corner_in,
    heads_ref, heads_work, heads_twin, heads_in, query_ref, keys, values, weighted, totals, attended, own_total,
    table_ref, turn_ref, ffn_ref, mix_ref,
    ffn_gain, mix_gain, latent_gain, gain_ref, routes_ref, scores_ref, base_ref, step_ref, latent_ref,
    rotary_ref, query_w, gate_ref, up_ref, down_ref, key_ref, value_ref, output_ref,
    row_send, row_recv, lat_send, lat_recv, send_sem, twin_sem, square_sem, column_sem, corner_sem, heads_sem, load_sem,
):
    f32, bf16 = jnp.float32, jnp.bfloat16
    ep, tp = lax.axis_index("ep"), lax.axis_index("tp")
    z, x, y, core = here()
    inner = ((z + 1) // 2) % 2
    planes = [z, flip(z, 1)]
    far = flip(z, 2)
    planes.append(far + inner * (1 - 2 * (far % 2)))
    planes.append(flip(planes[2], 1))
    depth = len(planes)
    x_next, y_next, twin = place(z, 1 - x, y, core), place(z, x, 1 - y, core), place(z, x, y, 1 - core)
    z_out, z_in = place(planes[1], x, y, core), place(flip(z, 3), x, y, core)
    parts, quarter = part_ref.shape[2:4]
    row_count = parts * quarter
    block_rows = 2 * row_count
    experts = 2 * depth
    half = ROPE // 2
    piece = quarter // PIECES
    first_own = pl.multiple_of(tp * quarter, quarter)
    copied = (
        (ffn_hbm.at[pl.ds(first_own, quarter)], ffn_ref), (ffn_gain_hbm, ffn_gain),
        (mix_hbm, mix_ref), (mix_gain_hbm, mix_gain), (rotary_hbm, rotary_ref),
        (base_hbm, base_ref), (step_hbm, step_ref), (routes_hbm, routes_ref), (scores_hbm, scores_ref),
        (latent_hbm, latent_ref), (latent_gain_hbm, latent_gain), (query_hbm, query_w),
        (gate_hbm, gate_ref), (up_hbm, up_ref), (down_hbm, down_ref),
        (key_hbm, key_ref), (value_hbm, value_ref), (output_hbm, output_ref), (out_gain_hbm, gain_ref),
    )
    loads = [pltpu.make_async_copy(src, dst, load_sem.at[n]) for n, (src, dst) in enumerate(copied)]
    greeted = greet([z_out, x_next, y_next, twin], z_in, inner == 1)
    early = 11
    for load in loads[:early]:
        load.start()
    waited = [0]

    def loaded(count):
        while waited[0] < count:
            loads[waited[0]].wait()
            waited[0] += 1

    always = None
    issued, settled, now = {}, set(), [0]

    def guarded(condition, action):
        if condition is None:
            action()
        else:
            pl.when(condition)(action)

    role = ["both"]

    def post(key, build, condition=always):
        if condition == "inner":
            if role[0] == "outer":
                return
            condition = always if role[0] == "inner" else is_inner
        issued.setdefault(key, (build, condition, now[0]))
        guarded(condition, lambda: build().start())

    numbers = {}

    def number(kind, key):
        taken = numbers.setdefault(kind, {})
        return taken.setdefault(key, len(taken))

    def at_piece(ref, g):
        return ref if g is None else ref.at[pl.ds(g * piece, piece)]

    def row_copy(origin, g, target, key):
        e, t = origin["ep"], origin["tp"]
        ref = at_piece(rows_all.at[e, t], g)
        return pltpu.make_async_remote_copy(
            src_ref=ref, dst_ref=ref, send_sem=row_send.at[number("row", key)],
            recv_sem=row_recv.at[e, t, g or 0], device_id=target, device_id_type=MESH,
        )

    def give_row(name, origin, g, target, towards, condition=always):
        key = (name, g, towards)
        post(("row",) + key, lambda: row_copy(origin, g, target, key), condition)

    def take_row(origin, g):
        row_copy(origin, g, twin, ("any",)).wait_recv()

    def lat_copy(origin, target, key):
        e, t = origin["ep"], origin["tp"]
        ref = lat_all.at[e, t]
        return pltpu.make_async_remote_copy(
            src_ref=ref, dst_ref=ref, send_sem=lat_send.at[number("lat", key)],
            recv_sem=lat_recv.at[e, t], device_id=target, device_id_type=MESH,
        )

    def give_lat(name, origin, target, towards, condition=always):
        key = (name, towards)
        post(("lat",) + key, lambda: lat_copy(origin, target, key), condition)

    def take_lat(origin):
        lat_copy(origin, twin, ("any",)).wait_recv()

    def make(src, dst, sem, target, key):
        return pltpu.make_async_remote_copy(
            src_ref=src, dst_ref=dst, send_sem=send_sem.at[number("sum", key)], recv_sem=sem,
            device_id=target, device_id_type=MESH,
        )

    def send(src, dst, sem, target, *key):
        post(("sum",) + key, lambda: make(src, dst, sem, target, key))

    def arrive(dst, sem):
        make(dst, dst, sem, twin, ("any",)).wait_recv()

    is_inner, is_outer = inner == 1, inner == 0
    up_out, up_in = z % 2 == 0, z == 1
    me = place(z, x, y, core)

    origins = {
        (s, dx, dy): place(planes[s], flip(x, dx), flip(y, dy), core)
        for s in range(depth) for dx in (0, 1) for dy in (0, 1)
    }

    def origin_of(s, dx, dy):
        return origins[s, dx, dy]

    def own_rows():
        for g in range(PIECES):
            give_row("own", me, g, z_out, "out")
            give_row("own", me, g, z_in, "in", "inner")
            give_row("own", me, g, x_next, "x")
            give_row("own", me, PIECES - 1 - g, y_next, "y")
        give_row("own", me, None, twin, "twin")

    def side_rows(first):
        by_x, by_y = origin_of(0, 1, 0), origin_of(0, 0, 1)
        for g in range(PIECES // 2):
            if first == "x":
                take_row(by_x, g)
                give_row("x0", by_x, g, y_next, "y")
            else:
                take_row(by_y, PIECES - 1 - g)
                give_row("y0", by_y, PIECES - 1 - g, x_next, "x")

    def side_rows_rest():
        by_x, by_y = origin_of(0, 1, 0), origin_of(0, 0, 1)
        for g in range(PIECES // 2):
            take_row(by_x, PIECES - 1 - g)
            take_row(by_y, g)
        give_row("x0", by_x, None, twin, "twin")
        give_row("y0", by_y, None, twin, "twin")

    def last(g):
        return g == PIECES - 1

    def corner_rows(g):
        corner = origin_of(0, 1, 1)
        take_row(corner, g)
        give_row("c0", corner, g, z_out, "out")
        give_row("c0", corner, g, z_in, "in", "inner")
        if last(g):
            give_row("c0", corner, None, twin, "twin")

    def column_rows(s, g, dx):
        origin = origin_of(s, dx, dx)
        name = f"{'zd'[dx]}{s}"
        take_row(origin, g)
        if s == 1:
            give_row(name, origin, g, z_in, "in", "inner")
        else:
            give_row(name, origin, g, z_out, "out", "inner")
        if not dx:
            give_row(name, origin, g, x_next, "x")
            give_row(name, origin, g, y_next, "y")
        if last(g):
            give_row(name, origin, None, twin, "twin")

    def square_rows(s, dx):
        origin = origin_of(s, dx, 1 - dx)
        for g in range(PIECES):
            take_row(origin, g)
        give_row(f"{'yx'[dx]}{s}", origin, None, twin, "twin")

    def own_lats():
        give_lat("own", me, z_out, "out", up_out)
        give_lat("own", me, z_in, "in", up_in)
        give_lat("own", me, x_next, "x")
        give_lat("own", me, y_next, "y")
        give_lat("own", me, twin, "twin")

    def side_lats(dx):
        origin = origin_of(0, dx, 1 - dx)
        name = f"{'yx'[dx]}0"
        take_lat(origin)
        if dx:
            give_lat(name, origin, y_next, "y")
        give_lat(name, origin, twin, "twin")

    def corner_lats():
        corner = origin_of(0, 1, 1)
        take_lat(corner)
        give_lat("c0", corner, z_out, "out", up_out)
        give_lat("c0", corner, z_in, "in", up_in)
        give_lat("c0", corner, twin, "twin")

    lower = [plane < z for plane in planes]
    up_two = z == 2

    def below(s):
        return lower[s]

    def column_lats(s, dx):
        origin = origin_of(s, dx, dx)
        name = f"{'zd'[dx]}{s}"

        @pl.when(below(s))
        def _():
            take_lat(origin)

        if s == 1:
            give_lat(name, origin, z_in, "in", up_in)
        else:
            give_lat(name, origin, z_out, "out", up_two)
        if not dx:
            give_lat(name, origin, x_next, "x", below(s))
            give_lat(name, origin, y_next, "y", below(s))
        give_lat(name, origin, twin, "twin", below(s))

    def square_lats(s, dx):
        origin = origin_of(s, dx, 1 - dx)

        @pl.when(below(s))
        def _():
            take_lat(origin)

        give_lat(f"{'yx'[dx]}{s}", origin, twin, "twin", below(s))

    def expert_plane(s):
        loaded(15)
        for a in (0, 1):
            for b in (0, 1):
                take_row(place(planes[s], flip(x, a), flip(y, b), 1 - core), None)
        pair = pl.ds(planes[s] * 2, 2)
        block = rows_all[pair, :, :, :width].reshape(block_rows, width)
        gate_part = jnp.dot(block, gate_ref[...], preferred_element_type=f32)
        up_part = jnp.dot(block, up_ref[...], preferred_element_type=f32)
        hidden = clamped_unit(gate_part, up_part).astype(bf16)
        table = rows_all[pair, :, :, width:].reshape(block_rows, 2 * ROPE)
        lane = lax.broadcasted_iota(jnp.int32, table.shape, 1)
        is_mine = (lane == ROPE + ep) | (lane == ROPE + experts + ep)
        share = jnp.sum(jnp.where(is_mine, table.astype(f32), 0.0), axis=1, keepdims=True)
        chunk = 512
        for n in range(0, width, chunk):
            out = jnp.dot(hidden, down_ref[:, n : n + chunk], preferred_element_type=f32) * share
            part_ref[s, :, :, :, n : n + chunk] = out.astype(bf16).reshape(2, parts, quarter, chunk)
        for a, b in ((1, 1), (0, 1), (1, 0), (0, 0)) if s % 2 else ((1, 1), (1, 0), (0, 1), (0, 0)):
            mine = part_ref.at[s, flip(x, a), flip(y, b) * 2 + 1 - core]
            send(mine, twin_in.at[s, a, b], twin_sem.at[s, a, b], twin, "twin", s, a, b)

    def paired(s, a, b, g=None):
        if not g:
            arrive(twin_in.at[s, a, b], twin_sem.at[s, a, b])
        rows = slice(None) if g is None else rows_of(g)
        own = part_ref[s, flip(x, a), flip(y, b) * 2 + core, rows]
        return own.astype(f32) + twin_in[s, a, b, rows].astype(f32)

    def rows_of(g):
        return pl.ds(g * piece, piece)

    def sum_pairs(s, corner):
        a, b = (1, 1) if corner else (0, 1) if s % 2 else (1, 0)
        value = paired(s, a, b)
        if corner and s == 0 and CROSS:
            for n in (1,) if role[0] == "outer" else (1, 2, 3):
                for g in range(PIECES):
                    arrive(corner_in.at[planes[n], rows_of(g)], corner_sem.at[planes[n], g])
                value = value + corner_in[planes[n]].astype(f32)
        work[s, a, b] = value.astype(bf16)
        for g in range(PIECES):
            rows = rows_of(g)
            if corner and s in CROSS:
                send(
                    work.at[s, a, b, rows], corner_in.at[z, rows], corner_sem.at[z, g],
                    place(planes[s], x, y, core), "corner", s, g,
                )
                continue
            landing, which = (hop_in, 0) if corner else (direct_in, 1)
            send(
                work.at[s, a, b, rows], landing.at[s, rows], square_sem.at[which, s, g],
                y_next if s % 2 else x_next, which, s, g,
            )

    def sum_relay(s, g):
        a, b = (1, 0) if s % 2 else (0, 1)
        rows = rows_of(g)
        value = paired(s, a, b, g)
        if s not in CROSS:
            arrive(hop_in.at[s, rows], square_sem.at[0, s, g])
            value = value + hop_in[s, rows].astype(f32)
        work[s, a, b, rows] = value.astype(bf16)
        send(
            work.at[s, a, b, rows], relay_in.at[s, rows], square_sem.at[2, s, g],
            x_next if s % 2 else y_next, 2, s, g,
        )

    def sum_square(s, g):
        rows = rows_of(g)
        value = paired(s, 0, 0, g)
        arrive(direct_in.at[s, rows], square_sem.at[1, s, g])
        value = value + direct_in[s, rows].astype(f32)
        arrive(relay_in.at[s, rows], square_sem.at[2, s, g])
        value = value + relay_in[s, rows].astype(f32)
        if s:
            work[s, 0, 0, rows] = value.astype(bf16)
            send(
                work.at[s, 0, 0, rows], column_in.at[z, rows], column_sem.at[z, g],
                place(planes[s], x, y, core), "column", s, g,
            )
        else:
            own_total[rows, :] = value

    across = (((1,), (1,)), ((), ()))
    score_scale = (NOPE + ROPE) ** (-0.5)

    def angles():
        near = base_ref[...]
        swapped = pltpu.roll(near, ROPE, 1)
        lane = lax.broadcasted_iota(jnp.int32, near.shape, 1)
        cosine, sine = jnp.where(lane < ROPE, near, swapped), jnp.where(lane < ROPE, swapped, near)
        step = jnp.broadcast_to(step_ref[pl.ds(ep, 1), :], near.shape)
        step_swapped = pltpu.roll(step, ROPE, 1)
        step_cos, step_sin = jnp.where(lane < ROPE, step, step_swapped), jnp.where(lane < ROPE, step_swapped, step)
        turn_ref[...] = jnp.where(
            lane < ROPE, cosine * step_cos - sine * step_sin, sine * step_cos + cosine * step_sin
        )

    def rotate(vectors, table):
        lane = lax.broadcasted_iota(jnp.int32, vectors.shape, 1)
        size = vectors.shape[1]
        turned = jnp.where(
            lane < half, -pltpu.roll(vectors, size - half, 1), pltpu.roll(vectors, half, 1)
        )
        sine = pltpu.roll(table, size - ROPE, 1)
        return jnp.where(lane < ROPE, vectors * table + turned * sine, 0.0)

    own = pl.ds(first_own, quarter)

    def own_normed():
        return rms_rows(mix_ref[own, :].astype(f32), mix_gain[...]).astype(bf16)

    def prepare_rows():
        loaded(9)
        rows_all[ep, tp, :, :width] = rms_rows(ffn_ref[...].astype(f32), ffn_gain[...]).astype(bf16)
        angles()
        turned = lax.dot_general(own_normed(), rotary_ref[...], across, preferred_element_type=f32)
        turned = jnp.concatenate([turned, jnp.zeros((quarter, ROPE), f32)], axis=1)
        rotary_key = rotate(turned, turn_ref[own, :])
        scores = scores_ref[...]
        shares = jnp.exp(scores - jnp.max(scores, axis=0, keepdims=True))
        shares = shares / jnp.sum(shares, axis=0, keepdims=True)
        routes = routes_ref[...]
        lane = lax.broadcasted_iota(jnp.int32, (2 * ROPE, row_count), 0)
        named = jnp.zeros((2 * ROPE, row_count), f32)
        for k in range(routes.shape[0]):
            hit = (lane == routes[k : k + 1] + ROPE) | (lane == routes[k : k + 1] + ROPE + experts)
            named = named + jnp.where(hit, shares[k : k + 1], 0.0)
        coarse = named.astype(bf16).astype(f32)
        table_ref[...] = jnp.where(lane < ROPE + experts, coarse, named - coarse).T
        rows_all[ep, tp, :, width:] = (rotary_key + table_ref[own, :]).astype(bf16)

    def prepare_lats():
        loaded(11)
        latent = jnp.dot(own_normed(), latent_ref[...], preferred_element_type=f32)
        lat_all[ep, tp] = rms_rows(latent, latent_gain[...]).astype(bf16)

    def prepare_queries():
        loaded(12)
        normed = rms_rows(mix_ref[...].astype(f32), mix_gain[...]).astype(bf16)
        for h in range(0, heads, 2):
            columns_of = slice(h * (NOPE + ROPE), (h + 2) * (NOPE + ROPE))
            two = jnp.dot(normed, query_w[:, columns_of], preferred_element_type=f32)
            table = turn_ref[...]
            middle, last = two[:, NOPE : 2 * NOPE], two[:, 2 * NOPE :]
            lane = lax.broadcasted_iota(jnp.int32, last.shape, 1)
            low, high = pltpu.roll(middle, ROPE, 1), pltpu.roll(last, ROPE, 1)
            query_ref[h, :, :NOPE] = two[:, :NOPE].astype(bf16)
            query_ref[h, :, NOPE:] = rotate(middle, table).astype(bf16)
            query_ref[h + 1, :, :NOPE] = jnp.where(lane < ROPE, low, high).astype(bf16)
            query_ref[h + 1, :, NOPE:] = rotate(high, table).astype(bf16)

    def attend_block(s):
        for a in (0, 1):
            for b in (0, 1):
                take_lat(place(planes[s], flip(x, a), flip(y, b), 1 - core))
        pair = pl.ds(planes[s] * 2, 2)
        latent = lat_all[pair].reshape(block_rows, lat_all.shape[3])
        rest = rows_all[pair, :, :, width:].reshape(block_rows, 2 * ROPE)
        key_block = jnp.dot(latent, key_ref[...], preferred_element_type=f32).astype(bf16)
        value_block = jnp.dot(latent, value_ref[...], preferred_element_type=f32).astype(bf16)
        for h in range(heads):
            keys[h, :, :NOPE] = key_block[:, h * NOPE : (h + 1) * NOPE]
            keys[h, :, NOPE:] = rest
            values[h] = value_block[:, h * VD : (h + 1) * VD]
        shape = (row_count, block_rows)
        places = lax.broadcasted_iota(jnp.int32, shape, 0) + ep * row_count
        allowed = lax.broadcasted_iota(jnp.int32, shape, 1) + planes[s] * block_rows <= places
        for h in range(heads):
            scores = lax.dot_general(query_ref[h], keys[h], across, preferred_element_type=f32)
            weights = jnp.where(allowed, jnp.exp(scores * score_scale), 0.0)
            total = jnp.broadcast_to(jnp.sum(weights, axis=1, keepdims=True), (row_count, VD))
            update = jnp.dot(weights.astype(bf16), values[h], preferred_element_type=f32)
            totals[h] = total if s == 0 else totals[h] + total
            weighted[h] = update if s == 0 else weighted[h] + update

    def attend_plane(s):
        loaded(17)
        if s == 0:
            attend_block(s)
        else:
            pl.when(below(s))(lambda: attend_block(s))

    def project():
        loaded(18)
        for h in range(heads):
            attended[:, h * VD : (h + 1) * VD] = (weighted[h] / totals[h]).astype(bf16)
        chunk = 512
        for n in range(0, width, chunk):
            out = jnp.dot(attended[...], output_ref[:, n : n + chunk], preferred_element_type=f32)
            heads_ref[:, :, n : n + chunk] = out.astype(bf16).reshape(parts, quarter, chunk)
        for b in (1, 0):
            send(
                heads_ref.at[flip(y, b) * 2 + 1 - core], heads_twin.at[b], heads_sem.at[b], twin,
                "heads", b,
            )

    def cross_heads():
        arrive(heads_twin.at[1], heads_sem.at[1])
        heads_work[...] = (
            heads_ref[(1 - y) * 2 + core].astype(f32) + heads_twin[1].astype(f32)
        ).astype(bf16)
        send(heads_work, heads_in, heads_sem.at[2], y_next, "heads", 2)

    def finish_heads():
        loaded(len(loads))
        arrive(heads_twin.at[0], heads_sem.at[0])
        arrive(heads_in, heads_sem.at[2])
        projected = (
            heads_ref[y * 2 + core].astype(f32) + heads_twin[0].astype(f32) + heads_in[...].astype(f32)
        )
        out_ref[0] = rms_rows(projected, gain_ref[...]).astype(bf16)

    def finish_moe():
        for g in range(PIECES):
            rows = rows_of(g)
            total = own_total[rows, :]
            for s in range(1, depth):
                arrive(column_in.at[planes[s], rows], column_sem.at[planes[s], g])
                total = total + column_in[planes[s], rows].astype(f32)
            out_ref[1, rows, :] = total.astype(bf16)

    def start_rows():
        prepare_rows()
        greeted()
        own_rows()
        for load in loads[early:]:
            load.start()

    steps = {
        "prep": start_rows, "lats": prepare_lats, "qry": prepare_queries, "Lown": own_lats,
        "X0a": lambda: side_rows("x"), "Y0b": lambda: side_rows("y"), "XY0": side_rows_rest,
        **{f"C0{g}": functools.partial(corner_rows, g) for g in range(PIECES)},
        "LX0": lambda: side_lats(1), "LY0": lambda: side_lats(0), "LC0": corner_lats,
        "PR": project, "CH": cross_heads, "FH": finish_heads, "FM": finish_moe,
    }
    kinds = {
        "Z": lambda s, g: column_rows(s, g, 0), "D": lambda s, g: column_rows(s, g, 1),
        "X": lambda s: square_rows(s, 1), "Y": lambda s: square_rows(s, 0),
        "LZ": lambda s: column_lats(s, 0), "LD": lambda s: column_lats(s, 1),
        "LX": lambda s: square_lats(s, 1), "LY": lambda s: square_lats(s, 0),
        "E": expert_plane, "A": attend_plane, "R": sum_relay, "Q": sum_square,
    }

    def run(step):
        if step in steps:
            steps[step]()
        elif step[0] == "P":
            sum_pairs(int(step[1]), step[2] == "a")
        else:
            kind = step.rstrip("0123456789")
            kinds[kind](*(int(digit) for digit in step[len(kind) :]))

    def settle(until, most):
        ready = [k for k, (_, _, step) in issued.items() if k not in settled and step <= until]
        for key in ready[:most]:
            build, condition, _ = issued[key]
            guarded(condition, lambda: build().wait_send())
            settled.add(key)

    def walk(order):
        for step in order:
            if isinstance(step, tuple):
                settle(*step)
            else:
                run(NAMES[step])
                now[0] += 1

    orders = (OUTER, INNER)
    shared = 0
    while orders[0][shared] == orders[1][shared]:
        shared += 1
    walk(orders[0][:shared])
    ready, sent, step_now, done = waited[0], dict(issued), now[0], set(settled)
    for name, chosen, order in (("outer", is_outer, orders[0]), ("inner", is_inner, orders[1])):
        role[0], waited[0], now[0] = name, ready, step_now
        issued.clear()
        issued.update(sent)
        settled.clear()
        settled.update(done)

        @pl.when(chosen)
        def _():
            walk(order[shared:])
            settle(now[0], len(issued))


def scoped_kernel(width, heads, sems, *refs):
    pl.run_scoped(lambda *held: layer_kernel(width, heads, *refs, *held), *sems)


def turn_tables(row_count, experts):
    inverse = rope_base ** (-np.arange(0, ROPE, 2) / ROPE)
    near, far = np.arange(row_count)[:, None] * inverse, row_count * np.arange(experts)[:, None] * inverse

    def lanes(angle):
        return np.concatenate([np.cos(angle)] * 2 + [np.sin(angle)] * 2, axis=1).astype(np.float32)

    return lanes(near), lanes(far)


def dense_local(
    mix_in, mix_gain, query_weight, latent_weight, rotary_weight, latent_gain, key_weight,
    value_weight, output_weight, out_gain, ffn_in, ffn_gain, gate_weight, up_weight, down_weight,
    routes, route_scores,
):
    experts, parts = lax.axis_size("ep"), lax.axis_size("tp")
    row_count, width = mix_in.shape
    quarter, depth = row_count // parts, experts // 2
    block_rows = 2 * row_count
    heads = query_weight.shape[1] // (NOPE + ROPE)
    base, step = turn_tables(row_count, experts)
    row = lambda gain: gain.reshape(1, -1)
    operands = (
        ffn_in, mix_in, row(ffn_gain), row(mix_gain), row(latent_gain), row(out_gain), routes.T,
        route_scores.T, jnp.asarray(base), jnp.asarray(step), latent_weight, rotary_weight.T, query_weight,
        gate_weight[0], up_weight[0], down_weight[0], key_weight, value_weight, output_weight,
    )
    held = lambda *lead: pltpu.VMEM(lead + (quarter, width), jnp.bfloat16)
    scratch = lambda *shape: pltpu.VMEM(shape, jnp.bfloat16)
    wide = lambda *shape: pltpu.VMEM(shape, jnp.float32)
    sems = lambda *shape: pltpu.SemaphoreType.DMA(shape)
    semaphores = (
        sems(160), sems(experts, parts, PIECES), sems(48), sems(experts, parts), sems(128),
        sems(depth, 2, 2), sems(3, depth, PIECES), sems(depth, PIECES), sems(depth, PIECES), sems(3),
        sems(len(operands)),
        )
    both = pl.pallas_call(
        functools.partial(scoped_kernel, width, heads, semaphores),
        out_shape=pltpu.VMEM((2, quarter, width), jnp.bfloat16),
        in_specs=[pl.BlockSpec(memory_space=pl.ANY)] * len(operands),
        out_specs=pl.BlockSpec(memory_space=pltpu.VMEM),
        scratch_shapes=[
            scratch(experts, parts, quarter, width + 2 * ROPE),
            scratch(experts, parts, quarter, latent_weight.shape[1]),
            held(depth, 2, parts), held(depth, 2, 2), held(depth, 2, 2),
            held(depth), held(depth), held(depth), held(depth), held(depth),
            held(parts), held(), held(2), held(),
            scratch(heads, row_count, NOPE + 2 * ROPE), scratch(heads, block_rows, NOPE + 2 * ROPE),
            scratch(heads, block_rows, VD), wide(heads, row_count, VD), wide(heads, row_count, VD),
            scratch(row_count, heads * VD), wide(quarter, width),
            wide(row_count, 2 * ROPE), wide(row_count, 2 * ROPE),
            pltpu.VMEM((quarter, width), ffn_in.dtype), pltpu.VMEM(mix_in.shape, mix_in.dtype),
        ]
        + [pltpu.VMEM(a.shape, a.dtype) for a in operands[2:]],
        compiler_params=pltpu.CompilerParams(
            collective_id=0, has_side_effects=True, vmem_limit_bytes=60 * 1024 * 1024
        ),
        name="layer",
    )(*operands)
    return both[0], both[1]


def solution(mesh):
    experts, parts = mesh.shape["ep"], mesh.shape["tp"]

    def body(*args):
        quarter, choose = args[10].shape[0] // parts, args[15].shape[1]
        every_row = 2 * quarter * choose >= quarter * experts
        paired = parts == 4 and experts == 8 and quarter % (8 * PIECES) == 0
        return (dense_local if every_row and paired else local)(*args)
    placed = (
        P("ep", None),
        P(),
        P(None, "tp"),
        P(),
        P(),
        P(),
        P(None, "tp"),
        P(None, "tp"),
        P("tp", None),
        P(),
        P("ep", None),
        P(),
        P("ep", None, "tp"),
        P("ep", None, "tp"),
        P("ep", "tp", None),
        P("ep", None),
        P("ep", None),
    )
    return jax.shard_map(
        body,
        mesh=mesh,
        in_specs=placed,
        out_specs=(P(("ep", "tp"), None), P(("ep", "tp"), None)),
        check_vma=False,
    )
```

```python
import jax
import jax.numpy as jnp
import functools
import numpy as np
from jax import lax
from jax.experimental import pallas as pl
from jax.experimental.pallas import tpu as pltpu
from jax.sharding import PartitionSpec as P

NOPE = 128
ROPE = 64
VD = 128


norm_eps = 1e-06
clamp_limit = 7.0
gate_slope = 1.702
rope_base = 10000.0


def rms_rows(rows_in, scales):
    mean_square = jnp.mean(rows_in * rows_in, axis=-1, keepdims=True)
    return rows_in * lax.rsqrt(mean_square + norm_eps) * scales


def rms_columns(columns, scales):
    mean_square = jnp.mean(columns * columns, axis=0, keepdims=True)
    return columns * lax.rsqrt(mean_square + norm_eps) * scales[:, None]


def turn_table(positions):
    inverse = rope_base ** (-jnp.arange(0, ROPE, 2).astype(jnp.float32) / ROPE)
    angle_rows = inverse[:, None] * positions.astype(jnp.float32)[None, :]
    return (jnp.cos(angle_rows), jnp.sin(angle_rows))


def clamped_unit(gate_part, linear):
    gate_part = jnp.minimum(gate_part, clamp_limit)
    linear = jnp.clip(linear, -clamp_limit, clamp_limit)
    return gate_part * jax.nn.sigmoid(gate_slope * gate_part) * (linear + 1.0)


def keep_state(running):
    return running


def local(
    mix_in,
    mix_gain,
    query_weight,
    latent_weight,
    rotary_weight,
    latent_gain,
    key_weight,
    value_weight,
    output_weight,
    out_gain,
    ffn_in,
    ffn_gain,
    gate_weight,
    up_weight,
    down_weight,
    routes,
    route_scores,
):
    row_count = mix_in.shape[0]
    first_row = lax.axis_index("ep") * row_count
    last_row = first_row + row_count - 1
    positions = first_row + jnp.arange(row_count, dtype=jnp.int32)
    normed = rms_rows(mix_in.astype(jnp.float32), mix_gain).astype(jnp.bfloat16)
    head_count = query_weight.shape[1] // (NOPE + ROPE)
    half_rope = ROPE // 2
    cosine, sine_rows = turn_table(positions)
    queries = jnp.dot(normed, query_weight, preferred_element_type=jnp.float32).reshape(
        row_count, head_count, NOPE + ROPE
    )
    query_plain = queries[..., :NOPE].astype(jnp.bfloat16)
    query_cos = cosine.T[:, None, :]
    query_sin = sine_rows.T[:, None, :]
    query_upper = queries[..., NOPE : NOPE + half_rope]
    query_lower = queries[..., NOPE + half_rope :]
    query_turn = jnp.concatenate(
        [
            query_upper * query_cos - query_lower * query_sin,
            query_lower * query_cos + query_upper * query_sin,
        ],
        axis=-1,
    ).astype(jnp.bfloat16)
    across = (((0,), (1,)), ((), ()))
    latent = rms_columns(
        lax.dot_general(latent_weight, normed, across, preferred_element_type=jnp.float32),
        latent_gain,
    ).astype(jnp.bfloat16)
    rot_raw = lax.dot_general(rotary_weight, normed, across, preferred_element_type=jnp.float32)
    rotary_key = jnp.concatenate(
        [
            rot_raw[:half_rope] * cosine - rot_raw[half_rope:] * sine_rows,
            rot_raw[half_rope:] * cosine + rot_raw[:half_rope] * sine_rows,
        ],
        axis=0,
    ).astype(jnp.bfloat16)
    score_scale = (NOPE + ROPE) ** (-0.5)
    contract_first = (((0,), (0,)), ((), ()))

    def expand(latent_block):
        key_block = lax.dot_general(
            key_weight, latent_block, contract_first, preferred_element_type=jnp.float32
        ).astype(jnp.bfloat16)
        value_block = lax.dot_general(
            value_weight, latent_block, contract_first, preferred_element_type=jnp.float32
        ).astype(jnp.bfloat16)
        return (key_block, value_block)

    def attend(key_block, value_block, turn_block):
        key_count = key_block.shape[1]
        key_block = key_block.reshape(head_count, NOPE, key_count)
        value_block = value_block.reshape(head_count, VD, key_count)
        scores = jnp.einsum(
            "ihd,hdj->hij", query_plain, key_block, preferred_element_type=jnp.float32
        )
        scores = scores + jnp.einsum(
            "ihd,dj->hij", query_turn, turn_block, preferred_element_type=jnp.float32
        )
        key_places = jnp.arange(key_count, dtype=jnp.int32)
        allowed = key_places[None, :] <= positions[:, None]
        weights = jnp.where(allowed[None], jnp.exp(scores * score_scale), 0.0)
        weighted = jnp.einsum(
            "hij,hdj->hid",
            weights.astype(jnp.bfloat16),
            value_block,
            preferred_element_type=jnp.float32,
        )
        return (jnp.sum(weights, axis=-1), weighted)

    initial = (
        jnp.zeros((head_count, row_count), jnp.float32),
        jnp.zeros((head_count, row_count, VD), jnp.float32),
    )
    shard_piece = (
        lax.all_gather(latent, "ep", axis=1, tiled=True),
        lax.all_gather(rotary_key, "ep", axis=1, tiled=True),
    )

    def compute_piece(running):
        key_block, value_block = expand(shard_piece[0])
        return attend(key_block, value_block, shard_piece[1])

    totals, weighted = lax.cond(jnp.int32(0) > last_row, keep_state, compute_piece, initial)
    attended = (weighted / totals[..., None]).astype(jnp.bfloat16)
    mixing = output_weight.reshape(head_count, VD, output_weight.shape[1])
    partial_value = jnp.einsum("hid,hde->ie", attended, mixing, preferred_element_type=jnp.float32)
    projected = lax.psum_scatter(
        lax.optimization_barrier(partial_value.astype(jnp.bfloat16))
        .astype(jnp.float32)
        .astype(jnp.bfloat16),
        "tp",
        scatter_dimension=0,
        tiled=True,
    ).astype(jnp.float32)
    mixed = rms_rows(projected, out_gain).astype(jnp.bfloat16)
    tokens = ffn_in.shape[0]
    part_count = lax.axis_size("tp")
    quarter_rows = tokens // part_count
    experts = lax.axis_size("ep")
    choose = routes.shape[1]
    capacity = max(2, 2 * quarter_rows * choose // experts)
    slot_count = capacity * part_count
    tp_index = lax.axis_index("tp")
    normed_b = rms_rows(ffn_in.astype(jnp.float32), ffn_gain).astype(jnp.bfloat16)
    padded = jnp.concatenate([normed_b, jnp.zeros((1, normed_b.shape[1]), jnp.bfloat16)], axis=0)
    gate_share = jax.nn.softmax(route_scores, axis=-1)
    grouped = routes.reshape(part_count, quarter_rows * choose)
    onehot = (grouped[:, :, None] == jnp.arange(experts, dtype=jnp.int32)[None, None, :]).astype(
        jnp.int32
    )
    slot_rank = jnp.sum((jnp.cumsum(onehot, axis=1) - 1) * onehot, axis=2)
    slot_index = jnp.arange(part_count, dtype=jnp.int32)[:, None] * capacity + slot_rank
    place_index = (slot_index * experts + grouped).reshape(-1)
    owners = jnp.arange(tokens * choose, dtype=jnp.int32) // choose
    slot_token = jnp.full((slot_count * experts,), tokens, jnp.int32).at[place_index].set(owners)
    unit_count = gate_weight.shape[2]
    chosen = lax.dynamic_slice_in_dim(
        slot_token, tp_index * capacity * experts, capacity * experts, 0
    )
    outgoing = padded[chosen].reshape(capacity, experts, -1)
    arrived = lax.all_to_all(outgoing, "ep", split_axis=1, concat_axis=1, tiled=True)
    row_block = lax.all_gather(arrived, "tp", axis=0, tiled=True)
    block_slots = row_block.shape[0]
    flat_rows = row_block.reshape(-1, row_block.shape[2])
    gate_part = jnp.dot(flat_rows, gate_weight[0], preferred_element_type=jnp.float32)
    up_part = jnp.dot(flat_rows, up_weight[0], preferred_element_type=jnp.float32)
    hidden = (
        clamped_unit(gate_part, up_part).astype(jnp.bfloat16).reshape(block_slots, -1, unit_count)
    )
    sources = hidden.shape[1]
    hidden_flat = hidden.reshape(slot_count * sources, unit_count)
    partial_value = jnp.dot(hidden_flat, down_weight[0], preferred_element_type=jnp.float32)
    result = lax.psum_scatter(
        lax.optimization_barrier(partial_value.astype(jnp.bfloat16))
        .astype(jnp.float32)
        .astype(jnp.bfloat16),
        "tp",
        scatter_dimension=0,
        tiled=True,
    )
    result = result.reshape(capacity, sources, -1)
    returned = lax.all_to_all(result, "ep", split_axis=1, concat_axis=1, tiled=True)
    back_rows = returned.reshape(capacity * experts, -1)
    own_rank = lax.dynamic_index_in_dim(slot_rank, tp_index, 0, keepdims=False)
    own_expert = lax.dynamic_index_in_dim(grouped, tp_index, 0, keepdims=False)
    picked = (
        back_rows[own_rank * experts + own_expert]
        .astype(jnp.float32)
        .reshape(quarter_rows, choose, -1)
    )
    own_gates = lax.dynamic_slice_in_dim(gate_share, tp_index * quarter_rows, quarter_rows, 0)
    moe_out = jnp.sum(picked * own_gates[:, :, None], axis=1).astype(jnp.bfloat16)
    return (mixed, moe_out)


MESH = pl.DeviceIdType.MESH
PIECES = 4
NAMES = (
    "A0", "A1", "A2", "A3", "C00", "C01", "C02", "C03", "CH", "D10", "D11", "D12", "D13", "D20", "D21", "D22",
    "D23", "D30", "D31", "D32", "D33", "E0", "E1", "E2", "E3", "FH", "FM", "LC0", "LD1", "LD2", "LD3", "LX0",
    "LX1", "LX2", "LX3", "LY0", "LY1", "LY2", "LY3", "LZ1", "LZ2", "LZ3", "Lown", "P0a", "P0b", "P1a", "P1b",
    "P2a", "P2b", "P3a", "P3b", "PR", "Q00", "Q01", "Q02", "Q03", "Q10", "Q11", "Q12", "Q13", "Q20", "Q21", "Q22",
    "Q23", "Q30", "Q31", "Q32", "Q33", "R00", "R01", "R02", "R03", "R10", "R11", "R12", "R13", "R20", "R21",
    "R22", "R23", "R30", "R31", "R32", "R33", "X0a", "X1", "X2", "X3", "XY0", "Y0b", "Y1", "Y2", "Y3", "Z10",
    "Z11", "Z12", "Z13", "Z20", "Z21", "Z22", "Z23", "Z30", "Z31", "Z32", "Z33", "lats", "prep", "qry",
)
OUTER = (
    106, 105, 42, 89, 84, 93, 94, 95, 96, 4, 31, (2, 22), 5, 6, 7, 35, (2, 111), 90, 97, 98, (7, 19), 27, 9, 10,
    88, 99, 100, 40, 101, (12, 23), 102, 107, 39, 85, 11, 12, (16, 23), 103, (21, 17), 22, 104, 91, (23, 45), 45,
    13, 86, 14, 15, 37, 46, 72, 73, 74, 16, 75, 21, 87, 92, 23, 17, 18, 19, 20, 41, 47, 48, 76, 77, 33, 78, 79,
    36, 32, 24, (50, 47), 49, 43, 50, 34, 60, 28, 61, 0, 62, 63, 30, 29, 56, 57, 38, 58, 59, 1, 80, 81, 3, 82, 83,
    44, 68, 2, 69, 51, 70, 64, 65, (68, 13), 8, 66, 67, 71, (68, 182), 25, 52, 53, 54, 55, 26,
)
INNER = (
    106, 105, 42, 84, 89, 97, 93, 98, 99, 94, 100, 95, 107, 96, 40, 4, (2, 21), 5, 101, 102, 6, 31, 7, (2, 46), 9,
    (6, 23), 10, 88, 103, 104, 13, (7, 18), 11, (8, 21), 86, 14, 91, 12, 15, 16, (10, 33), 90, 39, 35, 85, 23, 17,
    18, 22, 47, 87, 19, 20, 33, 41, 45, 32, 37, 92, 48, 28, 46, 21, 36, 27, 24, 34, (40, 45), 49, 72, 73, 76, 30,
    50, 29, 74, 38, 75, 77, 0, 56, (48, 20), 57, 3, 78, 79, 1, 80, 58, 59, 81, 82, 83, 2, 51, (60, 14), 64, 8, 65,
    43, 66, 60, (65, 18), 67, 44, (70, 32), 68, (75, 21), 69, (76, 21), 70, (87, 21), 71, 61, 62, (87, 50), 52,
    (87, 20), 53, 25, 63, 54, (93, 20), 55, (96, 20), 26,
)
CROSS = (1, 2)


def flip(value, bits):
    bit = 1
    while bit <= bits:
        if bits & bit:
            value = value + bit - 2 * bit * ((value // bit) % 2)
        bit *= 2
    return value


def here():
    ep, tp = lax.axis_index("ep"), lax.axis_index("tp")
    return ep // 2, ep % 2, tp // 2, tp % 2


def place(z, x, y, core):
    return {"ep": z * 2 + x, "tp": y * 2 + core}


def greet(partners, extra, has_extra):
    barrier = pltpu.get_barrier_semaphore()
    for partner in partners:
        pl.semaphore_signal(barrier, inc=1, device_id=partner, device_id_type=MESH)

    @pl.when(has_extra)
    def _():
        pl.semaphore_signal(barrier, inc=1, device_id=extra, device_id_type=MESH)

    def wait():
        @pl.when(has_extra)
        def _():
            pl.semaphore_wait(barrier, len(partners) + 1)

        @pl.when(jnp.logical_not(has_extra))
        def _():
            pl.semaphore_wait(barrier, len(partners))

    return wait


def layer_kernel(
    width, heads,
    ffn_hbm, mix_hbm, ffn_gain_hbm, mix_gain_hbm, latent_gain_hbm, out_gain_hbm, routes_hbm, scores_hbm,
    base_hbm, step_hbm, latent_hbm, rotary_hbm, query_hbm, gate_hbm, up_hbm, down_hbm, key_hbm,
    value_hbm, output_hbm, out_ref,
    rows_all, lat_all, part_ref, work, twin_in, hop_in, direct_in, relay_in, column_in, corner_in,
    heads_ref, heads_work, heads_twin, heads_in, query_ref, keys, values, weighted, totals, attended, own_total,
    table_ref, turn_ref, ffn_ref, mix_ref,
    ffn_gain, mix_gain, latent_gain, gain_ref, routes_ref, scores_ref, base_ref, step_ref, latent_ref,
    rotary_ref, query_w, gate_ref, up_ref, down_ref, key_ref, value_ref, output_ref,
    row_send, row_recv, lat_send, lat_recv, send_sem, twin_sem, square_sem, column_sem, corner_sem, heads_sem, load_sem,
):
    f32, bf16 = jnp.float32, jnp.bfloat16
    ep, tp = lax.axis_index("ep"), lax.axis_index("tp")
    z, x, y, core = here()
    inner = ((z + 1) // 2) % 2
    planes = [z, flip(z, 1)]
    far = flip(z, 2)
    planes.append(far + inner * (1 - 2 * (far % 2)))
    planes.append(flip(planes[2], 1))
    depth = len(planes)
    x_next, y_next, twin = place(z, 1 - x, y, core), place(z, x, 1 - y, core), place(z, x, y, 1 - core)
    z_out, z_in = place(planes[1], x, y, core), place(flip(z, 3), x, y, core)
    parts, quarter = part_ref.shape[2:4]
    row_count = parts * quarter
    block_rows = 2 * row_count
    experts = 2 * depth
    half = ROPE // 2
    piece = quarter // PIECES
    first_own = pl.multiple_of(tp * quarter, quarter)
    copied = (
        (ffn_hbm.at[pl.ds(first_own, quarter)], ffn_ref), (ffn_gain_hbm, ffn_gain),
        (mix_hbm, mix_ref), (mix_gain_hbm, mix_gain), (rotary_hbm, rotary_ref),
        (base_hbm, base_ref), (step_hbm, step_ref), (routes_hbm, routes_ref), (scores_hbm, scores_ref),
        (latent_hbm, latent_ref), (latent_gain_hbm, latent_gain), (query_hbm, query_w),
        (gate_hbm, gate_ref), (up_hbm, up_ref), (down_hbm, down_ref),
        (key_hbm, key_ref), (value_hbm, value_ref), (output_hbm, output_ref), (out_gain_hbm, gain_ref),
    )
    loads = [pltpu.make_async_copy(src, dst, load_sem.at[n]) for n, (src, dst) in enumerate(copied)]
    greeted = greet([z_out, x_next, y_next, twin], z_in, inner == 1)
    early = 11
    for load in loads[:early]:
        load.start()
    waited = [0]

    def loaded(count):
        while waited[0] < count:
            loads[waited[0]].wait()
            waited[0] += 1

    always = None
    issued, settled, now = {}, set(), [0]

    def guarded(condition, action):
        if condition is None:
            action()
        else:
            pl.when(condition)(action)

    role = ["both"]

    def post(key, build, condition=always):
        if condition == "inner":
            if role[0] == "outer":
                return
            condition = always if role[0] == "inner" else is_inner
        issued.setdefault(key, (build, condition, now[0]))
        guarded(condition, lambda: build().start())

    numbers = {}

    def number(kind, key):
        taken = numbers.setdefault(kind, {})
        return taken.setdefault(key, len(taken))

    def at_piece(ref, g):
        return ref if g is None else ref.at[pl.ds(g * piece, piece)]

    def row_copy(origin, g, target, key):
        e, t = origin["ep"], origin["tp"]
        ref = at_piece(rows_all.at[e, t], g)
        return pltpu.make_async_remote_copy(
            src_ref=ref, dst_ref=ref, send_sem=row_send.at[number("row", key)],
            recv_sem=row_recv.at[e, t, g or 0], device_id=target, device_id_type=MESH,
        )

    def give_row(name, origin, g, target, towards, condition=always):
        key = (name, g, towards)
        post(("row",) + key, lambda: row_copy(origin, g, target, key), condition)

    def take_row(origin, g):
        row_copy(origin, g, twin, ("any",)).wait_recv()

    def lat_copy(origin, target, key):
        e, t = origin["ep"], origin["tp"]
        ref = lat_all.at[e, t]
        return pltpu.make_async_remote_copy(
            src_ref=ref, dst_ref=ref, send_sem=lat_send.at[number("lat", key)],
            recv_sem=lat_recv.at[e, t], device_id=target, device_id_type=MESH,
        )

    def give_lat(name, origin, target, towards, condition=always):
        key = (name, towards)
        post(("lat",) + key, lambda: lat_copy(origin, target, key), condition)

    def take_lat(origin):
        lat_copy(origin, twin, ("any",)).wait_recv()

    def make(src, dst, sem, target, key):
        return pltpu.make_async_remote_copy(
            src_ref=src, dst_ref=dst, send_sem=send_sem.at[number("sum", key)], recv_sem=sem,
            device_id=target, device_id_type=MESH,
        )

    def send(src, dst, sem, target, *key):
        post(("sum",) + key, lambda: make(src, dst, sem, target, key))

    def arrive(dst, sem):
        make(dst, dst, sem, twin, ("any",)).wait_recv()

    is_inner, is_outer = inner == 1, inner == 0
    up_out, up_in = z % 2 == 0, z == 1
    me = place(z, x, y, core)

    origins = {
        (s, dx, dy): place(planes[s], flip(x, dx), flip(y, dy), core)
        for s in range(depth) for dx in (0, 1) for dy in (0, 1)
    }

    def origin_of(s, dx, dy):
        return origins[s, dx, dy]

    def own_rows():
        for g in range(PIECES):
            give_row("own", me, g, z_out, "out")
            give_row("own", me, g, z_in, "in", "inner")
            give_row("own", me, g, x_next, "x")
            give_row("own", me, PIECES - 1 - g, y_next, "y")
        give_row("own", me, None, twin, "twin")

    def side_rows(first):
        by_x, by_y = origin_of(0, 1, 0), origin_of(0, 0, 1)
        for g in range(PIECES // 2):
            if first == "x":
                take_row(by_x, g)
                give_row("x0", by_x, g, y_next, "y")
            else:
                take_row(by_y, PIECES - 1 - g)
                give_row("y0", by_y, PIECES - 1 - g, x_next, "x")

    def side_rows_rest():
        by_x, by_y = origin_of(0, 1, 0), origin_of(0, 0, 1)
        for g in range(PIECES // 2):
            take_row(by_x, PIECES - 1 - g)
            take_row(by_y, g)
        give_row("x0", by_x, None, twin, "twin")
        give_row("y0", by_y, None, twin, "twin")

    def last(g):
        return g == PIECES - 1

    def corner_rows(g):
        corner = origin_of(0, 1, 1)
        take_row(corner, g)
        give_row("c0", corner, g, z_out, "out")
        give_row("c0", corner, g, z_in, "in", "inner")
        if last(g):
            give_row("c0", corner, None, twin, "twin")

    def column_rows(s, g, dx):
        origin = origin_of(s, dx, dx)
        name = f"{'zd'[dx]}{s}"
        take_row(origin, g)
        if s == 1:
            give_row(name, origin, g, z_in, "in", "inner")
        else:
            give_row(name, origin, g, z_out, "out", "inner")
        if not dx:
            give_row(name, origin, g, x_next, "x")
            give_row(name, origin, g, y_next, "y")
        if last(g):
            give_row(name, origin, None, twin, "twin")

    def square_rows(s, dx):
        origin = origin_of(s, dx, 1 - dx)
        for g in range(PIECES):
            take_row(origin, g)
        give_row(f"{'yx'[dx]}{s}", origin, None, twin, "twin")

    def own_lats():
        give_lat("own", me, z_out, "out", up_out)
        give_lat("own", me, z_in, "in", up_in)
        give_lat("own", me, x_next, "x")
        give_lat("own", me, y_next, "y")
        give_lat("own", me, twin, "twin")

    def side_lats(dx):
        origin = origin_of(0, dx, 1 - dx)
        name = f"{'yx'[dx]}0"
        take_lat(origin)
        if dx:
            give_lat(name, origin, y_next, "y")
        give_lat(name, origin, twin, "twin")

    def corner_lats():
        corner = origin_of(0, 1, 1)
        take_lat(corner)
        give_lat("c0", corner, z_out, "out", up_out)
        give_lat("c0", corner, z_in, "in", up_in)
        give_lat("c0", corner, twin, "twin")

    lower = [plane < z for plane in planes]
    up_two = z == 2

    def below(s):
        return lower[s]

    def column_lats(s, dx):
        origin = origin_of(s, dx, dx)
        name = f"{'zd'[dx]}{s}"

        @pl.when(below(s))
        def _():
            take_lat(origin)

        if s == 1:
            give_lat(name, origin, z_in, "in", up_in)
        else:
            give_lat(name, origin, z_out, "out", up_two)
        if not dx:
            give_lat(name, origin, x_next, "x", below(s))
            give_lat(name, origin, y_next, "y", below(s))
        give_lat(name, origin, twin, "twin", below(s))

    def square_lats(s, dx):
        origin = origin_of(s, dx, 1 - dx)

        @pl.when(below(s))
        def _():
            take_lat(origin)

        give_lat(f"{'yx'[dx]}{s}", origin, twin, "twin", below(s))

    def expert_plane(s):
        loaded(15)
        for a in (1, 0):
            expert_half(s, a)

    def expert_half(s, a):
        for b in (0, 1):
            take_row(place(planes[s], flip(x, a), flip(y, b), 1 - core), None)
        e = planes[s] * 2 + flip(x, a)
        block = rows_all[e, :, :, :width].reshape(row_count, width)
        gate_part = jnp.dot(block, gate_ref[...], preferred_element_type=f32)
        up_part = jnp.dot(block, up_ref[...], preferred_element_type=f32)
        hidden = clamped_unit(gate_part, up_part).astype(bf16)
        table = rows_all[e, :, :, width:].reshape(row_count, 2 * ROPE)
        lane = lax.broadcasted_iota(jnp.int32, table.shape, 1)
        is_mine = (lane == ROPE + ep) | (lane == ROPE + experts + ep)
        share = jnp.sum(jnp.where(is_mine, table.astype(f32), 0.0), axis=1, keepdims=True)
        chunk = 512
        for n in range(0, width, chunk):
            out = jnp.dot(hidden, down_ref[:, n : n + chunk], preferred_element_type=f32) * share
            part_ref[s, flip(x, a), :, :, n : n + chunk] = out.astype(bf16).reshape(parts, quarter, chunk)
        for b in (1, 0):
            mine = part_ref.at[s, flip(x, a), flip(y, b) * 2 + 1 - core]
            send(mine, twin_in.at[s, a, b], twin_sem.at[s, a, b], twin, "twin", s, a, b)

    def paired(s, a, b, g=None):
        if not g:
            arrive(twin_in.at[s, a, b], twin_sem.at[s, a, b])
        rows = slice(None) if g is None else rows_of(g)
        own = part_ref[s, flip(x, a), flip(y, b) * 2 + core, rows]
        return own.astype(f32) + twin_in[s, a, b, rows].astype(f32)

    def rows_of(g):
        return pl.ds(g * piece, piece)

    def sum_pairs(s, corner):
        a, b = (1, 1) if corner else (0, 1) if s % 2 else (1, 0)
        value = paired(s, a, b)
        if corner and s == 0 and CROSS:
            for n in (1,) if role[0] == "outer" else (1, 2, 3):
                for g in range(PIECES):
                    arrive(corner_in.at[planes[n], rows_of(g)], corner_sem.at[planes[n], g])
                value = value + corner_in[planes[n]].astype(f32)
        work[s, a, b] = value.astype(bf16)
        for g in range(PIECES):
            rows = rows_of(g)
            if corner and s in CROSS:
                send(
                    work.at[s, a, b, rows], corner_in.at[z, rows], corner_sem.at[z, g],
                    place(planes[s], x, y, core), "corner", s, g,
                )
                continue
            landing, which = (hop_in, 0) if corner else (direct_in, 1)
            send(
                work.at[s, a, b, rows], landing.at[s, rows], square_sem.at[which, s, g],
                y_next if s % 2 else x_next, which, s, g,
            )

    def sum_relay(s, g):
        a, b = (1, 0) if s % 2 else (0, 1)
        rows = rows_of(g)
        value = paired(s, a, b, g)
        if s not in CROSS:
            arrive(hop_in.at[s, rows], square_sem.at[0, s, g])
            value = value + hop_in[s, rows].astype(f32)
        work[s, a, b, rows] = value.astype(bf16)
        send(
            work.at[s, a, b, rows], relay_in.at[s, rows], square_sem.at[2, s, g],
            x_next if s % 2 else y_next, 2, s, g,
        )

    def sum_square(s, g):
        rows = rows_of(g)
        value = paired(s, 0, 0, g)
        arrive(direct_in.at[s, rows], square_sem.at[1, s, g])
        value = value + direct_in[s, rows].astype(f32)
        arrive(relay_in.at[s, rows], square_sem.at[2, s, g])
        value = value + relay_in[s, rows].astype(f32)
        if s:
            work[s, 0, 0, rows] = value.astype(bf16)
            send(
                work.at[s, 0, 0, rows], column_in.at[z, rows], column_sem.at[z, g],
                place(planes[s], x, y, core), "column", s, g,
            )
        else:
            own_total[rows, :] = value

    across = (((1,), (1,)), ((), ()))
    score_scale = (NOPE + ROPE) ** (-0.5)

    def angles():
        near = base_ref[...]
        swapped = pltpu.roll(near, ROPE, 1)
        lane = lax.broadcasted_iota(jnp.int32, near.shape, 1)
        cosine, sine = jnp.where(lane < ROPE, near, swapped), jnp.where(lane < ROPE, swapped, near)
        step = jnp.broadcast_to(step_ref[pl.ds(ep, 1), :], near.shape)
        step_swapped = pltpu.roll(step, ROPE, 1)
        step_cos, step_sin = jnp.where(lane < ROPE, step, step_swapped), jnp.where(lane < ROPE, step_swapped, step)
        turn_ref[...] = jnp.where(
            lane < ROPE, cosine * step_cos - sine * step_sin, sine * step_cos + cosine * step_sin
        )

    def rotate(vectors, table):
        lane = lax.broadcasted_iota(jnp.int32, vectors.shape, 1)
        size = vectors.shape[1]
        turned = jnp.where(
            lane < half, -pltpu.roll(vectors, size - half, 1), pltpu.roll(vectors, half, 1)
        )
        sine = pltpu.roll(table, size - ROPE, 1)
        return jnp.where(lane < ROPE, vectors * table + turned * sine, 0.0)

    own = pl.ds(first_own, quarter)

    def own_normed():
        return rms_rows(mix_ref[own, :].astype(f32), mix_gain[...]).astype(bf16)

    def prepare_rows():
        loaded(9)
        rows_all[ep, tp, :, :width] = rms_rows(ffn_ref[...].astype(f32), ffn_gain[...]).astype(bf16)
        angles()
        turned = lax.dot_general(own_normed(), rotary_ref[...], across, preferred_element_type=f32)
        turned = jnp.concatenate([turned, jnp.zeros((quarter, ROPE), f32)], axis=1)
        rotary_key = rotate(turned, turn_ref[own, :])
        scores = scores_ref[...]
        shares = jnp.exp(scores - jnp.max(scores, axis=0, keepdims=True))
        shares = shares / jnp.sum(shares, axis=0, keepdims=True)
        routes = routes_ref[...]
        lane = lax.broadcasted_iota(jnp.int32, (2 * ROPE, row_count), 0)
        named = jnp.zeros((2 * ROPE, row_count), f32)
        for k in range(routes.shape[0]):
            hit = (lane == routes[k : k + 1] + ROPE) | (lane == routes[k : k + 1] + ROPE + experts)
            named = named + jnp.where(hit, shares[k : k + 1], 0.0)
        coarse = named.astype(bf16).astype(f32)
        table_ref[...] = jnp.where(lane < ROPE + experts, coarse, named - coarse).T
        rows_all[ep, tp, :, width:] = (rotary_key + table_ref[own, :]).astype(bf16)

    def prepare_lats():
        loaded(11)
        latent = jnp.dot(own_normed(), latent_ref[...], preferred_element_type=f32)
        lat_all[ep, tp] = rms_rows(latent, latent_gain[...]).astype(bf16)

    def prepare_queries():
        loaded(12)
        normed = rms_rows(mix_ref[...].astype(f32), mix_gain[...]).astype(bf16)
        for h in range(0, heads, 2):
            columns_of = slice(h * (NOPE + ROPE), (h + 2) * (NOPE + ROPE))
            two = jnp.dot(normed, query_w[:, columns_of], preferred_element_type=f32)
            table = turn_ref[...]
            middle, last = two[:, NOPE : 2 * NOPE], two[:, 2 * NOPE :]
            lane = lax.broadcasted_iota(jnp.int32, last.shape, 1)
            low, high = pltpu.roll(middle, ROPE, 1), pltpu.roll(last, ROPE, 1)
            query_ref[h, :, :NOPE] = two[:, :NOPE].astype(bf16)
            query_ref[h, :, NOPE:] = rotate(middle, table).astype(bf16)
            query_ref[h + 1, :, :NOPE] = jnp.where(lane < ROPE, low, high).astype(bf16)
            query_ref[h + 1, :, NOPE:] = rotate(high, table).astype(bf16)

    def attend_block(s):
        for a in (0, 1):
            for b in (0, 1):
                take_lat(place(planes[s], flip(x, a), flip(y, b), 1 - core))
        pair = pl.ds(planes[s] * 2, 2)
        latent = lat_all[pair].reshape(block_rows, lat_all.shape[3])
        rest = rows_all[pair, :, :, width:].reshape(block_rows, 2 * ROPE)
        key_block = jnp.dot(latent, key_ref[...], preferred_element_type=f32).astype(bf16)
        value_block = jnp.dot(latent, value_ref[...], preferred_element_type=f32).astype(bf16)
        for h in range(heads):
            keys[h, :, :NOPE] = key_block[:, h * NOPE : (h + 1) * NOPE]
            keys[h, :, NOPE:] = rest
            values[h] = value_block[:, h * VD : (h + 1) * VD]
        shape = (row_count, block_rows)
        places = lax.broadcasted_iota(jnp.int32, shape, 0) + ep * row_count
        allowed = lax.broadcasted_iota(jnp.int32, shape, 1) + planes[s] * block_rows <= places
        for h in range(heads):
            scores = lax.dot_general(query_ref[h], keys[h], across, preferred_element_type=f32)
            weights = jnp.where(allowed, jnp.exp(scores * score_scale), 0.0)
            total = jnp.broadcast_to(jnp.sum(weights, axis=1, keepdims=True), (row_count, VD))
            update = jnp.dot(weights.astype(bf16), values[h], preferred_element_type=f32)
            totals[h] = total if s == 0 else totals[h] + total
            weighted[h] = update if s == 0 else weighted[h] + update

    def attend_plane(s):
        loaded(17)
        if s == 0:
            attend_block(s)
        else:
            pl.when(below(s))(lambda: attend_block(s))

    def project():
        loaded(18)
        for h in range(heads):
            attended[:, h * VD : (h + 1) * VD] = (weighted[h] / totals[h]).astype(bf16)
        chunk = 512
        for n in range(0, width, chunk):
            out = jnp.dot(attended[...], output_ref[:, n : n + chunk], preferred_element_type=f32)
            heads_ref[:, :, n : n + chunk] = out.astype(bf16).reshape(parts, quarter, chunk)
        for b in (1, 0):
            send(
                heads_ref.at[flip(y, b) * 2 + 1 - core], heads_twin.at[b], heads_sem.at[b], twin,
                "heads", b,
            )

    def cross_heads():
        arrive(heads_twin.at[1], heads_sem.at[1])
        heads_work[...] = (
            heads_ref[(1 - y) * 2 + core].astype(f32) + heads_twin[1].astype(f32)
        ).astype(bf16)
        send(heads_work, heads_in, heads_sem.at[2], y_next, "heads", 2)

    def finish_heads():
        loaded(len(loads))
        arrive(heads_twin.at[0], heads_sem.at[0])
        arrive(heads_in, heads_sem.at[2])
        projected = (
            heads_ref[y * 2 + core].astype(f32) + heads_twin[0].astype(f32) + heads_in[...].astype(f32)
        )
        out_ref[0] = rms_rows(projected, gain_ref[...]).astype(bf16)

    def finish_moe():
        for g in range(PIECES):
            rows = rows_of(g)
            total = own_total[rows, :]
            for s in range(1, depth):
                arrive(column_in.at[planes[s], rows], column_sem.at[planes[s], g])
                total = total + column_in[planes[s], rows].astype(f32)
            out_ref[1, rows, :] = total.astype(bf16)

    def start_rows():
        prepare_rows()
        greeted()
        own_rows()
        for load in loads[early:]:
            load.start()

    steps = {
        "prep": start_rows, "lats": prepare_lats, "qry": prepare_queries, "Lown": own_lats,
        "X0a": lambda: side_rows("x"), "Y0b": lambda: side_rows("y"), "XY0": side_rows_rest,
        **{f"C0{g}": functools.partial(corner_rows, g) for g in range(PIECES)},
        "LX0": lambda: side_lats(1), "LY0": lambda: side_lats(0), "LC0": corner_lats,
        "PR": project, "CH": cross_heads, "FH": finish_heads, "FM": finish_moe,
    }
    kinds = {
        "Z": lambda s, g: column_rows(s, g, 0), "D": lambda s, g: column_rows(s, g, 1),
        "X": lambda s: square_rows(s, 1), "Y": lambda s: square_rows(s, 0),
        "LZ": lambda s: column_lats(s, 0), "LD": lambda s: column_lats(s, 1),
        "LX": lambda s: square_lats(s, 1), "LY": lambda s: square_lats(s, 0),
        "E": expert_plane, "A": attend_plane, "R": sum_relay, "Q": sum_square,
    }

    def run(step):
        if step in steps:
            steps[step]()
        elif step[0] == "P":
            sum_pairs(int(step[1]), step[2] == "a")
        else:
            kind = step.rstrip("0123456789")
            kinds[kind](*(int(digit) for digit in step[len(kind) :]))

    def settle(until, most):
        ready = [k for k, (_, _, step) in issued.items() if k not in settled and step <= until]
        for key in ready[:most]:
            build, condition, _ = issued[key]
            guarded(condition, lambda: build().wait_send())
            settled.add(key)

    def walk(order):
        for step in order:
            if isinstance(step, tuple):
                settle(*step)
            else:
                run(NAMES[step])
                now[0] += 1

    orders = (OUTER, INNER)
    shared = 0
    while orders[0][shared] == orders[1][shared]:
        shared += 1
    walk(orders[0][:shared])
    ready, sent, step_now, done = waited[0], dict(issued), now[0], set(settled)
    for name, chosen, order in (("outer", is_outer, orders[0]), ("inner", is_inner, orders[1])):
        role[0], waited[0], now[0] = name, ready, step_now
        issued.clear()
        issued.update(sent)
        settled.clear()
        settled.update(done)

        @pl.when(chosen)
        def _():
            walk(order[shared:])
            settle(now[0], len(issued))


def scoped_kernel(width, heads, sems, *refs):
    pl.run_scoped(lambda *held: layer_kernel(width, heads, *refs, *held), *sems)


def turn_tables(row_count, experts):
    inverse = rope_base ** (-np.arange(0, ROPE, 2) / ROPE)
    near, far = np.arange(row_count)[:, None] * inverse, row_count * np.arange(experts)[:, None] * inverse

    def lanes(angle):
        return np.concatenate([np.cos(angle)] * 2 + [np.sin(angle)] * 2, axis=1).astype(np.float32)

    return lanes(near), lanes(far)


def dense_local(
    mix_in, mix_gain, query_weight, latent_weight, rotary_weight, latent_gain, key_weight,
    value_weight, output_weight, out_gain, ffn_in, ffn_gain, gate_weight, up_weight, down_weight,
    routes, route_scores,
):
    experts, parts = lax.axis_size("ep"), lax.axis_size("tp")
    row_count, width = mix_in.shape
    quarter, depth = row_count // parts, experts // 2
    block_rows = 2 * row_count
    heads = query_weight.shape[1] // (NOPE + ROPE)
    base, step = turn_tables(row_count, experts)
    row = lambda gain: gain.reshape(1, -1)
    operands = (
        ffn_in, mix_in, row(ffn_gain), row(mix_gain), row(latent_gain), row(out_gain), routes.T,
        route_scores.T, jnp.asarray(base), jnp.asarray(step), latent_weight, rotary_weight.T, query_weight,
        gate_weight[0], up_weight[0], down_weight[0], key_weight, value_weight, output_weight,
    )
    held = lambda *lead: pltpu.VMEM(lead + (quarter, width), jnp.bfloat16)
    scratch = lambda *shape: pltpu.VMEM(shape, jnp.bfloat16)
    wide = lambda *shape: pltpu.VMEM(shape, jnp.float32)
    sems = lambda *shape: pltpu.SemaphoreType.DMA(shape)
    semaphores = (
        sems(160), sems(experts, parts, PIECES), sems(48), sems(experts, parts), sems(128),
        sems(depth, 2, 2), sems(3, depth, PIECES), sems(depth, PIECES), sems(depth, PIECES), sems(3),
        sems(len(operands)),
        )
    both = pl.pallas_call(
        functools.partial(scoped_kernel, width, heads, semaphores),
        out_shape=pltpu.VMEM((2, quarter, width), jnp.bfloat16),
        in_specs=[pl.BlockSpec(memory_space=pl.ANY)] * len(operands),
        out_specs=pl.BlockSpec(memory_space=pltpu.VMEM),
        scratch_shapes=[
            scratch(experts, parts, quarter, width + 2 * ROPE),
            scratch(experts, parts, quarter, latent_weight.shape[1]),
            held(depth, 2, parts), held(depth, 2, 2), held(depth, 2, 2),
            held(depth), held(depth), held(depth), held(depth), held(depth),
            held(parts), held(), held(2), held(),
            scratch(heads, row_count, NOPE + 2 * ROPE), scratch(heads, block_rows, NOPE + 2 * ROPE),
            scratch(heads, block_rows, VD), wide(heads, row_count, VD), wide(heads, row_count, VD),
            scratch(row_count, heads * VD), wide(quarter, width),
            wide(row_count, 2 * ROPE), wide(row_count, 2 * ROPE),
            pltpu.VMEM((quarter, width), ffn_in.dtype), pltpu.VMEM(mix_in.shape, mix_in.dtype),
        ]
        + [pltpu.VMEM(a.shape, a.dtype) for a in operands[2:]],
        compiler_params=pltpu.CompilerParams(
            collective_id=0, has_side_effects=True, vmem_limit_bytes=60 * 1024 * 1024
        ),
        name="layer",
    )(*operands)
    return both[0], both[1]


def solution(mesh):
    experts, parts = mesh.shape["ep"], mesh.shape["tp"]

    def body(*args):
        quarter, choose = args[10].shape[0] // parts, args[15].shape[1]
        every_row = 2 * quarter * choose >= quarter * experts
        paired = parts == 4 and experts == 8 and quarter % (8 * PIECES) == 0
        return (dense_local if every_row and paired else local)(*args)
    placed = (
        P("ep", None),
        P(),
        P(None, "tp"),
        P(),
        P(),
        P(),
        P(None, "tp"),
        P(None, "tp"),
        P("tp", None),
        P(),
        P("ep", None),
        P(),
        P("ep", None, "tp"),
        P("ep", None, "tp"),
        P("ep", "tp", None),
        P("ep", None),
        P("ep", None),
    )
    return jax.shard_map(
        body,
        mesh=mesh,
        in_specs=placed,
        out_specs=(P(("ep", "tp"), None), P(("ep", "tp"), None)),
        check_vma=False,
    )
```
